32 devices in a mesh: grp: 2 (over y), kv: 4 (over z), tp: 4 (over x, core).
Axes of the slice: x: 2, y: 2, z: 4, core: 2. Of those that a mesh axis runs over, the one named last changes fastest.
Arguments:
- tokens: bfloat16 [48, 4096], P('grp', ('kv', 'tp')), parts along dimension 0, may hold values from -12 to 12
- lengths: int32 [48], P('grp'), parts along dimension 0, may hold values from 1 to 128, 1536 in all
- attn_gain: float32 [4096], P('kv'), may hold values from 0.1 to 1.9
- w_query: bfloat16 [4096, 4096], P('kv', 'tp'), may hold values from -0.09375 to 0.09375
- w_key: bfloat16 [4096, 4096], P('kv', 'tp'), may hold values from -0.09375 to 0.09375
- w_value: bfloat16 [4096, 4096], P('kv', 'tp'), may hold values from -0.09375 to 0.09375
- w_gate: bfloat16 [4096, 4096], P('kv', 'tp'), may hold values from -0.09375 to 0.09375
- log_decay: float32 [16], P('tp'), may hold values from -1 to 0
- key_cache: bfloat16 [48, 128, 4096], P('grp', 'kv', 'tp'), parts along dimension 0, may hold values from -6 to 6
- value_cache: bfloat16 [48, 128, 4096], P('grp', 'kv', 'tp'), parts along dimension 0, may hold values from -6 to 6
- gn_gain: float32 [4096], P('tp'), may hold values from 0.1 to 1.9
- w_out: bfloat16 [4096, 4096], P('tp', 'kv'), may hold values from -0.1875 to 0.1875
- ffn_gain: float32 [4096], P('kv'), may hold values from 0.1 to 1.9
- w_ffn_gate: bfloat16 [4096, 11264], P('kv', 'tp'), may hold values from -0.09375 to 0.09375
- w_ffn_up: bfloat16 [4096, 11264], P('kv', 'tp'), may hold values from -0.09375 to 0.09375
- w_ffn_down: bfloat16 [11264, 4096], P('tp', 'kv'), may hold values from -0.109375 to 0.109375
Outputs:
- layer_out: bfloat16 [48, 4096], P('grp', ('kv', 'tp')), parts along dimension 0
The draws below stay inside these ranges and needn't reach their ends.
There are 2 independent parts, one for each index of `grp`. The reference program is written for one: setup_inputs(seed, part) draws one part's arguments, and reference() takes and returns one part's arrays. A program takes and returns all parts, laid end to end along the dimension named above; an argument that names none is the same for every part. Nothing has to cross between parts.
All inputs are finite; a program needn't handle non-finite values.
Results may differ from the reference program's by a relative error of at most 0.012.
Values may be sent and summed in bfloat16 or wider, within the bound.
A program may use at most 64 MiB of HBM per device.

```python
import math
import jax
import jax.numpy as jnp
import numpy as np
from jax import lax

HEADS = 16
DK = 256
FF = 11264
SEQS = 24
D = 4096
L_CACHE = 128
N_KV = 4


def draw_tokens(key, part):
    folded = jax.random.fold_in(key, 11)
    second_key = jax.random.fold_in(folded, 0)
    ramp = jnp.arange(N_KV, dtype=jnp.float32) / (N_KV - 1)
    block_scale = jnp.exp(ramp * 1.0986)
    entries = jnp.clip(jax.random.normal(second_key, (SEQS, D), jnp.float32), -4.0, 4.0)
    col_scale = jnp.repeat(block_scale, D // N_KV)
    return (entries * col_scale[None, :]).astype(jnp.bfloat16)


def draw_log_decay(key, part):
    folded = jax.random.fold_in(key, 23)
    pick_key, slow_key, fast_key = jax.random.split(folded, 3)
    slow_share = 0.5
    picked = jax.random.uniform(pick_key, (HEADS,), jnp.float32) < slow_share
    slow_rate = -2.3 * jax.random.uniform(slow_key, (HEADS,), jnp.float32, 0.3, 1.0) / L_CACHE
    fast_rate = -1.0 / jax.random.uniform(fast_key, (HEADS,), jnp.float32, 30.0, 60.0)
    return jnp.where(picked, slow_rate, fast_rate).astype(jnp.float32)


def levels(rng, dims, cuts, smallest, top_value):
    gain = 1.0
    for dim, parts in cuts:
        heights = jax.random.uniform(jax.random.fold_in(jax.random.fold_in(rng, 6), dim), (parts,), jnp.float32, smallest / len(cuts), top_value / len(cuts))
        gain = gain * jnp.repeat(jnp.exp(heights), dims[dim] // parts).reshape((-1,) + (1,) * (len(dims) - 1 - dim))
    return gain


def split_up(count, total, limit, skew):
    portions = [(1 << 20) // math.isqrt(rank ** skew) + 1 for rank in range(2, count + 1)]
    spare, holding = total - limit - (count - 1), [1] * (count - 1)
    while spare > 0:
        free = [i for i in range(count - 1) if holding[i] < limit]
        pool, left = sum([portions[i] for i in free]), spare
        for i in free:
            more = min(limit - holding[i], max(1, left * portions[i] // pool), spare)
            holding[i] = holding[i] + more
            spare = spare - more
    return np.array([limit] + holding)


def uneven_parts(key, count, total, reach, slope):
    if count == 2:
        one = jax.random.randint(key, (), max(1, total - reach), min(reach, total - 1) + 1)
        return jnp.stack([one, total - one])
    sizes = jnp.asarray(split_up(count, total, reach, slope), jnp.int32)
    twos = (count - 1) // 2
    giver, taker = sizes[1:1 + 2 * twos:2], sizes[2:2 + 2 * twos:2]
    margin = jnp.minimum(giver - 1, reach - taker)
    moved = jax.random.randint(jax.random.fold_in(key, 1), (twos,), 0, 1 << 20) % (margin + 1)
    sizes = sizes.at[1:1 + 2 * twos:2].set(giver - moved).at[2:2 + 2 * twos:2].set(taker + moved)
    return sizes[jax.random.permutation(jax.random.fold_in(key, 2), count)]


def centred(stream_key, shape, scale, limit, pieces=(), kind=jnp.bfloat16):
    array = scale * jax.random.normal(stream_key, shape, jnp.float32)
    if pieces:
        array = array * levels(stream_key, shape, pieces, -0.22, 0.18)
    return jnp.clip(array, -limit, limit).astype(kind)


def setup_inputs(seed: int = 0, part: int = 0) -> dict:
    splits = jax.random.split(jax.random.key(seed), 17)
    own_keys = jax.random.split(jax.random.fold_in(splits[16], part), 17)
    return {
        "tokens": draw_tokens(jax.random.fold_in(jax.random.fold_in(splits[16], part), 71), part),
        "lengths": uneven_parts(own_keys[1], SEQS, SEQS * L_CACHE // 2, L_CACHE, 2).astype(jnp.int32),
        "attn_gain": jnp.clip(1.0 + 0.18 * jax.random.normal(splits[2], (D,), jnp.float32), 0.1, 1.9),
        "w_query": centred(splits[3], (D, D), D ** -0.5, 0.09375, ((0, 4), (1, 4))),
        "w_key": centred(splits[4], (D, D), D ** -0.5, 0.09375, ((0, 4), (1, 4))),
        "w_value": centred(splits[5], (D, D), D ** -0.5, 0.09375, ((0, 4), (1, 4))),
        "w_gate": centred(splits[6], (D, D), D ** -0.5, 0.09375, ((0, 4), (1, 4))),
        "log_decay": draw_log_decay(jax.random.fold_in(splits[16], 71), part),
        "key_cache": centred(own_keys[8], (SEQS, L_CACHE, D), 1.0, 6.0, ((1, 4), (2, 4))),
        "value_cache": centred(own_keys[9], (SEQS, L_CACHE, D), 1.0, 6.0, ((1, 4), (2, 4))),
        "gn_gain": jnp.clip(1.0 + 0.18 * jax.random.normal(splits[10], (D,), jnp.float32), 0.1, 1.9),
        "w_out": centred(splits[11], (D, D), (D // 4) ** -0.5, 0.1875, ((0, 4), (1, 4))),
        "ffn_gain": jnp.clip(1.0 + 0.18 * jax.random.normal(splits[12], (D,), jnp.float32), 0.1, 1.9),
        "w_ffn_gate": centred(splits[13], (D, FF), D ** -0.5, 0.09375, ((0, 4), (1, 4))),
        "w_ffn_up": centred(splits[14], (D, FF), D ** -0.5, 0.09375, ((0, 4), (1, 4))),
        "w_ffn_down": centred(splits[15], (FF, D), (FF // 4) ** -0.5, 0.109375, ((0, 4), (1, 4))),
    }


RMS_EPS = 0.1
GN_EPS = 1.0
ROPE_BASE = 10000.0

def rotate(vectors, positions):
    half_dim = vectors.shape[-1] // 2
    inverse = ROPE_BASE ** (-jnp.arange(half_dim, dtype=jnp.float32) / half_dim)
    angles = positions[:, None, None] * inverse[None, None, :]
    cosine = jnp.cos(angles)
    sine_part = jnp.sin(angles)
    front_part = vectors[..., :half_dim]
    back_part = vectors[..., half_dim:]
    return jnp.concatenate([front_part * cosine - back_part * sine_part, front_part * sine_part + back_part * cosine], axis=-1)

def group_norm(totals, gn_gain):
    width = totals.shape[-1]
    center = lax.optimization_barrier(jnp.sum(totals, axis=-1, keepdims=True)) / width
    spread = lax.optimization_barrier(jnp.sum(totals * totals, axis=-1, keepdims=True)) / width - center * center
    normed = (totals - center) * lax.rsqrt(spread + GN_EPS)
    return normed.reshape(normed.shape[0], -1) * gn_gain

def reference(tokens, lengths, attn_gain, w_query, w_key, w_value, w_gate, log_decay, key_cache, value_cache, gn_gain, w_out, ffn_gain, w_ffn_gate, w_ffn_up, w_ffn_down):
    batch_rows = tokens.shape[0]
    heads_all = log_decay.shape[0]
    widened = tokens.astype(jnp.float32)
    factor = lax.rsqrt(lax.optimization_barrier(jnp.sum(widened * widened, axis=1)) / D + RMS_EPS)[:, None]
    scaled = (widened * attn_gain).astype(jnp.bfloat16)
    queries = jnp.dot(scaled, w_query, preferred_element_type=jnp.float32) * factor
    new_keys = jnp.dot(scaled, w_key, preferred_element_type=jnp.float32) * factor
    new_values = jnp.dot(scaled, w_value, preferred_element_type=jnp.float32) * factor
    gates = jnp.dot(scaled, w_gate, preferred_element_type=jnp.float32) * factor
    positions = lengths.astype(jnp.float32)
    queries = rotate(queries.reshape(batch_rows, heads_all, DK), positions) * DK ** (-0.5)
    new_keys = rotate(new_keys.reshape(batch_rows, heads_all, DK), positions)
    new_values = new_values.reshape(batch_rows, heads_all, DK)
    query_low = queries.astype(jnp.bfloat16)
    cache_len = key_cache.shape[1]
    slots = jnp.arange(cache_len, dtype=jnp.int32)

    def one_sequence(packed):
        keys_seq, values_seq, query_seq, length = packed
        keys_wide = keys_seq.astype(jnp.float32).reshape(cache_len, heads_all, DK)
        scores = jnp.einsum('phd,hd->ph', keys_wide, query_seq.astype(jnp.float32))
        gaps = (length - slots).astype(jnp.float32)
        decays = jnp.exp(log_decay[None, :] * jnp.maximum(gaps, 0.0)[:, None])
        mixing = jnp.where((slots < length)[:, None], scores * decays, 0.0).astype(jnp.bfloat16)
        values_wide = values_seq.astype(jnp.float32).reshape(cache_len, heads_all, DK)
        return jnp.einsum('ph,phd->hd', mixing.astype(jnp.float32), values_wide)
    cached = lax.map(one_sequence, (key_cache, value_cache, query_low, lengths.astype(jnp.int32)))
    own_term = lax.optimization_barrier(jnp.sum(queries * new_keys, axis=-1, keepdims=True)) * new_values
    normed = group_norm(cached + own_term, gn_gain)
    gated = (jax.nn.silu(gates) * normed).astype(jnp.bfloat16)
    mixed = jnp.dot(gated, w_out, preferred_element_type=jnp.float32)
    resid = (widened + mixed).astype(jnp.bfloat16)
    resid_wide = resid.astype(jnp.float32)
    factor_mid = lax.rsqrt(lax.optimization_barrier(jnp.sum(resid_wide * resid_wide, axis=1)) / D + RMS_EPS)[:, None]
    scaled_mid = (resid_wide * ffn_gain).astype(jnp.bfloat16)
    gate_mid = jnp.dot(scaled_mid, w_ffn_gate, preferred_element_type=jnp.float32) * factor_mid
    up_mid = jnp.dot(scaled_mid, w_ffn_up, preferred_element_type=jnp.float32) * factor_mid
    hidden = (jax.nn.silu(gate_mid) * up_mid).astype(jnp.bfloat16)
    down = jnp.dot(hidden, w_ffn_down, preferred_element_type=jnp.float32)
    return (resid_wide + down).astype(jnp.bfloat16)
```

```python
import functools
import math

import jax
import jax.numpy as jnp
from jax import lax
from jax.experimental import pallas as pl
from jax.experimental.pallas import tpu as pltpu
from jax.sharding import PartitionSpec as P

DK = 256
D = 4096


RMS_EPS = 0.1
GN_EPS = 1.0
ROPE_BASE = 10000.0


def rotate(vectors, positions):
    half_dim = vectors.shape[-1] // 2
    inverse = ROPE_BASE ** (-jnp.arange(half_dim, dtype=jnp.float32) / half_dim)
    angles = positions[:, None, None] * inverse[None, None, :]
    cosine = jnp.cos(angles)
    sine_part = jnp.sin(angles)
    front_part = vectors[..., :half_dim]
    back_part = vectors[..., half_dim:]
    return jnp.concatenate(
        [front_part * cosine - back_part * sine_part, front_part * sine_part + back_part * cosine],
        axis=-1,
    )


def group_norm(totals, gn_gain):
    width = totals.shape[-1]
    center = jnp.sum(totals, axis=-1, keepdims=True) / width
    spread = jnp.sum(totals * totals, axis=-1, keepdims=True) / width - center * center
    normed = (totals - center) * lax.rsqrt(spread + GN_EPS)
    return normed.reshape(normed.shape[0], -1) * gn_gain


def channel_stat(own_squares):
    return lax.psum(own_squares, "kv")


def input_stat(own_squares):
    return lax.psum(own_squares, "kv")


def cache_partial(query_low, lengths, log_decay, key_cache, value_cache, heads_here):
    batch_rows = query_low.shape[0]
    span = key_cache.shape[1]
    slots = lax.axis_index("kv") * span + jnp.arange(span, dtype=jnp.int32)
    live = slots[None, :] < lengths[:, None]
    gaps = jnp.maximum((lengths[:, None] - slots[None, :]).astype(jnp.float32), 0.0)
    decays = jnp.exp(log_decay[None, None, :] * gaps[:, :, None])
    keys_here = key_cache.reshape(batch_rows, span, heads_here, DK)
    values_here = value_cache.reshape(batch_rows, span, heads_here, DK)
    scores = jnp.einsum("bphd,bhd->bph", keys_here, query_low, preferred_element_type=jnp.float32)
    mixing = jnp.where(live[:, :, None], scores * decays, 0.0).astype(jnp.bfloat16)
    return jnp.einsum("bph,bphd->bhd", mixing, values_here, preferred_element_type=jnp.float32)


def local(
    tokens,
    lengths,
    attn_gain,
    w_query,
    w_key,
    w_value,
    w_gate,
    log_decay,
    key_cache,
    value_cache,
    gn_gain,
    w_out,
    ffn_gain,
    w_ffn_gate,
    w_ffn_up,
    w_ffn_down,
):
    batch_rows = tokens.shape[0]
    heads_here = log_decay.shape[0]
    row_block = lax.all_gather(tokens, "tp", axis=1, tiled=True)
    widened = row_block.astype(jnp.float32)
    own_squares = jnp.sum(widened * widened, axis=1)
    scaled = (widened * attn_gain).astype(jnp.bfloat16)
    part_query = jnp.dot(scaled, w_query, preferred_element_type=jnp.float32)
    part_key = jnp.dot(scaled, w_key, preferred_element_type=jnp.float32)
    part_value = jnp.dot(scaled, w_value, preferred_element_type=jnp.float32)
    part_gate = jnp.dot(scaled, w_gate, preferred_element_type=jnp.float32)
    positions = lengths.astype(jnp.float32)
    total_squares = input_stat(own_squares)
    queries, new_keys, new_values, gates = lax.psum(
        (part_query, part_key, part_value, part_gate), "kv"
    )
    factor = lax.rsqrt(total_squares / D + RMS_EPS)[:, None]
    queries = rotate((queries * factor).reshape(batch_rows, heads_here, DK), positions) * DK ** (
        -0.5
    )
    new_keys = rotate((new_keys * factor).reshape(batch_rows, heads_here, DK), positions)
    new_values = (new_values * factor).reshape(batch_rows, heads_here, DK)
    gates = gates * factor
    query_low = queries.astype(jnp.bfloat16)
    partial_value = cache_partial(query_low, lengths, log_decay, key_cache, value_cache, heads_here)
    cached = lax.psum(partial_value.reshape(batch_rows, heads_here * DK), "kv")
    own_term = jnp.sum(queries * new_keys, axis=-1, keepdims=True) * new_values
    normed = group_norm(cached.reshape(batch_rows, heads_here, DK) + own_term, gn_gain)
    gated = (jax.nn.silu(gates) * normed).astype(jnp.bfloat16)
    out_partial = jnp.dot(gated, w_out, preferred_element_type=jnp.float32)
    mixed = lax.psum_scatter(out_partial, "tp", scatter_dimension=1, tiled=True)
    resid = (tokens.astype(jnp.float32) + mixed).astype(jnp.bfloat16)
    resid_block = lax.all_gather(resid, "tp", axis=1, tiled=True).astype(jnp.float32)
    mid_squares = jnp.sum(resid_block * resid_block, axis=1)
    scaled_mid = (resid_block * ffn_gain).astype(jnp.bfloat16)
    gate_part = jnp.dot(scaled_mid, w_ffn_gate, preferred_element_type=jnp.float32)
    up_part = jnp.dot(scaled_mid, w_ffn_up, preferred_element_type=jnp.float32)
    total_mid = channel_stat(mid_squares)
    gate_sum, up_sum = lax.psum((gate_part, up_part), "kv")
    factor_mid = lax.rsqrt(total_mid / D + RMS_EPS)[:, None]
    hidden = (jax.nn.silu(gate_sum * factor_mid) * (up_sum * factor_mid)).astype(jnp.bfloat16)
    down_partial = jnp.dot(hidden, w_ffn_down, preferred_element_type=jnp.float32)
    down = lax.psum_scatter(down_partial, "tp", scatter_dimension=1, tiled=True)
    return (resid.astype(jnp.float32) + down).astype(jnp.bfloat16)


LANES = 128
STAGE_TILES = 2
F32 = jnp.float32
BF16 = jnp.bfloat16


def window_start(index, tiles, width, parts):
    return (index * (tiles - width) + (parts - 1) // 2) // (parts - 1)


def partner(index, j, parts):
    found, bit = 0, 1
    while bit < parts:
        digit = (index // bit) % 2
        found = found + bit * ((1 - digit) if (j // bit) % 2 else digit)
        bit *= 2
    return found


def pack(value):
    middle = value.shape[1] // 2
    return jnp.concatenate([value[:, :middle], value[:, middle:]], axis=0).astype(BF16)


def unpack(packed):
    wide = packed.astype(F32)
    rows = wide.shape[0] // 2
    return jnp.concatenate([wide[:rows], wide[rows:]], axis=1)


def stage_spans(tiles, n_kv):
    step = STAGE_TILES * n_kv
    return [(first, min(step, tiles - first)) for first in range(0, tiles, step)]


def layer_kernel(
    n_kv,
    n_tp,
    tokens_hbm,
    lengths_hbm,
    attn_gain_hbm,
    log_decay_hbm,
    gn_gain_hbm,
    ffn_gain_hbm,
    wq_hbm,
    wk_hbm,
    wv_hbm,
    wg_hbm,
    kc_hbm,
    vc_hbm,
    wo_hbm,
    wfg_hbm,
    wfu_hbm,
    wfd_hbm,
    out_ref,
    wq,
    wk,
    wv,
    wg,
    kc,
    vc,
    wo,
    wfg,
    wfu,
    wfd,
    tokens_ref,
    lengths_ref,
    attn_gain_ref,
    log_decay_ref,
    gn_gain_ref,
    ffn_gain_ref,
    tok_buf,
    x_buf,
    sq_send,
    sq_recv,
    q_send,
    q_recv,
    q_full,
    trig,
    decay_buf,
    kvg_send,
    kvg_recv,
    ca_own,
    ca_send,
    ca_recv,
    ot_buf,
    o_own,
    o_send,
    o_recv,
    chip_send,
    chip_recv,
    resid_buf,
    sqm_send,
    sqm_recv,
    gu_own,
    gu_send,
    gu_recv,
    hid_buf,
    down_buf,
    d_send,
    d_recv,
    load_sem,
    kv_send_sem,
    kv_recv_sem,
    tp_send_sem,
    tp_recv_sem,
):
    rows, own_cols = tokens_ref.shape
    depth, wide = wq.shape
    span = kc.shape[1]
    half = DK // 2
    tiles = wfg.shape[1] // LANES
    win = STAGE_TILES * LANES
    stages = stage_spans(tiles, n_kv)
    heads = n_kv
    me_kv = lax.axis_index("kv")
    me_tp = lax.axis_index("tp")

    def kv_peer(j):
        return partner(me_kv, j, n_kv)

    def tp_peer(j):
        return partner(me_tp, j, n_tp)

    kv_order = tuple(range(n_kv - 1, 0, -1))
    tp_order = tuple(range(n_tp - 1, 0, -1))

    barrier = pltpu.get_barrier_semaphore()
    for j in range(1, n_kv):
        pl.semaphore_signal(
            barrier, inc=1, device_id={"kv": kv_peer(j)}, device_id_type=pl.DeviceIdType.MESH
        )
    for j in range(1, n_tp):
        pl.semaphore_signal(
            barrier, inc=1, device_id={"tp": tp_peer(j)}, device_id_type=pl.DeviceIdType.MESH
        )

    loads = {}
    for slot, (name, src, dst) in enumerate(
        (
            ("tok", tokens_hbm, tokens_ref),
            ("len", lengths_hbm, lengths_ref),
            ("ag", attn_gain_hbm, attn_gain_ref),
            ("ld", log_decay_hbm, log_decay_ref),
            ("gg", gn_gain_hbm, gn_gain_ref),
            ("fg", ffn_gain_hbm, ffn_gain_ref),
            ("wq", wq_hbm, wq),
            ("kc", kc_hbm, kc),
            ("vc", vc_hbm, vc),
            ("wk", wk_hbm, wk),
            ("wv", wv_hbm, wv),
            ("wg", wg_hbm, wg),
            ("wo", wo_hbm, wo),
            ("wfg", wfg_hbm, wfg),
            ("wfu", wfu_hbm, wfu),
            ("wfd", wfd_hbm, wfd),
        )
    ):
        loads[name] = pltpu.make_async_copy(src, dst, load_sem.at[slot])

    sent = []

    def to_kv(phase, j, src, dst):
        copy = pltpu.make_async_remote_copy(
            src_ref=src,
            dst_ref=dst,
            send_sem=kv_send_sem.at[phase, j],
            recv_sem=kv_recv_sem.at[phase, j],
            device_id={"kv": kv_peer(j)},
            device_id_type=pl.DeviceIdType.MESH,
        )
        copy.start()
        sent.append(copy)
        return copy

    def tp_copy(phase, j, src, dst, slot=None):
        return pltpu.make_async_remote_copy(
            src_ref=src,
            dst_ref=dst,
            send_sem=tp_send_sem.at[phase, j],
            recv_sem=tp_recv_sem.at[phase, j if slot is None else slot],
            device_id={"tp": tp_peer(j)},
            device_id_type=pl.DeviceIdType.MESH,
        )

    def to_tp(phase, j, src, dst):
        copy = tp_copy(phase, j, src, dst)
        copy.start()
        sent.append(copy)
        return copy

    P_SQ, P_Q, P_KVG, P_CA, P_OT = 0, 1, 1 + heads, 2 + heads, 2 + 2 * heads
    P_SQM, P_GU, P_HID = 3 + 2 * heads, 4 + 2 * heads, 4 + 2 * heads + len(stages)

    for name in ("tok", "len", "ld", "ag", "wq"):
        loads[name].start()
    loads["tok"].wait()
    pl.semaphore_wait(barrier, n_kv + n_tp - 2)

    tok_copies = [to_tp(0, j, tokens_ref, tok_buf.at[me_tp]) for j in tp_order]
    for name in ("wk", "wv", "wg", "kc", "vc", "gg", "fg"):
        loads[name].start()
    tok_buf[me_tp] = tokens_ref[...]

    for name in ("len", "ld", "ag"):
        loads[name].wait()
    row_id = lax.broadcasted_iota(jnp.int32, (rows, LANES), 0)
    lens = jnp.zeros((rows, LANES), jnp.int32)
    for b in range(rows):
        lens = jnp.where(row_id == b, lengths_ref[b], lens)
    lane = lax.broadcasted_iota(jnp.int32, (rows, half), 1).astype(F32)
    inverse = jnp.exp(lane * (-math.log(ROPE_BASE) / half))
    angles = lens[:, :1].astype(F32) * inverse
    trig[0] = jnp.cos(angles)
    trig[1] = jnp.sin(angles)
    places = rows * span
    col = lax.broadcasted_iota(jnp.int32, (rows, places), 1)
    row = lax.broadcasted_iota(jnp.int32, (rows, places), 0)
    slot = col - row * span
    position = slot + me_kv * span
    gap = lens[:, :1] - position
    live = (slot >= 0) & (slot < span) & (gap > 0)
    gap_f = jnp.where(live, gap, 0).astype(F32)
    for h in range(heads):
        decay_buf[h] = jnp.where(live, jnp.exp(gap_f * log_decay_ref[h]), 0.0)

    def rotate_in(front, back):
        cosine, sine = trig[0], trig[1]
        return front * cosine - back * sine, front * sine + back * cosine

    for copy in tok_copies:
        copy.wait_recv()
    squares = jnp.zeros((rows, 1), F32)
    for c in range(n_tp):
        wide_tok = tok_buf[c].astype(F32)
        squares = squares + jnp.sum(wide_tok * wide_tok, axis=1, keepdims=True)
        cols = pl.ds(c * own_cols, own_cols)
        x_buf[:, cols] = (wide_tok * attn_gain_ref[:, cols]).astype(BF16)
    sq_send[...] = jnp.broadcast_to(squares, (rows, LANES))

    x = x_buf[...]
    loads["wq"].wait()
    q_copies = {}
    sq_copies = None
    for h in range(heads):
        cols = pl.ds(h * DK, DK)
        q_own = jnp.dot(x, wq[:, cols], preferred_element_type=F32)
        q_send[h] = pack(q_own)
        q_full[:, cols] = q_own
        for j in kv_order:
            q_copies[h, j] = to_kv(P_Q + h, j, q_send.at[h], q_recv.at[h, j])
        if sq_copies is None:
            sq_copies = [to_kv(P_SQ, j, sq_send, sq_recv.at[j]) for j in kv_order]
    for name in ("wo", "wfg", "wfu", "wfd"):
        loads[name].start()

    for name in ("wk", "wv", "wg"):
        loads[name].wait()
    kvg_copies = []
    for j in kv_order + (0,):
        cols = pl.ds(pl.multiple_of(kv_peer(j) * DK, DK), DK)
        parts = [
            jnp.dot(x, weight[:, cols], preferred_element_type=F32) for weight in (wk, wv, wg)
        ]
        if j:
            kvg_send[j] = pack(jnp.concatenate(parts, axis=1))
            kvg_copies.append(to_kv(P_KVG, j, kvg_send.at[j], kvg_recv.at[j]))
        else:
            own_kvg = jnp.concatenate(parts, axis=1)

    for copy in sq_copies:
        copy.wait_recv()
    total_sq = sq_send[...]
    for j in range(1, n_kv):
        total_sq = total_sq + sq_recv[j]
    factor = lax.rsqrt(total_sq / D + RMS_EPS)[:, :1]

    loads["kc"].wait()
    loads["vc"].wait()
    ca_copies = {}
    for h in range(heads):
        cols = pl.ds(h * DK, DK)
        for j in kv_order:
            q_copies[h, j].wait_recv()
        query = q_full[:, cols]
        for j in kv_order:
            query = query + unpack(q_recv[h, j])
        query = query * factor
        front, back = rotate_in(query[:, :half], query[:, half:])
        query = jnp.concatenate([front, back], axis=1) * DK ** (-0.5)
        q_full[:, cols] = query
        scores = lax.dot_general(
            query.astype(BF16),
            kc[:, :, cols].reshape(places, DK),
            (((1,), (1,)), ((), ())),
            preferred_element_type=F32,
        )
        mixing = (scores * decay_buf[h]).astype(BF16)
        cached = jnp.dot(mixing, vc[:, :, cols].reshape(places, DK), preferred_element_type=F32)
        ca_own[h] = cached
        ca_send[h] = pack(cached)
        for j in kv_order:
            ca_copies[h, j] = to_kv(P_CA + h, j, ca_send.at[h], ca_recv.at[h, j])

    loads["gg"].wait()
    for copy in kvg_copies:
        copy.wait_recv()
    own_head = pl.ds(pl.multiple_of(me_kv * DK, DK), DK)
    for j in kv_order:
        own_kvg = own_kvg + unpack(kvg_recv[j])
    own_kvg = own_kvg * factor
    new_key, new_value, gate = [own_kvg[:, i * DK : (i + 1) * DK] for i in range(3)]
    front, back = rotate_in(new_key[:, :half], new_key[:, half:])
    query = q_full[:, own_head]
    score = jnp.sum(query[:, :half] * front + query[:, half:] * back, axis=1, keepdims=True)
    gate = gate / (1.0 + jnp.exp(-gate)) * gn_gain_ref[:, own_head]
    ot_buf[me_kv, 0] = pack(score * new_value)
    ot_buf[me_kv, 1] = pack(gate)
    ot_copies = [to_kv(P_OT, j, ot_buf.at[me_kv], ot_buf.at[me_kv]) for j in kv_order]

    loads["wo"].wait()
    for copy in ot_copies:
        copy.wait_recv()
    out_part = None
    for h in range(heads):
        for j in kv_order:
            ca_copies[h, j].wait_recv()
        totals = ca_own[h] + unpack(ot_buf[h, 0])
        for j in kv_order:
            totals = totals + unpack(ca_recv[h, j])
        center = jnp.sum(totals, axis=1, keepdims=True) / DK
        spread = jnp.sum(totals * totals, axis=1, keepdims=True) / DK - center * center
        normed = (totals - center) * lax.rsqrt(spread + GN_EPS)
        x_buf[:, pl.ds(h * DK, DK)] = (unpack(ot_buf[h, 1]) * normed).astype(BF16)
    out_part = jnp.dot(x_buf[...], wo[...], preferred_element_type=F32)
    o_own[...] = out_part
    o_send[...] = pack(out_part)
    o_copy = to_tp(1, 1, o_send, o_recv)
    o_copy.wait_recv()
    chip_sum = o_own[...] + unpack(o_recv[...])
    o_own[...] = chip_sum
    chip_send[...] = pack(chip_sum)
    chips = range(2, n_tp, 2)
    relays = []
    for j in chips:
        for other in (1, 0):
            relays.append(tp_copy(2, j + other, chip_send, chip_recv.at[j // 2], slot=j))

    @pl.when(me_tp % 2 == 1)
    def _():
        for copy in relays:
            copy.start()

    loads["fg"].wait()
    for j in chips:
        relays[j - 2].wait_recv()
    squares = jnp.zeros((rows, 1), F32)
    mixed = o_own[...]
    for j in chips:
        mixed = mixed + unpack(chip_recv[j // 2])
    for c in range(n_tp):
        cols = pl.ds(c * own_cols, own_cols)
        own_mixed = mixed[:, c * own_cols : (c + 1) * own_cols]
        resid = (tok_buf[c].astype(F32) + own_mixed).astype(BF16)
        resid_wide = resid.astype(F32)
        resid_buf[c] = resid_wide
        squares = squares + jnp.sum(resid_wide * resid_wide, axis=1, keepdims=True)
        x_buf[:, cols] = (resid_wide * ffn_gain_ref[:, cols]).astype(BF16)
    sqm_send[...] = jnp.broadcast_to(squares, (rows, LANES))

    x = x_buf[...]
    loads["wfg"].wait()
    loads["wfu"].wait()

    def stage_start(s, index):
        first, count = stages[s]
        begin = first + window_start(index, count, STAGE_TILES, n_kv)
        return pl.multiple_of(begin * LANES, LANES)

    gu_copies = {}
    sqm_copies = None
    for s in range(len(stages)):
        for j in kv_order:
            cols = pl.ds(stage_start(s, kv_peer(j)), win)
            for i, weight in enumerate((wfg, wfu)):
                part = jnp.dot(x, weight[:, cols], preferred_element_type=F32)
                gu_send[s, j, i] = pack(part)
            gu_copies[s, j] = to_kv(P_GU + s, j, gu_send.at[s, j], gu_recv.at[s, j])
        if sqm_copies is None:
            sqm_copies = [to_kv(P_SQM, j, sqm_send, sqm_recv.at[j]) for j in kv_order]
    for s in range(len(stages)):
        cols = pl.ds(stage_start(s, me_kv), win)
        for i, weight in enumerate((wfg, wfu)):
            gu_own[s, i] = jnp.dot(x, weight[:, cols], preferred_element_type=F32)

    for copy in sqm_copies:
        copy.wait_recv()
    total_sq = sqm_send[...]
    for j in range(1, n_kv):
        total_sq = total_sq + sqm_recv[j]
    factor = lax.rsqrt(total_sq / D + RMS_EPS)[:, :1]
    hid_copies = {}
    for s in range(len(stages)):
        for j in kv_order:
            gu_copies[s, j].wait_recv()
        both = []
        for i in range(2):
            total = gu_own[s, i]
            for j in kv_order:
                total = total + unpack(gu_recv[s, j, i])
            both.append(total * factor)
        gate, up = both
        hidden = gate / (1.0 + jnp.exp(-gate)) * up
        first, count = stages[s]
        if count < STAGE_TILES * n_kv:
            here, after = stage_start(s, me_kv), stage_start(s, me_kv + 1)
            kept = jnp.where(me_kv == n_kv - 1, win, after - here)
            column = lax.broadcasted_iota(jnp.int32, (rows, win), 1)
            hidden = jnp.where(column < kept, hidden, 0.0)
        hid_buf[s, 0] = pack(hidden)
        for j in kv_order:
            hid_copies[s, j] = to_kv(P_HID + s, j, hid_buf.at[s, 0], hid_buf.at[s, j])

    loads["wfd"].wait()

    def down_of(s, j):
        weight = wfd[pl.ds(stage_start(s, kv_peer(j)), win), :]
        chunk = unpack(hid_buf[s, j]).astype(BF16)
        return jnp.dot(chunk, weight, preferred_element_type=F32)

    down = down_of(0, 0)
    for s in range(1, len(stages)):
        down = down + down_of(s, 0)
    for s in range(len(stages)):
        for j in range(1, n_kv):
            hid_copies[s, j].wait_recv()
            down = down + down_of(s, j)
    down_buf[...] = down
    d_copies = {}
    for j in tp_order:
        cols = pl.ds(pl.multiple_of(tp_peer(j) * own_cols, own_cols), own_cols)
        d_send[j] = pack(down_buf[:, cols])
        d_copies[j] = to_tp(3, j, d_send.at[j], d_recv.at[j])
    own = pl.ds(pl.multiple_of(me_tp * own_cols, own_cols), own_cols)
    result = down_buf[:, own] + resid_buf[me_tp]
    for j in range(1, n_tp):
        d_copies[j].wait_recv()
        result = result + unpack(d_recv[j])
    out_ref[...] = result.astype(BF16)
    for copy in sent:
        copy.wait_send()

    @pl.when(me_tp % 2 == 1)
    def _():
        for copy in relays:
            copy.wait_send()


def fused(
    n_kv,
    n_tp,
    tokens,
    lengths,
    attn_gain,
    w_query,
    w_key,
    w_value,
    w_gate,
    log_decay,
    key_cache,
    value_cache,
    gn_gain,
    w_out,
    ffn_gain,
    w_ffn_gate,
    w_ffn_up,
    w_ffn_down,
):
    rows, own_cols = tokens.shape
    depth, wide = w_query.shape
    span = key_cache.shape[1]
    heads = log_decay.shape[0]
    win = STAGE_TILES * LANES
    n_stage = len(stage_spans(w_ffn_gate.shape[1] // LANES, n_kv))
    vmem = pl.BlockSpec(memory_space=pltpu.VMEM)
    hbm = pl.BlockSpec(memory_space=pl.ANY)
    small = (
        tokens,
        lengths,
        attn_gain[None, :],
        log_decay,
        gn_gain[None, :],
        ffn_gain[None, :],
    )
    streamed = (
        w_query,
        w_key,
        w_value,
        w_gate,
        key_cache,
        value_cache,
        w_out,
        w_ffn_gate,
        w_ffn_up,
        w_ffn_down,
    )
    kv_phases = 4 + 2 * heads + 2 * n_stage
    scratch = [pltpu.VMEM(a.shape, a.dtype) for a in streamed] + [
        (pltpu.SMEM if a.ndim == 1 else pltpu.VMEM)(a.shape, a.dtype) for a in small
    ]
    scratch += [
        pltpu.VMEM((n_tp, rows, own_cols), BF16),
        pltpu.VMEM((rows, depth), BF16),
        pltpu.VMEM((rows, LANES), F32),
        pltpu.VMEM((n_kv, rows, LANES), F32),
        pltpu.VMEM((heads, 2 * rows, DK // 2), BF16),
        pltpu.VMEM((heads, n_kv, 2 * rows, DK // 2), BF16),
        pltpu.VMEM((rows, wide), F32),
        pltpu.VMEM((2, rows, DK // 2), F32),
        pltpu.VMEM((heads, rows, rows * span), F32),
        pltpu.VMEM((n_kv, 2 * rows, 3 * DK // 2), BF16),
        pltpu.VMEM((n_kv, 2 * rows, 3 * DK // 2), BF16),
        pltpu.VMEM((heads, rows, DK), F32),
        pltpu.VMEM((heads, 2 * rows, DK // 2), BF16),
        pltpu.VMEM((heads, n_kv, 2 * rows, DK // 2), BF16),
        pltpu.VMEM((n_kv, 2, 2 * rows, DK // 2), BF16),
        pltpu.VMEM((rows, depth), F32),
        pltpu.VMEM((2 * rows, depth // 2), BF16),
        pltpu.VMEM((2 * rows, depth // 2), BF16),
        pltpu.VMEM((2 * rows, depth // 2), BF16),
        pltpu.VMEM((n_tp // 2, 2 * rows, depth // 2), BF16),
        pltpu.VMEM((n_tp, rows, own_cols), F32),
        pltpu.VMEM((rows, LANES), F32),
        pltpu.VMEM((n_kv, rows, LANES), F32),
        pltpu.VMEM((n_stage, 2, rows, win), F32),
        pltpu.VMEM((n_stage, n_kv, 2, 2 * rows, win // 2), BF16),
        pltpu.VMEM((n_stage, n_kv, 2, 2 * rows, win // 2), BF16),
        pltpu.VMEM((n_stage, n_kv, 2 * rows, win // 2), BF16),
        pltpu.VMEM((rows, depth), F32),
        pltpu.VMEM((n_tp, 2 * rows, own_cols // 2), BF16),
        pltpu.VMEM((n_tp, 2 * rows, own_cols // 2), BF16),
        pltpu.SemaphoreType.DMA((len(small) + len(streamed),)),
        pltpu.SemaphoreType.DMA((kv_phases, n_kv)),
        pltpu.SemaphoreType.DMA((kv_phases, n_kv)),
        pltpu.SemaphoreType.DMA((4, n_tp)),
        pltpu.SemaphoreType.DMA((4, n_tp)),
    ]
    return pl.pallas_call(
        functools.partial(layer_kernel, n_kv, n_tp),
        out_shape=pltpu.VMEM((rows, own_cols), BF16),
        in_specs=[hbm] * (len(small) + len(streamed)),
        out_specs=vmem,
        scratch_shapes=scratch,
        compiler_params=pltpu.CompilerParams(
            collective_id=0, has_side_effects=True, vmem_limit_bytes=60 * 1024 * 1024
        ),
    )(*small, *streamed)


def fits(mesh, tokens, log_decay, key_cache, w_query, w_ffn_gate):
    n_kv, n_tp, n_grp = mesh.shape["kv"], mesh.shape["tp"], mesh.shape["grp"]
    heads, span = log_decay.shape[0], key_cache.shape[1] // n_kv
    tiles = w_ffn_gate.shape[1] // n_tp // LANES
    return (
        n_kv > 1
        and n_tp > 2
        and n_kv & (n_kv - 1) == 0
        and n_tp & (n_tp - 1) == 0
        and heads == n_kv * n_tp
        and tokens.shape[1] // n_kv == heads * DK // n_tp
        and tokens.shape[1] % (n_kv * n_tp * 2 * LANES) == 0
        and heads * DK // n_tp % (4 * LANES) == 0
        and w_ffn_gate.shape[1] % (n_tp * LANES) == 0
        and stage_spans(tiles, n_kv)[-1][1] >= STAGE_TILES
        and tokens.shape[0] // n_grp % 8 == 0
        and span % 16 == 0
        and span <= 64
    )


def solution(mesh):
    specs = (
        P("grp", ("kv", "tp")),
        P("grp"),
        P("kv"),
        P("kv", "tp"),
        P("kv", "tp"),
        P("kv", "tp"),
        P("kv", "tp"),
        P("tp"),
        P("grp", "kv", "tp"),
        P("grp", "kv", "tp"),
        P("tp"),
        P("tp", "kv"),
        P("kv"),
        P("kv", "tp"),
        P("kv", "tp"),
        P("tp", "kv"),
    )

    def whole(*arrays):
        tokens, w_query, log_decay, key_cache = arrays[0], arrays[3], arrays[7], arrays[8]
        if fits(mesh, tokens, log_decay, key_cache, w_query, arrays[13]):
            body = functools.partial(fused, mesh.shape["kv"], mesh.shape["tp"])
        else:
            body = local
        return jax.shard_map(
            body,
            mesh=mesh,
            in_specs=specs,
            out_specs=P("grp", ("kv", "tp")),
            check_vma=False,
        )(*arrays)

    return whole
```

```python
import functools
import math

import jax
import jax.numpy as jnp
from jax import lax
from jax.experimental import pallas as pl
from jax.experimental.pallas import tpu as pltpu
from jax.sharding import PartitionSpec as P

DK = 256
D = 4096


RMS_EPS = 0.1
GN_EPS = 1.0
ROPE_BASE = 10000.0


def rotate(vectors, positions):
    half_dim = vectors.shape[-1] // 2
    inverse = ROPE_BASE ** (-jnp.arange(half_dim, dtype=jnp.float32) / half_dim)
    angles = positions[:, None, None] * inverse[None, None, :]
    cosine = jnp.cos(angles)
    sine_part = jnp.sin(angles)
    front_part = vectors[..., :half_dim]
    back_part = vectors[..., half_dim:]
    return jnp.concatenate(
        [front_part * cosine - back_part * sine_part, front_part * sine_part + back_part * cosine],
        axis=-1,
    )


def group_norm(totals, gn_gain):
    width = totals.shape[-1]
    center = jnp.sum(totals, axis=-1, keepdims=True) / width
    spread = jnp.sum(totals * totals, axis=-1, keepdims=True) / width - center * center
    normed = (totals - center) * lax.rsqrt(spread + GN_EPS)
    return normed.reshape(normed.shape[0], -1) * gn_gain


def channel_stat(own_squares):
    return lax.psum(own_squares, "kv")


def input_stat(own_squares):
    return lax.psum(own_squares, "kv")


def cache_partial(query_low, lengths, log_decay, key_cache, value_cache, heads_here):
    batch_rows = query_low.shape[0]
    span = key_cache.shape[1]
    slots = lax.axis_index("kv") * span + jnp.arange(span, dtype=jnp.int32)
    live = slots[None, :] < lengths[:, None]
    gaps = jnp.maximum((lengths[:, None] - slots[None, :]).astype(jnp.float32), 0.0)
    decays = jnp.exp(log_decay[None, None, :] * gaps[:, :, None])
    keys_here = key_cache.reshape(batch_rows, span, heads_here, DK)
    values_here = value_cache.reshape(batch_rows, span, heads_here, DK)
    scores = jnp.einsum("bphd,bhd->bph", keys_here, query_low, preferred_element_type=jnp.float32)
    mixing = jnp.where(live[:, :, None], scores * decays, 0.0).astype(jnp.bfloat16)
    return jnp.einsum("bph,bphd->bhd", mixing, values_here, preferred_element_type=jnp.float32)


def local(
    tokens,
    lengths,
    attn_gain,
    w_query,
    w_key,
    w_value,
    w_gate,
    log_decay,
    key_cache,
    value_cache,
    gn_gain,
    w_out,
    ffn_gain,
    w_ffn_gate,
    w_ffn_up,
    w_ffn_down,
):
    batch_rows = tokens.shape[0]
    heads_here = log_decay.shape[0]
    row_block = lax.all_gather(tokens, "tp", axis=1, tiled=True)
    widened = row_block.astype(jnp.float32)
    own_squares = jnp.sum(widened * widened, axis=1)
    scaled = (widened * attn_gain).astype(jnp.bfloat16)
    part_query = jnp.dot(scaled, w_query, preferred_element_type=jnp.float32)
    part_key = jnp.dot(scaled, w_key, preferred_element_type=jnp.float32)
    part_value = jnp.dot(scaled, w_value, preferred_element_type=jnp.float32)
    part_gate = jnp.dot(scaled, w_gate, preferred_element_type=jnp.float32)
    positions = lengths.astype(jnp.float32)
    total_squares = input_stat(own_squares)
    queries, new_keys, new_values, gates = lax.psum(
        (part_query, part_key, part_value, part_gate), "kv"
    )
    factor = lax.rsqrt(total_squares / D + RMS_EPS)[:, None]
    queries = rotate((queries * factor).reshape(batch_rows, heads_here, DK), positions) * DK ** (
        -0.5
    )
    new_keys = rotate((new_keys * factor).reshape(batch_rows, heads_here, DK), positions)
    new_values = (new_values * factor).reshape(batch_rows, heads_here, DK)
    gates = gates * factor
    query_low = queries.astype(jnp.bfloat16)
    partial_value = cache_partial(query_low, lengths, log_decay, key_cache, value_cache, heads_here)
    cached = lax.psum(partial_value.reshape(batch_rows, heads_here * DK), "kv")
    own_term = jnp.sum(queries * new_keys, axis=-1, keepdims=True) * new_values
    normed = group_norm(cached.reshape(batch_rows, heads_here, DK) + own_term, gn_gain)
    gated = (jax.nn.silu(gates) * normed).astype(jnp.bfloat16)
    out_partial = jnp.dot(gated, w_out, preferred_element_type=jnp.float32)
    mixed = lax.psum_scatter(out_partial, "tp", scatter_dimension=1, tiled=True)
    resid = (tokens.astype(jnp.float32) + mixed).astype(jnp.bfloat16)
    resid_block = lax.all_gather(resid, "tp", axis=1, tiled=True).astype(jnp.float32)
    mid_squares = jnp.sum(resid_block * resid_block, axis=1)
    scaled_mid = (resid_block * ffn_gain).astype(jnp.bfloat16)
    gate_part = jnp.dot(scaled_mid, w_ffn_gate, preferred_element_type=jnp.float32)
    up_part = jnp.dot(scaled_mid, w_ffn_up, preferred_element_type=jnp.float32)
    total_mid = channel_stat(mid_squares)
    gate_sum, up_sum = lax.psum((gate_part, up_part), "kv")
    factor_mid = lax.rsqrt(total_mid / D + RMS_EPS)[:, None]
    hidden = (jax.nn.silu(gate_sum * factor_mid) * (up_sum * factor_mid)).astype(jnp.bfloat16)
    down_partial = jnp.dot(hidden, w_ffn_down, preferred_element_type=jnp.float32)
    down = lax.psum_scatter(down_partial, "tp", scatter_dimension=1, tiled=True)
    return (resid.astype(jnp.float32) + down).astype(jnp.bfloat16)


LANES = 128
STAGE_TILES = 2
F32 = jnp.float32
BF16 = jnp.bfloat16


def window_start(index, tiles, width, parts):
    return (index * (tiles - width) + (parts - 1) // 2) // (parts - 1)


def partner(index, j, parts):
    found, bit = 0, 1
    while bit < parts:
        digit = (index // bit) % 2
        found = found + bit * ((1 - digit) if (j // bit) % 2 else digit)
        bit *= 2
    return found


def pack(value):
    middle = value.shape[1] // 2
    return jnp.concatenate([value[:, :middle], value[:, middle:]], axis=0).astype(BF16)


def unpack(packed):
    wide = packed.astype(F32)
    rows = wide.shape[0] // 2
    return jnp.concatenate([wide[:rows], wide[rows:]], axis=1)


def stage_spans(tiles, n_kv):
    step = STAGE_TILES * n_kv
    return [(first, min(step, tiles - first)) for first in range(0, tiles, step)]


def layer_kernel(
    n_kv,
    n_tp,
    tokens_hbm,
    lengths_hbm,
    attn_gain_hbm,
    log_decay_hbm,
    gn_gain_hbm,
    ffn_gain_hbm,
    wq_hbm,
    wk_hbm,
    wv_hbm,
    wg_hbm,
    kc_hbm,
    vc_hbm,
    wo_hbm,
    wfg_hbm,
    wfu_hbm,
    wfd_hbm,
    out_ref,
    wq,
    wk,
    wv,
    wg,
    kc,
    vc,
    wo,
    wfg,
    wfu,
    wfd,
    tokens_ref,
    lengths_ref,
    attn_gain_ref,
    log_decay_ref,
    gn_gain_ref,
    ffn_gain_ref,
    tok_buf,
    x_buf,
    sq_send,
    sq_recv,
    q_send,
    q_recv,
    q_full,
    trig,
    decay_buf,
    key_own,
    vg_send,
    vg_in,
    ca_send,
    ca_in,
    sc_send,
    sc_in,
    gt_send,
    gt_buf,
    o_buf,
    resid_buf,
    sqm_send,
    sqm_recv,
    gu_own,
    gu_send,
    gu_recv,
    hid_buf,
    down_buf,
    d_send,
    d_recv,
    load_sem,
    kv_send_sem,
    kv_recv_sem,
    tp_send_sem,
    tp_recv_sem,
    own_send_sem,
    own_recv_sem,
    gt_send_sem,
    gt_recv_sem,
):
    rows, own_cols = tokens_ref.shape
    depth, wide = wq.shape
    span = kc.shape[1]
    half = DK // 2
    tiles = wfg.shape[1] // LANES
    win = STAGE_TILES * LANES
    stages = stage_spans(tiles, n_kv)
    heads = n_kv
    middle = n_kv // 2 - 1
    shared = heads // 2
    me_kv = lax.axis_index("kv")
    me_tp = lax.axis_index("tp")
    me_core = me_tp % 2
    first_core = me_tp - me_core
    is_owner = (me_core == 1) & (me_kv >= middle) & (me_kv < middle + 2)

    def kv_peer(j):
        return partner(me_kv, j, n_kv)

    def tp_peer(j):
        return partner(me_tp, j, n_tp)

    kv_order = tuple(range(n_kv - 1, 0, -1))
    tp_order = tuple(range(n_tp - 1, 0, -1))

    barrier = pltpu.get_barrier_semaphore()
    for j in range(1, n_kv):
        pl.semaphore_signal(
            barrier, inc=1, device_id={"kv": kv_peer(j)}, device_id_type=pl.DeviceIdType.MESH
        )
        pl.semaphore_signal(
            barrier,
            inc=1,
            device_id={"kv": kv_peer(j), "tp": tp_peer(1)},
            device_id_type=pl.DeviceIdType.MESH,
        )
    for j in range(1, n_tp):
        pl.semaphore_signal(
            barrier, inc=1, device_id={"tp": tp_peer(j)}, device_id_type=pl.DeviceIdType.MESH
        )

    loads = {}
    for slot, (name, src, dst) in enumerate(
        (
            ("tok", tokens_hbm, tokens_ref),
            ("len", lengths_hbm, lengths_ref),
            ("ag", attn_gain_hbm, attn_gain_ref),
            ("ld", log_decay_hbm, log_decay_ref),
            ("gg", gn_gain_hbm, gn_gain_ref),
            ("fg", ffn_gain_hbm, ffn_gain_ref),
            ("wq", wq_hbm, wq),
            ("kc", kc_hbm, kc),
            ("vc", vc_hbm, vc),
            ("wk", wk_hbm, wk),
            ("wv", wv_hbm, wv),
            ("wg", wg_hbm, wg),
            ("wo", wo_hbm, wo),
            ("wfg", wfg_hbm, wfg),
            ("wfu", wfu_hbm, wfu),
            ("wfd", wfd_hbm, wfd),
        )
    ):
        loads[name] = pltpu.make_async_copy(src, dst, load_sem.at[slot])

    sent = []

    def to_kv(phase, j, src, dst):
        copy = pltpu.make_async_remote_copy(
            src_ref=src,
            dst_ref=dst,
            send_sem=kv_send_sem.at[phase, j],
            recv_sem=kv_recv_sem.at[phase, j],
            device_id={"kv": kv_peer(j)},
            device_id_type=pl.DeviceIdType.MESH,
        )
        copy.start()
        sent.append(copy)
        return copy

    def tp_waiter(phase, j, ref):
        return pltpu.make_async_remote_copy(
            src_ref=ref,
            dst_ref=ref,
            send_sem=tp_send_sem.at[phase, j],
            recv_sem=tp_recv_sem.at[phase, tp_peer(j)],
            device_id={"tp": tp_peer(j)},
            device_id_type=pl.DeviceIdType.MESH,
        )

    def tp_target(place):
        chip, core = place
        return partner(first_core, 2 * chip, n_tp) + core

    far = [(chip, core) for chip in range(n_tp // 2 - 1, 0, -1) for core in (0, 1)]

    def to_tp(phase, src_of, dst):
        def send(target, slot):
            copy = pltpu.make_async_remote_copy(
                src_ref=src_of(target),
                dst_ref=dst,
                send_sem=tp_send_sem.at[phase, slot],
                recv_sem=tp_recv_sem.at[phase, me_tp],
                device_id={"tp": target},
                device_id_type=pl.DeviceIdType.MESH,
            )
            copy.start()
            sent.append(copy)

        for slot, place in enumerate(far):
            send(tp_target(place), slot)
        send(tp_peer(1), len(far))

    def owner_copy(kind, h, src, dst):
        slot = own_send_sem.at[kind, h]
        return pltpu.make_async_remote_copy(
            src_ref=src,
            dst_ref=dst,
            send_sem=slot,
            recv_sem=own_recv_sem.at[kind, me_core, me_kv, h % shared],
            device_id={"kv": middle + h // shared, "tp": first_core + 1},
            device_id_type=pl.DeviceIdType.MESH,
        )

    def owns(h):
        return (me_core == 1) & (me_kv == middle + h // shared)

    def to_owner(pairs):
        for h, copies in pairs:

            @pl.when(jnp.logical_not(owns(h)))
            def _():
                for copy in copies:
                    copy.start()

            to_owners.append((h, copies))

    to_owners = []
    VG, CA, SC = 0, 1, 2

    def column_tile(columns):
        lane_id = lax.broadcasted_iota(jnp.int32, (8, LANES), 1)
        tile = jnp.zeros((8, LANES), F32)
        groups = rows // 8
        for i, column in enumerate(columns):
            for r in range(groups):
                part = jnp.broadcast_to(column[r * 8 : (r + 1) * 8], (8, LANES))
                tile = jnp.where(lane_id == i * groups + r, part, tile)
        return tile

    def tile_column(tile, i):
        groups = rows // 8
        return jnp.concatenate(
            [tile[:, i * groups + r : i * groups + r + 1] for r in range(groups)], axis=0
        )

    P_SQ, P_Q = 0, 1
    P_SQM, P_GU, P_HID = 1 + heads, 2 + heads, 2 + heads + len(stages)

    for name in ("tok", "len", "ld", "ag", "wq"):
        loads[name].start()
    loads["tok"].wait()
    pl.semaphore_wait(barrier, 2 * (n_kv - 1) + n_tp - 1)

    to_tp(0, lambda target: tokens_ref, tok_buf.at[me_tp])
    for name in ("wk", "wv", "wg", "kc", "vc", "gg", "fg"):
        loads[name].start()
    tok_buf[me_tp] = tokens_ref[...]

    for name in ("len", "ld", "ag"):
        loads[name].wait()
    row_id = lax.broadcasted_iota(jnp.int32, (rows, LANES), 0)
    lens = jnp.zeros((rows, LANES), jnp.int32)
    for b in range(rows):
        lens = jnp.where(row_id == b, lengths_ref[b], lens)
    lane = lax.broadcasted_iota(jnp.int32, (rows, half), 1).astype(F32)
    inverse = jnp.exp(lane * (-math.log(ROPE_BASE) / half))
    angles = lens[:, :1].astype(F32) * inverse
    trig[0] = jnp.cos(angles)
    trig[1] = jnp.sin(angles)
    places = rows * span
    col = lax.broadcasted_iota(jnp.int32, (rows, places), 1)
    row = lax.broadcasted_iota(jnp.int32, (rows, places), 0)
    slot = col - row * span
    position = slot + me_kv * span
    gap = lens[:, :1] - position
    live = (slot >= 0) & (slot < span) & (gap > 0)
    gap_f = jnp.where(live, gap, 0).astype(F32)
    for h in range(heads):
        decay_buf[h] = jnp.where(live, jnp.exp(gap_f * log_decay_ref[h]), 0.0)

    def rotate_in(front, back):
        cosine, sine = trig[0], trig[1]
        return front * cosine - back * sine, front * sine + back * cosine

    for j in tp_order:
        tp_waiter(0, j, tokens_ref).wait_recv()
    squares = jnp.zeros((rows, 1), F32)
    for c in range(n_tp):
        wide_tok = tok_buf[c].astype(F32)
        squares = squares + jnp.sum(wide_tok * wide_tok, axis=1, keepdims=True)
        cols = pl.ds(c * own_cols, own_cols)
        x_buf[:, cols] = (wide_tok * attn_gain_ref[:, cols]).astype(BF16)
    sq_send[...] = column_tile([squares])
    sq_copies = [to_kv(P_SQ, j, sq_send, sq_recv.at[j]) for j in kv_order]

    x = x_buf[...]
    loads["wq"].wait()
    q_copies = {}
    for pair in range(heads // 2):
        q_own = jnp.dot(x, wq[:, pl.ds(pair * 2 * DK, 2 * DK)], preferred_element_type=F32)
        for i in range(2):
            h = pair * 2 + i
            piece = q_own[:, i * DK : (i + 1) * DK]
            q_send[h] = pack(piece)
            q_full[:, pl.ds(h * DK, DK)] = piece
            for j in kv_order:
                q_copies[h, j] = to_kv(P_Q + h, j, q_send.at[h], q_recv.at[h, j])
    for name in ("wo", "wfg", "wfu", "wfd"):
        loads[name].start()

    for name in ("wk", "wv", "wg"):
        loads[name].wait()
    for i, weight in enumerate((wv, wg)):
        for pair in range(heads // 2):
            part = jnp.dot(x, weight[:, pl.ds(pair * 2 * DK, 2 * DK)], preferred_element_type=F32)
            for k in range(2):
                vg_send[pair * 2 + k, i] = pack(part[:, k * DK : (k + 1) * DK])
    key_own[...] = jnp.dot(x, wk[...], preferred_element_type=F32)

    for copy in sq_copies:
        copy.wait_recv()
    total_sq = sq_send[...]
    for j in range(1, n_kv):
        total_sq = total_sq + sq_recv[j]
    factor = lax.rsqrt(tile_column(total_sq, 0) / D + RMS_EPS)

    loads["kc"].wait()
    loads["vc"].wait()
    own_scores = []
    for h in range(heads):
        cols = pl.ds(h * DK, DK)
        for j in kv_order:
            q_copies[h, j].wait_recv()
        query = q_full[:, cols]
        for j in kv_order:
            query = query + unpack(q_recv[h, j])
        query = query * factor
        front, back = rotate_in(query[:, :half], query[:, half:])
        query = jnp.concatenate([front, back], axis=1) * DK ** (-0.5)
        scores = lax.dot_general(
            query.astype(BF16),
            kc[:, :, cols].reshape(places, DK),
            (((1,), (1,)), ((), ())),
            preferred_element_type=F32,
        )
        mixing = (scores * decay_buf[h]).astype(BF16)
        cached = jnp.dot(mixing, vc[:, :, cols].reshape(places, DK), preferred_element_type=F32)
        ca_send[h] = pack(cached)
        key = key_own[:, cols]
        front, back = rotate_in(key[:, :half], key[:, half:])
        own_scores.append(
            jnp.sum(query[:, :half] * front + query[:, half:] * back, axis=1, keepdims=True)
            * factor
        )
        pairs = [(h, [owner_copy(CA, h, ca_send.at[h], ca_in.at[me_core, me_kv, h % shared])])]
        if h % shared == shared - 1:
            oi = h // shared
            sc_send[oi] = column_tile(own_scores[oi * shared :])
            pairs[0][1].append(owner_copy(SC, oi * shared, sc_send.at[oi], sc_in.at[me_core, me_kv]))
        to_owner(pairs)
        if h == 0:
            to_owner(
                [
                    (
                        g,
                        [
                            owner_copy(
                                VG, g, vg_send.at[g], vg_in.at[me_core, me_kv, g % shared]
                            )
                        ],
                    )
                    for g in range(heads)
                ]
            )

    def owned(c, kind, hh, j, ref):
        at = me_kv if j == 0 else kv_peer(j)
        return pltpu.make_async_remote_copy(
            src_ref=ref,
            dst_ref=ref,
            send_sem=own_send_sem.at[kind, 0],
            recv_sem=own_recv_sem.at[kind, c, at, hh],
            device_id={"kv": kv_peer(1)},
            device_id_type=pl.DeviceIdType.MESH,
        )

    def gt_copies(c, hh, head):
        peers = kv_order + ((0,) if c == 0 else ())
        return [
            pltpu.make_async_remote_copy(
                src_ref=gt_send.at[c, hh],
                dst_ref=gt_buf.at[head],
                send_sem=gt_send_sem.at[c, hh, j],
                recv_sem=gt_recv_sem.at[head],
                device_id={"kv": me_kv if j == 0 else kv_peer(j), "tp": first_core + c},
                device_id_type=pl.DeviceIdType.MESH,
            )
            for j in peers
        ]

    @pl.when(is_owner)
    def _():
        base = (me_kv - middle) * shared
        units = [(c, hh) for c in (1, 0) for hh in range(shared)]
        for c, hh in units:
            for j in kv_order + ((0,) if c == 0 else ()):
                owned(c, VG, hh, j, vg_in.at[0, 0, 0]).wait_recv()
        gates, news = {}, {}
        for c, hh in units:
            if c:
                both = [unpack(vg_send[base + hh, i]) for i in range(2)]
            else:
                both = [unpack(vg_in[0, me_kv, hh, i]) for i in range(2)]
            for j in kv_order:
                both = [both[i] + unpack(vg_in[c, kv_peer(j), hh, i]) for i in range(2)]
            new_value, gate = both[0] * factor, both[1] * factor
            news[c, hh] = new_value
            gates[c, hh] = gate / (1.0 + jnp.exp(-gate))
        for c in (1, 0):
            for j in kv_order + ((0,) if c == 0 else ()):
                owned(c, SC, 0, j, sc_in.at[0, 0]).wait_recv()
        for c, hh in units:
            for j in kv_order + ((0,) if c == 0 else ()):
                owned(c, CA, hh, j, ca_in.at[0, 0, 0]).wait_recv()
            if c:
                totals = unpack(ca_send[base + hh])
                tile = sc_send[me_kv - middle]
            else:
                totals = unpack(ca_in[0, me_kv, hh])
                tile = sc_in[0, me_kv]
            for j in kv_order:
                totals = totals + unpack(ca_in[c, kv_peer(j), hh])
                tile = tile + sc_in[c, kv_peer(j)]
            totals = totals + tile_column(tile, hh) * news[c, hh]
            center = jnp.sum(totals, axis=1, keepdims=True) / DK
            spread = jnp.sum(totals * totals, axis=1, keepdims=True) / DK - center * center
            normed = (totals - center) * lax.rsqrt(spread + GN_EPS)
            result = pack(gates[c, hh] * normed)
            gt_send[c, hh] = result
            if c:
                gt_buf[base + hh] = result
            for copy in gt_copies(c, hh, base + hh):
                copy.start()

    loads["wo"].wait()
    loads["gg"].wait()
    for h in range(heads):
        waiter = pltpu.make_async_remote_copy(
            src_ref=gt_send.at[0, 0],
            dst_ref=gt_buf.at[h],
            send_sem=gt_send_sem.at[0, 0, 0],
            recv_sem=gt_recv_sem.at[h],
            device_id={"kv": kv_peer(1)},
            device_id_type=pl.DeviceIdType.MESH,
        )

        @pl.when(jnp.logical_not(owns(h)))
        def _():
            waiter.wait_recv()

    for h in range(heads):
        cols = pl.ds(h * DK, DK)
        x_buf[:, cols] = (unpack(gt_buf[h]) * gn_gain_ref[:, cols]).astype(BF16)
    gated = x_buf[...]
    for part in range(2):
        width = depth // 2
        piece = jnp.dot(
            gated, wo[:, pl.ds(part * width, width)], preferred_element_type=F32
        )
        o_buf[part, me_tp] = pack(piece)
        to_tp(1 + part, lambda target: o_buf.at[part, me_tp], o_buf.at[part, me_tp])
    loads["fg"].wait()
    for part in range(2):
        for j in tp_order:
            tp_waiter(1 + part, j, o_buf.at[part, 0]).wait_recv()
    squares = jnp.zeros((rows, 1), F32)
    halves = []
    for part in range(2):
        total = unpack(o_buf[part, 0])
        for t in range(1, n_tp):
            total = total + unpack(o_buf[part, t])
        halves.append(total)
    mixed = jnp.concatenate(halves, axis=1)
    for c in range(n_tp):
        cols = pl.ds(c * own_cols, own_cols)
        own_mixed = mixed[:, c * own_cols : (c + 1) * own_cols]
        resid = (tok_buf[c].astype(F32) + own_mixed).astype(BF16)
        resid_wide = resid.astype(F32)
        resid_buf[c] = resid_wide
        squares = squares + jnp.sum(resid_wide * resid_wide, axis=1, keepdims=True)
        x_buf[:, cols] = (resid_wide * ffn_gain_ref[:, cols]).astype(BF16)
    sqm_send[...] = column_tile([squares])
    sqm_copies = [to_kv(P_SQM, j, sqm_send, sqm_recv.at[j]) for j in kv_order]

    x = x_buf[...]
    loads["wfg"].wait()
    loads["wfu"].wait()

    def stage_start(s, index):
        first, count = stages[s]
        begin = first + window_start(index, count, STAGE_TILES, n_kv)
        return pl.multiple_of(begin * LANES, LANES)

    gu_copies = {}
    for s in range(len(stages)):
        for j in kv_order:
            cols = pl.ds(stage_start(s, kv_peer(j)), win)
            for i, weight in enumerate((wfg, wfu)):
                part = jnp.dot(x, weight[:, cols], preferred_element_type=F32)
                gu_send[s, j, i] = pack(part)
            gu_copies[s, j] = to_kv(P_GU + s, j, gu_send.at[s, j], gu_recv.at[s, j])
    for s in range(len(stages)):
        cols = pl.ds(stage_start(s, me_kv), win)
        for i, weight in enumerate((wfg, wfu)):
            gu_own[s, i] = jnp.dot(x, weight[:, cols], preferred_element_type=F32)

    for copy in sqm_copies:
        copy.wait_recv()
    total_sq = sqm_send[...]
    for j in range(1, n_kv):
        total_sq = total_sq + sqm_recv[j]
    factor = lax.rsqrt(tile_column(total_sq, 0) / D + RMS_EPS)
    hid_copies = {}
    for s in range(len(stages)):
        for j in kv_order:
            gu_copies[s, j].wait_recv()
        both = []
        for i in range(2):
            total = gu_own[s, i]
            for j in kv_order:
                total = total + unpack(gu_recv[s, j, i])
            both.append(total * factor)
        gate, up = both
        hidden = gate / (1.0 + jnp.exp(-gate)) * up
        first, count = stages[s]
        if count < STAGE_TILES * n_kv:
            here, after = stage_start(s, me_kv), stage_start(s, me_kv + 1)
            kept = jnp.where(me_kv == n_kv - 1, win, after - here)
            column = lax.broadcasted_iota(jnp.int32, (rows, win), 1)
            hidden = jnp.where(column < kept, hidden, 0.0)
        hid_buf[s, 0] = pack(hidden)
        for j in kv_order:
            hid_copies[s, j] = to_kv(P_HID + s, j, hid_buf.at[s, 0], hid_buf.at[s, j])

    loads["wfd"].wait()

    def down_of(s, j):
        weight = wfd[pl.ds(stage_start(s, kv_peer(j)), win), :]
        chunk = unpack(hid_buf[s, j]).astype(BF16)
        return jnp.dot(chunk, weight, preferred_element_type=F32)

    down = down_of(0, 0)
    for s in range(1, len(stages)):
        down = down + down_of(s, 0)
    for s in range(len(stages)):
        for j in range(1, n_kv):
            hid_copies[s, j].wait_recv()
            down = down + down_of(s, j)
    down_buf[...] = down
    for t in range(n_tp):
        d_send[t] = pack(down_buf[:, pl.ds(t * own_cols, own_cols)])
    to_tp(3, lambda target: d_send.at[target], d_recv.at[me_tp])
    own = pl.ds(pl.multiple_of(me_tp * own_cols, own_cols), own_cols)
    result = down_buf[:, own] + resid_buf[me_tp]
    for j in range(1, n_tp):
        tp_waiter(3, j, d_recv.at[0]).wait_recv()
        result = result + unpack(d_recv[tp_peer(j)])
    out_ref[...] = result.astype(BF16)
    for copy in sent:
        copy.wait_send()
    for h in range(heads):

        @pl.when(jnp.logical_not(owns(h)))
        def _():
            for head, copies in to_owners:
                if head == h:
                    for copy in copies:
                        copy.wait_send()

    @pl.when(is_owner)
    def _():
        for c in (1, 0):
            for hh in range(shared):
                for copy in gt_copies(c, hh, hh):
                    copy.wait_send()


def fused(
    n_kv,
    n_tp,
    tokens,
    lengths,
    attn_gain,
    w_query,
    w_key,
    w_value,
    w_gate,
    log_decay,
    key_cache,
    value_cache,
    gn_gain,
    w_out,
    ffn_gain,
    w_ffn_gate,
    w_ffn_up,
    w_ffn_down,
):
    rows, own_cols = tokens.shape
    depth, wide = w_query.shape
    span = key_cache.shape[1]
    heads = log_decay.shape[0]
    shared = heads // 2
    win = STAGE_TILES * LANES
    n_stage = len(stage_spans(w_ffn_gate.shape[1] // LANES, n_kv))
    vmem = pl.BlockSpec(memory_space=pltpu.VMEM)
    hbm = pl.BlockSpec(memory_space=pl.ANY)
    small = (
        tokens,
        lengths,
        attn_gain[None, :],
        log_decay,
        gn_gain[None, :],
        ffn_gain[None, :],
    )
    streamed = (
        w_query,
        w_key,
        w_value,
        w_gate,
        key_cache,
        value_cache,
        w_out,
        w_ffn_gate,
        w_ffn_up,
        w_ffn_down,
    )
    kv_phases = 2 + heads + 2 * n_stage
    scratch = [pltpu.VMEM(a.shape, a.dtype) for a in streamed] + [
        (pltpu.SMEM if a.ndim == 1 else pltpu.VMEM)(a.shape, a.dtype) for a in small
    ]
    scratch += [
        pltpu.VMEM((n_tp, rows, own_cols), BF16),
        pltpu.VMEM((rows, depth), BF16),
        pltpu.VMEM((8, LANES), F32),
        pltpu.VMEM((n_kv, 8, LANES), F32),
        pltpu.VMEM((heads, 2 * rows, DK // 2), BF16),
        pltpu.VMEM((heads, n_kv, 2 * rows, DK // 2), BF16),
        pltpu.VMEM((rows, wide), F32),
        pltpu.VMEM((2, rows, DK // 2), F32),
        pltpu.VMEM((heads, rows, rows * span), F32),
        pltpu.VMEM((rows, wide), F32),
        pltpu.VMEM((heads, 2, 2 * rows, DK // 2), BF16),
        pltpu.VMEM((2, n_kv, shared, 2, 2 * rows, DK // 2), BF16),
        pltpu.VMEM((heads, 2 * rows, DK // 2), BF16),
        pltpu.VMEM((2, n_kv, shared, 2 * rows, DK // 2), BF16),
        pltpu.VMEM((2, 8, LANES), F32),
        pltpu.VMEM((2, n_kv, 8, LANES), F32),
        pltpu.VMEM((2, shared, 2 * rows, DK // 2), BF16),
        pltpu.VMEM((heads, 2 * rows, DK // 2), BF16),
        pltpu.VMEM((2, n_tp, 2 * rows, depth // 4), BF16),
        pltpu.VMEM((n_tp, rows, own_cols), F32),
        pltpu.VMEM((8, LANES), F32),
        pltpu.VMEM((n_kv, 8, LANES), F32),
        pltpu.VMEM((n_stage, 2, rows, win), F32),
        pltpu.VMEM((n_stage, n_kv, 2, 2 * rows, win // 2), BF16),
        pltpu.VMEM((n_stage, n_kv, 2, 2 * rows, win // 2), BF16),
        pltpu.VMEM((n_stage, n_kv, 2 * rows, win // 2), BF16),
        pltpu.VMEM((rows, depth), F32),
        pltpu.VMEM((n_tp, 2 * rows, own_cols // 2), BF16),
        pltpu.VMEM((n_tp, 2 * rows, own_cols // 2), BF16),
        pltpu.SemaphoreType.DMA((len(small) + len(streamed),)),
        pltpu.SemaphoreType.DMA((kv_phases, n_kv)),
        pltpu.SemaphoreType.DMA((kv_phases, n_kv)),
        pltpu.SemaphoreType.DMA((4, n_tp)),
        pltpu.SemaphoreType.DMA((4, n_tp)),
        pltpu.SemaphoreType.DMA((3, heads)),
        pltpu.SemaphoreType.DMA((3, 2, n_kv, shared)),
        pltpu.SemaphoreType.DMA((2, shared, n_kv)),
        pltpu.SemaphoreType.DMA((heads,)),
    ]
    return pl.pallas_call(
        functools.partial(layer_kernel, n_kv, n_tp),
        out_shape=pltpu.VMEM((rows, own_cols), BF16),
        in_specs=[hbm] * (len(small) + len(streamed)),
        out_specs=vmem,
        scratch_shapes=scratch,
        compiler_params=pltpu.CompilerParams(
            collective_id=0, has_side_effects=True, vmem_limit_bytes=60 * 1024 * 1024
        ),
    )(*small, *streamed)


def fits(mesh, tokens, log_decay, key_cache, w_query, w_ffn_gate):
    n_kv, n_tp, n_grp = mesh.shape["kv"], mesh.shape["tp"], mesh.shape["grp"]
    heads, span = log_decay.shape[0], key_cache.shape[1] // n_kv
    tiles = w_ffn_gate.shape[1] // n_tp // LANES
    rows = tokens.shape[0] // n_grp
    return (
        n_kv > 1
        and n_tp > 2
        and n_kv & (n_kv - 1) == 0
        and n_tp & (n_tp - 1) == 0
        and heads == n_kv * n_tp
        and heads // n_tp * (rows // 8) <= 2 * LANES
        and tokens.shape[1] // n_kv == heads * DK // n_tp
        and tokens.shape[1] % (n_kv * n_tp * 2 * LANES) == 0
        and heads * DK // n_tp % (4 * LANES) == 0
        and w_ffn_gate.shape[1] % (n_tp * LANES) == 0
        and stage_spans(tiles, n_kv)[-1][1] >= STAGE_TILES
        and tokens.shape[0] // n_grp % 8 == 0
        and span % 16 == 0
        and span <= 64
    )


def solution(mesh):
    specs = (
        P("grp", ("kv", "tp")),
        P("grp"),
        P("kv"),
        P("kv", "tp"),
        P("kv", "tp"),
        P("kv", "tp"),
        P("kv", "tp"),
        P("tp"),
        P("grp", "kv", "tp"),
        P("grp", "kv", "tp"),
        P("tp"),
        P("tp", "kv"),
        P("kv"),
        P("kv", "tp"),
        P("kv", "tp"),
        P("tp", "kv"),
    )

    def whole(*arrays):
        tokens, w_query, log_decay, key_cache = arrays[0], arrays[3], arrays[7], arrays[8]
        if fits(mesh, tokens, log_decay, key_cache, w_query, arrays[13]):
            body = functools.partial(fused, mesh.shape["kv"], mesh.shape["tp"])
        else:
            body = local
        return jax.shard_map(
            body,
            mesh=mesh,
            in_specs=specs,
            out_specs=P("grp", ("kv", "tp")),
            check_vma=False,
        )(*arrays)

    return whole
```

```python
import functools
import math

import jax
import jax.numpy as jnp
from jax import lax
from jax.experimental import pallas as pl
from jax.experimental.pallas import tpu as pltpu
from jax.sharding import PartitionSpec as P

DK = 256
D = 4096


RMS_EPS = 0.1
GN_EPS = 1.0
ROPE_BASE = 10000.0


def rotate(vectors, positions):
    half_dim = vectors.shape[-1] // 2
    inverse = ROPE_BASE ** (-jnp.arange(half_dim, dtype=jnp.float32) / half_dim)
    angles = positions[:, None, None] * inverse[None, None, :]
    cosine = jnp.cos(angles)
    sine_part = jnp.sin(angles)
    front_part = vectors[..., :half_dim]
    back_part = vectors[..., half_dim:]
    return jnp.concatenate(
        [front_part * cosine - back_part * sine_part, front_part * sine_part + back_part * cosine],
        axis=-1,
    )


def group_norm(totals, gn_gain):
    width = totals.shape[-1]
    center = jnp.sum(totals, axis=-1, keepdims=True) / width
    spread = jnp.sum(totals * totals, axis=-1, keepdims=True) / width - center * center
    normed = (totals - center) * lax.rsqrt(spread + GN_EPS)
    return normed.reshape(normed.shape[0], -1) * gn_gain


def channel_stat(own_squares):
    return lax.psum(own_squares, "kv")


def input_stat(own_squares):
    return lax.psum(own_squares, "kv")


def cache_partial(query_low, lengths, log_decay, key_cache, value_cache, heads_here):
    batch_rows = query_low.shape[0]
    span = key_cache.shape[1]
    slots = lax.axis_index("kv") * span + jnp.arange(span, dtype=jnp.int32)
    live = slots[None, :] < lengths[:, None]
    gaps = jnp.maximum((lengths[:, None] - slots[None, :]).astype(jnp.float32), 0.0)
    decays = jnp.exp(log_decay[None, None, :] * gaps[:, :, None])
    keys_here = key_cache.reshape(batch_rows, span, heads_here, DK)
    values_here = value_cache.reshape(batch_rows, span, heads_here, DK)
    scores = jnp.einsum("bphd,bhd->bph", keys_here, query_low, preferred_element_type=jnp.float32)
    mixing = jnp.where(live[:, :, None], scores * decays, 0.0).astype(jnp.bfloat16)
    return jnp.einsum("bph,bphd->bhd", mixing, values_here, preferred_element_type=jnp.float32)


def local(
    tokens,
    lengths,
    attn_gain,
    w_query,
    w_key,
    w_value,
    w_gate,
    log_decay,
    key_cache,
    value_cache,
    gn_gain,
    w_out,
    ffn_gain,
    w_ffn_gate,
    w_ffn_up,
    w_ffn_down,
):
    batch_rows = tokens.shape[0]
    heads_here = log_decay.shape[0]
    row_block = lax.all_gather(tokens, "tp", axis=1, tiled=True)
    widened = row_block.astype(jnp.float32)
    own_squares = jnp.sum(widened * widened, axis=1)
    scaled = (widened * attn_gain).astype(jnp.bfloat16)
    part_query = jnp.dot(scaled, w_query, preferred_element_type=jnp.float32)
    part_key = jnp.dot(scaled, w_key, preferred_element_type=jnp.float32)
    part_value = jnp.dot(scaled, w_value, preferred_element_type=jnp.float32)
    part_gate = jnp.dot(scaled, w_gate, preferred_element_type=jnp.float32)
    positions = lengths.astype(jnp.float32)
    total_squares = input_stat(own_squares)
    queries, new_keys, new_values, gates = lax.psum(
        (part_query, part_key, part_value, part_gate), "kv"
    )
    factor = lax.rsqrt(total_squares / D + RMS_EPS)[:, None]
    queries = rotate((queries * factor).reshape(batch_rows, heads_here, DK), positions) * DK ** (
        -0.5
    )
    new_keys = rotate((new_keys * factor).reshape(batch_rows, heads_here, DK), positions)
    new_values = (new_values * factor).reshape(batch_rows, heads_here, DK)
    gates = gates * factor
    query_low = queries.astype(jnp.bfloat16)
    partial_value = cache_partial(query_low, lengths, log_decay, key_cache, value_cache, heads_here)
    cached = lax.psum(partial_value.reshape(batch_rows, heads_here * DK), "kv")
    own_term = jnp.sum(queries * new_keys, axis=-1, keepdims=True) * new_values
    normed = group_norm(cached.reshape(batch_rows, heads_here, DK) + own_term, gn_gain)
    gated = (jax.nn.silu(gates) * normed).astype(jnp.bfloat16)
    out_partial = jnp.dot(gated, w_out, preferred_element_type=jnp.float32)
    mixed = lax.psum_scatter(out_partial, "tp", scatter_dimension=1, tiled=True)
    resid = (tokens.astype(jnp.float32) + mixed).astype(jnp.bfloat16)
    resid_block = lax.all_gather(resid, "tp", axis=1, tiled=True).astype(jnp.float32)
    mid_squares = jnp.sum(resid_block * resid_block, axis=1)
    scaled_mid = (resid_block * ffn_gain).astype(jnp.bfloat16)
    gate_part = jnp.dot(scaled_mid, w_ffn_gate, preferred_element_type=jnp.float32)
    up_part = jnp.dot(scaled_mid, w_ffn_up, preferred_element_type=jnp.float32)
    total_mid = channel_stat(mid_squares)
    gate_sum, up_sum = lax.psum((gate_part, up_part), "kv")
    factor_mid = lax.rsqrt(total_mid / D + RMS_EPS)[:, None]
    hidden = (jax.nn.silu(gate_sum * factor_mid) * (up_sum * factor_mid)).astype(jnp.bfloat16)
    down_partial = jnp.dot(hidden, w_ffn_down, preferred_element_type=jnp.float32)
    down = lax.psum_scatter(down_partial, "tp", scatter_dimension=1, tiled=True)
    return (resid.astype(jnp.float32) + down).astype(jnp.bfloat16)


LANES = 128
STAGE_TILES = 2
VG_AFTER = 1
F32 = jnp.float32
BF16 = jnp.bfloat16


def partner(index, j, parts):
    found, bit = 0, 1
    while bit < parts:
        digit = (index // bit) % 2
        found = found + bit * ((1 - digit) if (j // bit) % 2 else digit)
        bit *= 2
    return found


def stack(value, pieces):
    width = value.shape[1] // pieces
    return jnp.concatenate(
        [value[:, i * width : (i + 1) * width] for i in range(pieces)], axis=0
    ).astype(BF16)


def unstack(packed, pieces):
    wide = packed.astype(F32)
    rows = wide.shape[0] // pieces
    return jnp.concatenate([wide[i * rows : (i + 1) * rows] for i in range(pieces)], axis=1)


def pack(value):
    return stack(value, 2)


def unpack(packed):
    return unstack(packed, 2)


def plan(tiles, n_kv):
    step = STAGE_TILES * n_kv
    return tiles // step, tiles % step


def layer_kernel(
    n_kv,
    n_tp,
    tokens_hbm,
    lengths_hbm,
    attn_gain_hbm,
    log_decay_hbm,
    gn_gain_hbm,
    ffn_gain_hbm,
    wq_hbm,
    wk_hbm,
    wv_hbm,
    wg_hbm,
    kc_hbm,
    vc_hbm,
    wo_hbm,
    wfg_hbm,
    wfu_hbm,
    wfd_hbm,
    out_ref,
    wq,
    wk,
    wv,
    wg,
    kc,
    vc,
    wo,
    wfg,
    wfu,
    wfd,
    tokens_ref,
    lengths_ref,
    attn_gain_ref,
    log_decay_ref,
    gn_gain_ref,
    ffn_gain_ref,
    tok_buf,
    x_buf,
    sq_send,
    sq_recv,
    q_send,
    q_recv,
    q_full,
    trig,
    decay_buf,
    key_own,
    vg_send,
    vg_in,
    ca_send,
    ca_in,
    sc_send,
    sc_in,
    gt_send,
    gt_buf,
    o_buf,
    resid_buf,
    sqm_send,
    sqm_recv,
    gu_own,
    gu_send,
    gu_recv,
    hid_send,
    hid_recv,
    rest_send,
    rest_recv,
    rest_hid,
    down_buf,
    d_send,
    d_recv,
    load_sem,
    send_sem,
    recv_sem,
):
    rows, own_cols = tokens_ref.shape
    depth, wide = wq.shape
    span = kc.shape[1]
    half = DK // 2
    tiles = wfg.shape[1] // LANES
    win = STAGE_TILES * LANES
    n_full, rest = plan(tiles, n_kv)
    rest_tiles = rest // 2
    rest_base = n_full * STAGE_TILES * n_kv * LANES
    heads = n_kv
    middle = n_kv // 2 - 1
    shared = heads // 2
    me_kv = lax.axis_index("kv")
    me_tp = lax.axis_index("tp")
    me_core = me_tp % 2
    first_core = me_tp - me_core
    is_middle = (me_kv >= middle) & (me_kv < middle + 2)
    is_owner = (me_core == 1) & is_middle

    def kv_peer(j):
        return partner(me_kv, j, n_kv)

    def tp_peer(j):
        return partner(me_tp, j, n_tp)

    kv_order = tuple(range(n_kv - 1, 0, -1))

    barrier = pltpu.get_barrier_semaphore()
    for j in range(1, n_kv):
        for places in ({"kv": kv_peer(j)}, {"kv": kv_peer(j), "tp": tp_peer(1)}):
            pl.semaphore_signal(
                barrier, inc=1, device_id=places, device_id_type=pl.DeviceIdType.MESH
            )
    for j in range(1, n_tp):
        pl.semaphore_signal(
            barrier, inc=1, device_id={"tp": tp_peer(j)}, device_id_type=pl.DeviceIdType.MESH
        )

    loads = {}
    for slot, (name, src, dst) in enumerate(
        (
            ("tok", tokens_hbm, tokens_ref),
            ("len", lengths_hbm, lengths_ref),
            ("ag", attn_gain_hbm, attn_gain_ref),
            ("ld", log_decay_hbm, log_decay_ref),
            ("gg", gn_gain_hbm, gn_gain_ref),
            ("fg", ffn_gain_hbm, ffn_gain_ref),
            ("wq", wq_hbm, wq),
            ("kc", kc_hbm, kc),
            ("vc", vc_hbm, vc),
            ("wk", wk_hbm, wk),
            ("wv", wv_hbm, wv),
            ("wg", wg_hbm, wg),
            ("wo", wo_hbm, wo),
            ("wfg", wfg_hbm, wfg),
            ("wfu", wfu_hbm, wfu),
            ("wfd", wfd_hbm, wfd),
        )
    ):
        loads[name] = pltpu.make_async_copy(src, dst, load_sem.at[slot])

    names = ["tok", "sq", "q", "o", "sqm", "gu", "hid", "d", "gt", "rhid"]
    names += [f"{kind}{i}" for kind in ("vg", "ca", "sc", "rest") for i in range(2)]
    out_slot = {name: i for i, name in enumerate(names)}
    names = ["tok", "sq", "vg", "ca", "sc", "gt0", "gt1", "o0", "o1", "sqm", "d"]
    names += [f"q{h}" for h in range(heads)] + ["rest", "rhid0", "rhid1"]
    names += [f"{kind}{i}" for kind in ("gu", "hid") for i in range(n_full)]
    in_slot = {name: i for i, name in enumerate(names)}

    def remote(out, into, src, dst, where):
        return pltpu.make_async_remote_copy(
            src_ref=src,
            dst_ref=dst,
            send_sem=send_sem.at[out_slot[out]],
            recv_sem=recv_sem.at[in_slot[into]],
            device_id=where,
            device_id_type=pl.DeviceIdType.MESH,
        )

    def wait_in(into, ref):
        remote("tok", into, ref, ref, {"kv": kv_peer(1)}).wait_recv()

    def wait_out(out, ref):
        remote(out, "tok", ref, ref, {"kv": kv_peer(1)}).wait_send()

    def to_tp(out, into, src_of, dst):
        for chip in range(n_tp // 2 - 1, 0, -1):
            for core in (0, 1):
                target = partner(first_core, 2 * chip, n_tp) + core
                remote(out, into, src_of(target), dst, {"tp": target}).start()
        remote(out, into, src_of(tp_peer(1)), dst, {"tp": tp_peer(1)}).start()

    def column_tile(columns):
        lane_id = lax.broadcasted_iota(jnp.int32, (8, LANES), 1)
        tile = jnp.zeros((8, LANES), F32)
        groups = rows // 8
        for i, column in enumerate(columns):
            for r in range(groups):
                part = jnp.broadcast_to(column[r * 8 : (r + 1) * 8], (8, LANES))
                tile = jnp.where(lane_id == i * groups + r, part, tile)
        return tile

    def tile_column(tile, i):
        groups = rows // 8
        return jnp.concatenate(
            [tile[:, i * groups + r : i * groups + r + 1] for r in range(groups)], axis=0
        )

    for name in ("tok", "len", "ld", "ag", "wq"):
        loads[name].start()
    loads["tok"].wait()
    pl.semaphore_wait(barrier, 2 * (n_kv - 1) + n_tp - 1)

    to_tp("tok", "tok", lambda target: tokens_ref, tok_buf.at[me_tp])
    for name in ("wk", "wv", "wg", "kc", "vc", "gg", "fg"):
        loads[name].start()
    tok_buf[me_tp] = tokens_ref[...]

    for name in ("len", "ld", "ag"):
        loads[name].wait()
    row_id = lax.broadcasted_iota(jnp.int32, (rows, LANES), 0)
    lens = jnp.zeros((rows, LANES), jnp.int32)
    for b in range(rows):
        lens = jnp.where(row_id == b, lengths_ref[b], lens)
    lane = lax.broadcasted_iota(jnp.int32, (rows, half), 1).astype(F32)
    inverse = jnp.exp(lane * (-math.log(ROPE_BASE) / half))
    angles = lens[:, :1].astype(F32) * inverse
    trig[0] = jnp.cos(angles)
    trig[1] = jnp.sin(angles)
    places = rows * span
    col = lax.broadcasted_iota(jnp.int32, (rows, places), 1)
    row = lax.broadcasted_iota(jnp.int32, (rows, places), 0)
    slot = col - row * span
    position = slot + me_kv * span
    gap = lens[:, :1] - position
    live = (slot >= 0) & (slot < span) & (gap > 0)
    gap_f = jnp.where(live, gap, 0).astype(F32)
    for h in range(heads):
        decay_buf[h] = jnp.where(live, jnp.exp(gap_f * log_decay_ref[h]), 0.0)

    def rotate_in(front, back):
        cosine, sine = trig[0], trig[1]
        return front * cosine - back * sine, front * sine + back * cosine

    wait_in("tok", tok_buf.at[pl.ds(0, n_tp - 1)])
    squares = jnp.zeros((rows, 1), F32)
    for c in range(n_tp):
        wide_tok = tok_buf[c].astype(F32)
        squares = squares + jnp.sum(wide_tok * wide_tok, axis=1, keepdims=True)
        cols = pl.ds(c * own_cols, own_cols)
        x_buf[:, cols] = (wide_tok * attn_gain_ref[:, cols]).astype(BF16)
    sq_send[...] = column_tile([squares])
    for j in kv_order:
        remote("sq", "sq", sq_send, sq_recv.at[j - 1], {"kv": kv_peer(j)}).start()

    x = x_buf[...]
    loads["wq"].wait()
    for pair in range(heads // 2):
        q_own = jnp.dot(x, wq[:, pl.ds(pair * 2 * DK, 2 * DK)], preferred_element_type=F32)
        for i in range(2):
            h = pair * 2 + i
            piece = q_own[:, i * DK : (i + 1) * DK]
            q_send[h] = pack(piece)
            q_full[:, pl.ds(h * DK, DK)] = piece
            for j in kv_order:
                remote(
                    "q", f"q{h}", q_send.at[h], q_recv.at[h, j - 1], {"kv": kv_peer(j)}
                ).start()
    for name in ("wo", "wfg", "wfu", "wfd"):
        loads[name].start()

    for name in ("wk", "wv", "wg"):
        loads[name].wait()
    for i, weight in enumerate((wv, wg)):
        for pair in range(heads // 2):
            part = jnp.dot(x, weight[:, pl.ds(pair * 2 * DK, 2 * DK)], preferred_element_type=F32)
            for k in range(2):
                vg_send[pair * 2 + k, i] = pack(part[:, k * DK : (k + 1) * DK])
    key_own[...] = jnp.dot(x, wk[...], preferred_element_type=F32)

    wait_in("sq", sq_recv)
    total_sq = sq_send[...]
    for j in range(1, n_kv):
        total_sq = total_sq + sq_recv[j - 1]
    factor = lax.rsqrt(tile_column(total_sq, 0) / D + RMS_EPS)

    loads["kc"].wait()
    loads["vc"].wait()

    def owner_slot(oi):
        apart = partner(me_kv, middle + oi, n_kv)
        return jnp.where(me_core == 0, me_kv, n_kv - 1 + apart)

    def to_owner(oi, copies):
        @pl.when(jnp.logical_not((me_core == 1) & (me_kv == middle + oi)))
        def _():
            for kind, src, dst in copies:
                where = {"kv": middle + oi, "tp": first_core + 1}
                remote(f"{kind}{oi}", kind, src, dst, where).start()

    own_scores = []
    for h in range(heads):
        cols = pl.ds(h * DK, DK)
        wait_in(f"q{h}", q_recv.at[h])
        query = q_full[:, cols]
        for j in kv_order:
            query = query + unpack(q_recv[h, j - 1])
        query = query * factor
        front, back = rotate_in(query[:, :half], query[:, half:])
        query = jnp.concatenate([front, back], axis=1) * DK ** (-0.5)
        scores = lax.dot_general(
            query.astype(BF16),
            kc[:, :, cols].reshape(places, DK),
            (((1,), (1,)), ((), ())),
            preferred_element_type=F32,
        )
        mixing = (scores * decay_buf[h]).astype(BF16)
        cached = jnp.dot(mixing, vc[:, :, cols].reshape(places, DK), preferred_element_type=F32)
        ca_send[h] = pack(cached)
        key = key_own[:, cols]
        front, back = rotate_in(key[:, :half], key[:, half:])
        own_scores.append(
            jnp.sum(query[:, :half] * front + query[:, half:] * back, axis=1, keepdims=True)
            * factor
        )
        oi, hh = h // shared, h % shared
        copies = [("ca", ca_send.at[h], ca_in.at[owner_slot(oi), hh])]
        if hh == shared - 1:
            sc_send[oi] = column_tile(own_scores[oi * shared :])
            copies.append(("sc", sc_send.at[oi], sc_in.at[owner_slot(oi)]))
        to_owner(oi, copies)
        if h == VG_AFTER:
            for i in range(2):
                group = vg_send.at[pl.ds(i * shared, shared)]
                to_owner(i, [("vg", group, vg_in.at[owner_slot(i)])])

    @pl.when(is_owner)
    def _():
        oi = me_kv - middle
        base = oi * shared
        units = [(c, hh) for c in (1, 0) for hh in range(shared)]
        slots = {0: range(n_kv), 1: range(n_kv, 2 * n_kv - 1)}
        wait_in("vg", vg_in)
        gates, news = {}, {}
        for c, hh in units:
            parts = [[vg_in[k, hh, i] for k in slots[c]] for i in range(2)]
            if c:
                parts = [[vg_send[base + hh, i]] + parts[i] for i in range(2)]
            both = []
            for i in range(2):
                total = unpack(parts[i][0])
                for part in parts[i][1:]:
                    total = total + unpack(part)
                both.append(total * factor)
            news[c, hh] = both[0]
            gates[c, hh] = both[1] / (1.0 + jnp.exp(-both[1]))
        wait_in("sc", sc_in)
        wait_in("ca", ca_in)
        tiles_of = {}
        for c in (0, 1):
            parts = [sc_in[k] for k in slots[c]] + ([sc_send[oi]] if c else [])
            tiles_of[c] = functools.reduce(lambda p, q: p + q, parts)
        totals = {}
        for c, hh in units:
            total = tile_column(tiles_of[c], hh) * news[c, hh]
            if c:
                total = total + unpack(ca_send[base + hh])
            for k in slots[c]:
                total = total + unpack(ca_in[k, hh])
            totals[c, hh] = total
        sums = {u: jnp.sum(totals[u], axis=1, keepdims=True) for u in units}
        squared = {u: jnp.sum(totals[u] * totals[u], axis=1, keepdims=True) for u in units}
        for c, hh in units:
            center = sums[c, hh] / DK
            spread = squared[c, hh] / DK - center * center
            normed = (totals[c, hh] - center) * lax.rsqrt(spread + GN_EPS)
            result = pack(gates[c, hh] * normed)
            gt_send[c, hh] = result
            if c:
                gt_buf[oi, hh] = result
        for c in (0, 1):
            for j in kv_order + ((0,) if c == 0 else ()):
                where = {"kv": kv_peer(j) if j else me_kv, "tp": first_core + c}
                for i in range(2):

                    @pl.when(oi == i)
                    def _():
                        remote("gt", f"gt{i}", gt_send.at[c], gt_buf.at[i], where).start()

    loads["wo"].wait()
    loads["gg"].wait()
    for i in range(2):

        @pl.when(jnp.logical_not((me_core == 1) & (me_kv == middle + i)))
        def _():
            wait_in(f"gt{i}", gt_buf.at[i])

    for h in range(heads):
        cols = pl.ds(h * DK, DK)
        x_buf[:, cols] = (
            unpack(gt_buf[h // shared, h % shared]) * gn_gain_ref[:, cols]
        ).astype(BF16)
    gated = x_buf[...]
    for part in range(2):
        width = depth // 2
        piece = jnp.dot(gated, wo[:, pl.ds(part * width, width)], preferred_element_type=F32)
        o_buf[part, me_tp] = pack(piece)
        to_tp("o", f"o{part}", lambda target: o_buf.at[part, me_tp], o_buf.at[part, me_tp])
    loads["fg"].wait()
    for part in range(2):
        wait_in(f"o{part}", o_buf.at[part, pl.ds(0, n_tp - 1)])
    squares = jnp.zeros((rows, 1), F32)
    halves = []
    for part in range(2):
        total = unpack(o_buf[part, 0])
        for t in range(1, n_tp):
            total = total + unpack(o_buf[part, t])
        halves.append(total)
    mixed = jnp.concatenate(halves, axis=1)
    for c in range(n_tp):
        cols = pl.ds(c * own_cols, own_cols)
        own_mixed = mixed[:, c * own_cols : (c + 1) * own_cols]
        resid = (tok_buf[c].astype(F32) + own_mixed).astype(BF16)
        resid_wide = resid.astype(F32)
        resid_buf[c] = resid_wide
        squares = squares + jnp.sum(resid_wide * resid_wide, axis=1, keepdims=True)
        x_buf[:, cols] = (resid_wide * ffn_gain_ref[:, cols]).astype(BF16)
    sqm_send[...] = column_tile([squares])
    for j in kv_order:
        remote("sqm", "sqm", sqm_send, sqm_recv.at[j - 1], {"kv": kv_peer(j)}).start()

    x = x_buf[...]
    loads["wfg"].wait()
    loads["wfu"].wait()

    def stage_start(s, index):
        return pl.multiple_of((s * n_kv + index) * win, win)

    for s in range(n_full):
        for j in kv_order:
            cols = pl.ds(stage_start(s, kv_peer(j)), win)
            for i, weight in enumerate((wfg, wfu)):
                part = jnp.dot(x, weight[:, cols], preferred_element_type=F32)
                gu_send[s, j - 1, i] = pack(part)
            remote(
                "gu", f"gu{s}", gu_send.at[s, j - 1], gu_recv.at[s, j - 1], {"kv": kv_peer(j)}
            ).start()
    if rest:
        cols = pl.ds(rest_base, rest * LANES)
        both = [jnp.dot(x, w[:, cols], preferred_element_type=F32) for w in (wfg, wfu)]
        width = rest_tiles * LANES
        for o in range(2):
            mine = jnp.concatenate([b[:, o * width : (o + 1) * width] for b in both], axis=1)
            rest_send[o] = stack(mine, 2 * rest_tiles)
        for o in range(2):

            @pl.when(me_kv != middle + o)
            def _():
                apart = partner(me_kv, middle + o, n_kv)
                where = {"kv": middle + o}
                remote(
                    f"rest{o}", "rest", rest_send.at[o], rest_recv.at[apart - 1], where
                ).start()

    for s in range(n_full):
        cols = pl.ds(stage_start(s, me_kv), win)
        for i, weight in enumerate((wfg, wfu)):
            gu_own[s, i] = jnp.dot(x, weight[:, cols], preferred_element_type=F32)

    wait_in("sqm", sqm_recv)
    total_sq = sqm_send[...]
    for j in range(1, n_kv):
        total_sq = total_sq + sqm_recv[j - 1]
    factor = lax.rsqrt(tile_column(total_sq, 0) / D + RMS_EPS)

    def activate(gate, up):
        gate, up = gate * factor, up * factor
        return gate / (1.0 + jnp.exp(-gate)) * up

    for s in range(n_full):
        wait_in(f"gu{s}", gu_recv.at[s])
        both = []
        for i in range(2):
            total = gu_own[s, i]
            for j in kv_order:
                total = total + unpack(gu_recv[s, j - 1, i])
            both.append(total)
        hid_send[s] = pack(activate(*both))
        for j in kv_order:
            remote(
                "hid", f"hid{s}", hid_send.at[s], hid_recv.at[s, j - 1], {"kv": kv_peer(j)}
            ).start()

    if rest:

        @pl.when(is_middle)
        def _():
            o = me_kv - middle
            wait_in("rest", rest_recv)
            total = unstack(rest_send[o], 2 * rest_tiles)
            for k in range(n_kv - 1):
                total = total + unstack(rest_recv[k], 2 * rest_tiles)
            width = rest_tiles * LANES
            rest_hid[o] = stack(activate(total[:, :width], total[:, width:]), rest_tiles)
            for j in kv_order:
                for i in range(2):

                    @pl.when(o == i)
                    def _():
                        remote(
                            "rhid",
                            f"rhid{i}",
                            rest_hid.at[i],
                            rest_hid.at[i],
                            {"kv": kv_peer(j)},
                        ).start()

    loads["wfd"].wait()

    def down_of(s, index, packed):
        weight = wfd[pl.ds(stage_start(s, index), win), :]
        return jnp.dot(unpack(packed).astype(BF16), weight, preferred_element_type=F32)

    down = None
    for s in range(n_full):
        part = down_of(s, me_kv, hid_send[s])
        down = part if down is None else down + part
    for s in range(n_full):
        wait_in(f"hid{s}", hid_recv.at[s])
        for j in range(1, n_kv):
            down = down + down_of(s, kv_peer(j), hid_recv[s, j - 1])
    if rest:
        for o in range(2):

            @pl.when(me_kv != middle + o)
            def _():
                wait_in(f"rhid{o}", rest_hid.at[o])

        chunk = jnp.concatenate([unstack(rest_hid[o], rest_tiles) for o in range(2)], axis=1)
        weight = wfd[pl.ds(rest_base, rest * LANES), :]
        down = down + jnp.dot(chunk.astype(BF16), weight, preferred_element_type=F32)
    down_buf[...] = down
    for t in range(n_tp):
        d_send[t] = pack(down_buf[:, pl.ds(t * own_cols, own_cols)])
    to_tp("d", "d", lambda target: d_send.at[target], d_recv.at[me_tp])
    own = pl.ds(pl.multiple_of(me_tp * own_cols, own_cols), own_cols)
    result = down_buf[:, own] + resid_buf[me_tp]
    wait_in("d", d_recv.at[pl.ds(0, n_tp - 1)])
    for j in range(1, n_tp):
        result = result + unpack(d_recv[tp_peer(j)])
    out_ref[...] = result.astype(BF16)
    wait_out("tok", tok_buf.at[pl.ds(0, n_tp - 1)])
    wait_out("sq", sq_recv)
    wait_out("q", q_recv)
    wait_out("o", o_buf.at[:, pl.ds(0, n_tp - 1)])
    wait_out("sqm", sqm_recv)
    wait_out("gu", gu_recv)
    wait_out("hid", hid_recv)
    wait_out("d", d_recv.at[pl.ds(0, n_tp - 1)])
    for i in range(2):

        @pl.when(jnp.logical_not((me_core == 1) & (me_kv == middle + i)))
        def _():
            group = pl.ds(i * shared, shared)
            wait_out(f"vg{i}", vg_send.at[group])
            wait_out(f"ca{i}", ca_send.at[group])
            wait_out(f"sc{i}", sc_send.at[i])

        if rest:

            @pl.when(me_kv != middle + i)
            def _():
                wait_out(f"rest{i}", rest_send.at[i])

    @pl.when(is_owner)
    def _():
        wait_out("gt", ca_in)

    if rest:

        @pl.when(is_middle)
        def _():
            wait_out("rhid", rest_hid)


def fused(
    n_kv,
    n_tp,
    tokens,
    lengths,
    attn_gain,
    w_query,
    w_key,
    w_value,
    w_gate,
    log_decay,
    key_cache,
    value_cache,
    gn_gain,
    w_out,
    ffn_gain,
    w_ffn_gate,
    w_ffn_up,
    w_ffn_down,
):
    rows, own_cols = tokens.shape
    depth, wide = w_query.shape
    span = key_cache.shape[1]
    heads = log_decay.shape[0]
    shared = heads // 2
    win = STAGE_TILES * LANES
    n_full, rest = plan(w_ffn_gate.shape[1] // LANES, n_kv)
    rest_rows = max(rest // 2, 1) * rows
    peers = n_kv - 1
    vmem = pl.BlockSpec(memory_space=pltpu.VMEM)
    hbm = pl.BlockSpec(memory_space=pl.ANY)
    small = (
        tokens,
        lengths,
        attn_gain[None, :],
        log_decay,
        gn_gain[None, :],
        ffn_gain[None, :],
    )
    streamed = (
        w_query,
        w_key,
        w_value,
        w_gate,
        key_cache,
        value_cache,
        w_out,
        w_ffn_gate,
        w_ffn_up,
        w_ffn_down,
    )
    scratch = [pltpu.VMEM(a.shape, a.dtype) for a in streamed] + [
        (pltpu.SMEM if a.ndim == 1 else pltpu.VMEM)(a.shape, a.dtype) for a in small
    ]
    piece = (2 * rows, DK // 2)
    scratch += [
        pltpu.VMEM((n_tp, rows, own_cols), BF16),
        pltpu.VMEM((rows, depth), BF16),
        pltpu.VMEM((8, LANES), F32),
        pltpu.VMEM((peers, 8, LANES), F32),
        pltpu.VMEM((heads, *piece), BF16),
        pltpu.VMEM((heads, peers, *piece), BF16),
        pltpu.VMEM((rows, wide), F32),
        pltpu.VMEM((2, rows, DK // 2), F32),
        pltpu.VMEM((heads, rows, rows * span), F32),
        pltpu.VMEM((rows, wide), F32),
        pltpu.VMEM((heads, 2, *piece), BF16),
        pltpu.VMEM((2 * n_kv - 1, shared, 2, *piece), BF16),
        pltpu.VMEM((heads, *piece), BF16),
        pltpu.VMEM((2 * n_kv - 1, shared, *piece), BF16),
        pltpu.VMEM((2, 8, LANES), F32),
        pltpu.VMEM((2 * n_kv - 1, 8, LANES), F32),
        pltpu.VMEM((2, shared, *piece), BF16),
        pltpu.VMEM((2, shared, *piece), BF16),
        pltpu.VMEM((2, n_tp, 2 * rows, depth // 4), BF16),
        pltpu.VMEM((n_tp, rows, own_cols), F32),
        pltpu.VMEM((8, LANES), F32),
        pltpu.VMEM((peers, 8, LANES), F32),
        pltpu.VMEM((n_full, 2, rows, win), F32),
        pltpu.VMEM((n_full, peers, 2, 2 * rows, win // 2), BF16),
        pltpu.VMEM((n_full, peers, 2, 2 * rows, win // 2), BF16),
        pltpu.VMEM((n_full, 2 * rows, win // 2), BF16),
        pltpu.VMEM((n_full, peers, 2 * rows, win // 2), BF16),
        pltpu.VMEM((2, 2 * rest_rows, LANES), BF16),
        pltpu.VMEM((peers, 2 * rest_rows, LANES), BF16),
        pltpu.VMEM((peers, rest_rows, LANES), BF16),
        pltpu.VMEM((rows, depth), F32),
        pltpu.VMEM((n_tp, 2 * rows, own_cols // 2), BF16),
        pltpu.VMEM((n_tp, 2 * rows, own_cols // 2), BF16),
        pltpu.SemaphoreType.DMA((len(small) + len(streamed),)),
        pltpu.SemaphoreType.DMA((18,)),
        pltpu.SemaphoreType.DMA((14 + heads + 2 * n_full,)),
    ]
    return pl.pallas_call(
        functools.partial(layer_kernel, n_kv, n_tp),
        out_shape=pltpu.VMEM((rows, own_cols), BF16),
        in_specs=[hbm] * (len(small) + len(streamed)),
        out_specs=vmem,
        scratch_shapes=scratch,
        compiler_params=pltpu.CompilerParams(
            collective_id=0, has_side_effects=True, vmem_limit_bytes=60 * 1024 * 1024
        ),
    )(*small, *streamed)


def fits(mesh, tokens, log_decay, key_cache, w_query, w_ffn_gate):
    n_kv, n_tp, n_grp = mesh.shape["kv"], mesh.shape["tp"], mesh.shape["grp"]
    heads, span = log_decay.shape[0], key_cache.shape[1] // n_kv
    tiles = w_ffn_gate.shape[1] // n_tp // LANES
    rows = tokens.shape[0] // n_grp
    return (
        n_kv > 1
        and n_tp > 2
        and n_kv & (n_kv - 1) == 0
        and n_tp & (n_tp - 1) == 0
        and heads == n_kv * n_tp
        and heads // n_tp * (rows // 8) <= 2 * LANES
        and tokens.shape[1] // n_kv == heads * DK // n_tp
        and tokens.shape[1] % (n_kv * n_tp * 2 * LANES) == 0
        and heads * DK // n_tp % (4 * LANES) == 0
        and w_ffn_gate.shape[1] % (n_tp * LANES) == 0
        and plan(tiles, n_kv)[0] > 0
        and plan(tiles, n_kv)[1] % 2 == 0
        and n_kv > 2
        and tokens.shape[0] // n_grp % 8 == 0
        and span % 16 == 0
        and span <= 64
    )


def solution(mesh):
    specs = (
        P("grp", ("kv", "tp")),
        P("grp"),
        P("kv"),
        P("kv", "tp"),
        P("kv", "tp"),
        P("kv", "tp"),
        P("kv", "tp"),
        P("tp"),
        P("grp", "kv", "tp"),
        P("grp", "kv", "tp"),
        P("tp"),
        P("tp", "kv"),
        P("kv"),
        P("kv", "tp"),
        P("kv", "tp"),
        P("tp", "kv"),
    )

    def whole(*arrays):
        tokens, w_query, log_decay, key_cache = arrays[0], arrays[3], arrays[7], arrays[8]
        if fits(mesh, tokens, log_decay, key_cache, w_query, arrays[13]):
            body = functools.partial(fused, mesh.shape["kv"], mesh.shape["tp"])
        else:
            body = local
        return jax.shard_map(
            body,
            mesh=mesh,
            in_specs=specs,
            out_specs=P("grp", ("kv", "tp")),
            check_vma=False,
        )(*arrays)

    return whole
```

```python
import functools
import math

import jax
import jax.numpy as jnp
from jax import lax
from jax.experimental import pallas as pl
from jax.experimental.pallas import tpu as pltpu
from jax.sharding import PartitionSpec as P

DK = 256
D = 4096


RMS_EPS = 0.1
GN_EPS = 1.0
ROPE_BASE = 10000.0


def rotate(vectors, positions):
    half_dim = vectors.shape[-1] // 2
    inverse = ROPE_BASE ** (-jnp.arange(half_dim, dtype=jnp.float32) / half_dim)
    angles = positions[:, None, None] * inverse[None, None, :]
    cosine = jnp.cos(angles)
    sine_part = jnp.sin(angles)
    front_part = vectors[..., :half_dim]
    back_part = vectors[..., half_dim:]
    return jnp.concatenate(
        [front_part * cosine - back_part * sine_part, front_part * sine_part + back_part * cosine],
        axis=-1,
    )


def group_norm(totals, gn_gain):
    width = totals.shape[-1]
    center = jnp.sum(totals, axis=-1, keepdims=True) / width
    spread = jnp.sum(totals * totals, axis=-1, keepdims=True) / width - center * center
    normed = (totals - center) * lax.rsqrt(spread + GN_EPS)
    return normed.reshape(normed.shape[0], -1) * gn_gain


def channel_stat(own_squares):
    return lax.psum(own_squares, "kv")


def input_stat(own_squares):
    return lax.psum(own_squares, "kv")


def cache_partial(query_low, lengths, log_decay, key_cache, value_cache, heads_here):
    batch_rows = query_low.shape[0]
    span = key_cache.shape[1]
    slots = lax.axis_index("kv") * span + jnp.arange(span, dtype=jnp.int32)
    live = slots[None, :] < lengths[:, None]
    gaps = jnp.maximum((lengths[:, None] - slots[None, :]).astype(jnp.float32), 0.0)
    decays = jnp.exp(log_decay[None, None, :] * gaps[:, :, None])
    keys_here = key_cache.reshape(batch_rows, span, heads_here, DK)
    values_here = value_cache.reshape(batch_rows, span, heads_here, DK)
    scores = jnp.einsum("bphd,bhd->bph", keys_here, query_low, preferred_element_type=jnp.float32)
    mixing = jnp.where(live[:, :, None], scores * decays, 0.0).astype(jnp.bfloat16)
    return jnp.einsum("bph,bphd->bhd", mixing, values_here, preferred_element_type=jnp.float32)


def local(
    tokens,
    lengths,
    attn_gain,
    w_query,
    w_key,
    w_value,
    w_gate,
    log_decay,
    key_cache,
    value_cache,
    gn_gain,
    w_out,
    ffn_gain,
    w_ffn_gate,
    w_ffn_up,
    w_ffn_down,
):
    batch_rows = tokens.shape[0]
    heads_here = log_decay.shape[0]
    row_block = lax.all_gather(tokens, "tp", axis=1, tiled=True)
    widened = row_block.astype(jnp.float32)
    own_squares = jnp.sum(widened * widened, axis=1)
    scaled = (widened * attn_gain).astype(jnp.bfloat16)
    part_query = jnp.dot(scaled, w_query, preferred_element_type=jnp.float32)
    part_key = jnp.dot(scaled, w_key, preferred_element_type=jnp.float32)
    part_value = jnp.dot(scaled, w_value, preferred_element_type=jnp.float32)
    part_gate = jnp.dot(scaled, w_gate, preferred_element_type=jnp.float32)
    positions = lengths.astype(jnp.float32)
    total_squares = input_stat(own_squares)
    queries, new_keys, new_values, gates = lax.psum(
        (part_query, part_key, part_value, part_gate), "kv"
    )
    factor = lax.rsqrt(total_squares / D + RMS_EPS)[:, None]
    queries = rotate((queries * factor).reshape(batch_rows, heads_here, DK), positions) * DK ** (
        -0.5
    )
    new_keys = rotate((new_keys * factor).reshape(batch_rows, heads_here, DK), positions)
    new_values = (new_values * factor).reshape(batch_rows, heads_here, DK)
    gates = gates * factor
    query_low = queries.astype(jnp.bfloat16)
    partial_value = cache_partial(query_low, lengths, log_decay, key_cache, value_cache, heads_here)
    cached = lax.psum(partial_value.reshape(batch_rows, heads_here * DK), "kv")
    own_term = jnp.sum(queries * new_keys, axis=-1, keepdims=True) * new_values
    normed = group_norm(cached.reshape(batch_rows, heads_here, DK) + own_term, gn_gain)
    gated = (jax.nn.silu(gates) * normed).astype(jnp.bfloat16)
    out_partial = jnp.dot(gated, w_out, preferred_element_type=jnp.float32)
    mixed = lax.psum_scatter(out_partial, "tp", scatter_dimension=1, tiled=True)
    resid = (tokens.astype(jnp.float32) + mixed).astype(jnp.bfloat16)
    resid_block = lax.all_gather(resid, "tp", axis=1, tiled=True).astype(jnp.float32)
    mid_squares = jnp.sum(resid_block * resid_block, axis=1)
    scaled_mid = (resid_block * ffn_gain).astype(jnp.bfloat16)
    gate_part = jnp.dot(scaled_mid, w_ffn_gate, preferred_element_type=jnp.float32)
    up_part = jnp.dot(scaled_mid, w_ffn_up, preferred_element_type=jnp.float32)
    total_mid = channel_stat(mid_squares)
    gate_sum, up_sum = lax.psum((gate_part, up_part), "kv")
    factor_mid = lax.rsqrt(total_mid / D + RMS_EPS)[:, None]
    hidden = (jax.nn.silu(gate_sum * factor_mid) * (up_sum * factor_mid)).astype(jnp.bfloat16)
    down_partial = jnp.dot(hidden, w_ffn_down, preferred_element_type=jnp.float32)
    down = lax.psum_scatter(down_partial, "tp", scatter_dimension=1, tiled=True)
    return (resid.astype(jnp.float32) + down).astype(jnp.bfloat16)


LANES = 128
STAGE_TILES = 2
VG_AFTER = 1
F32 = jnp.float32
BF16 = jnp.bfloat16


def partner(index, j, parts):
    found, bit = 0, 1
    while bit < parts:
        digit = (index // bit) % 2
        found = found + bit * ((1 - digit) if (j // bit) % 2 else digit)
        bit *= 2
    return found


def stack(value, pieces):
    width = value.shape[1] // pieces
    return jnp.concatenate(
        [value[:, i * width : (i + 1) * width] for i in range(pieces)], axis=0
    ).astype(BF16)


def unstack(packed, pieces):
    wide = packed.astype(F32)
    rows = wide.shape[0] // pieces
    return jnp.concatenate([wide[i * rows : (i + 1) * rows] for i in range(pieces)], axis=1)


def pack(value):
    return stack(value, 2)


def unpack(packed):
    return unstack(packed, 2)


def plan(tiles, n_kv):
    step = STAGE_TILES * n_kv
    return tiles // step, tiles % step


def layer_kernel(
    n_kv,
    n_tp,
    tokens_hbm,
    lengths_hbm,
    attn_gain_hbm,
    log_decay_hbm,
    gn_gain_hbm,
    ffn_gain_hbm,
    wq_hbm,
    wk_hbm,
    wv_hbm,
    wg_hbm,
    kc_hbm,
    vc_hbm,
    wo_hbm,
    wfg_hbm,
    wfu_hbm,
    wfd_hbm,
    out_ref,
    wq,
    wk,
    wv,
    wg,
    kc,
    vc,
    wo,
    wfg,
    wfu,
    wfd,
    tokens_ref,
    lengths_ref,
    attn_gain_ref,
    log_decay_ref,
    gn_gain_ref,
    ffn_gain_ref,
    tok_buf,
    x_buf,
    q_send,
    q_recv,
    q_full,
    trig,
    decay_buf,
    key_own,
    vg_send,
    vg_in,
    ca_send,
    ca_in,
    sc_send,
    sc_in,
    gt_send,
    gt_buf,
    o_buf,
    resid_buf,
    sqm_send,
    sqm_recv,
    gu_own,
    gu_send,
    gu_recv,
    hid_send,
    hid_recv,
    rest_send,
    rest_recv,
    rest_out,
    rest_hid,
    down_buf,
    d_send,
    d_recv,
    load_sem,
    send_sem,
    recv_sem,
    go_sem,
):
    rows, own_cols = tokens_ref.shape
    depth, wide = wq.shape
    span = kc.shape[1]
    half = DK // 2
    tiles = wfg.shape[1] // LANES
    win = STAGE_TILES * LANES
    n_full, rest = plan(tiles, n_kv)
    rest_tiles = rest // 2
    rest_base = n_full * STAGE_TILES * n_kv * LANES
    heads = n_kv
    middle = n_kv // 2 - 1
    shared = heads // 2
    me_kv = lax.axis_index("kv")
    me_tp = lax.axis_index("tp")
    me_core = me_tp % 2
    first_core = me_tp - me_core
    is_middle = (me_kv >= middle) & (me_kv < middle + 2)
    is_owner = (me_core == 1) & is_middle

    def kv_peer(j):
        return partner(me_kv, j, n_kv)

    def tp_peer(j):
        return partner(me_tp, j, n_tp)

    kv_order = tuple(range(n_kv - 1, 0, -1))

    barrier = pltpu.get_barrier_semaphore()
    for j in range(1, n_tp):
        pl.semaphore_signal(
            barrier, inc=1, device_id={"tp": tp_peer(j)}, device_id_type=pl.DeviceIdType.MESH
        )
    for k in range(1, n_kv):

        @pl.when(me_kv < k)
        def _():
            pl.semaphore_signal(
                barrier, inc=1, device_id={"kv": k}, device_id_type=pl.DeviceIdType.MESH
            )

    loads = {}
    for slot, (name, src, dst) in enumerate(
        (
            ("tok", tokens_hbm, tokens_ref),
            ("len", lengths_hbm, lengths_ref),
            ("ag", attn_gain_hbm, attn_gain_ref),
            ("ld", log_decay_hbm, log_decay_ref),
            ("gg", gn_gain_hbm, gn_gain_ref),
            ("fg", ffn_gain_hbm, ffn_gain_ref),
            ("wq", wq_hbm, wq),
            ("kc", kc_hbm, kc),
            ("vc", vc_hbm, vc),
            ("wk", wk_hbm, wk),
            ("wv", wv_hbm, wv),
            ("wg", wg_hbm, wg),
            ("wo", wo_hbm, wo),
            ("wfg", wfg_hbm, wfg),
            ("wfu", wfu_hbm, wfu),
            ("wfd", wfd_hbm, wfd),
        )
    ):
        loads[name] = pltpu.make_async_copy(src, dst, load_sem.at[slot])

    names = ["tok", "q", "o", "sqm", "gu", "hid", "d", "gt", "rhid"]
    names += [f"{kind}{i}" for kind in ("vg", "ca", "sc", "rest") for i in range(2)]
    out_slot = {name: i for i, name in enumerate(names)}
    names = ["tok", "vg", "ca", "sc", "gt0", "gt1", "o0", "o1", "sqm", "d"]
    names += [f"q{h}" for h in range(heads)] + ["rest", "rhid0", "rhid1"]
    names += [f"{kind}{i}" for kind in ("gu", "hid") for i in range(n_full)]
    in_slot = {name: i for i, name in enumerate(names)}

    def remote(out, into, src, dst, where):
        return pltpu.make_async_remote_copy(
            src_ref=src,
            dst_ref=dst,
            send_sem=send_sem.at[out_slot[out]],
            recv_sem=recv_sem.at[in_slot[into]],
            device_id=where,
            device_id_type=pl.DeviceIdType.MESH,
        )

    def wait_in(into, ref):
        remote("tok", into, ref, ref, {"kv": kv_peer(1)}).wait_recv()

    def wait_out(out, ref):
        remote(out, "tok", ref, ref, {"kv": kv_peer(1)}).wait_send()

    def to_tp(out, into, src_of, dst):
        for chip in range(n_tp // 2 - 1, 0, -1):
            for core in (0, 1):
                target = partner(first_core, 2 * chip, n_tp) + core
                remote(out, into, src_of(target), dst, {"tp": target}).start()
        remote(out, into, src_of(tp_peer(1)), dst, {"tp": tp_peer(1)}).start()

    lane_id = lax.broadcasted_iota(jnp.int32, (8, LANES), 1)
    row_of = lax.broadcasted_iota(jnp.int32, (8, LANES), 0)

    def lanes_of(columns):
        spread = jnp.zeros((8, LANES), F32)
        for i, column in enumerate(columns):
            for first in range(0, rows, 8):
                part = jnp.broadcast_to(column[first : first + 8], (8, LANES))
                spread = jnp.where(lane_id == row_of + (i * rows + first), part, spread)
        return jnp.sum(spread, axis=0, keepdims=True)

    def column_of(line, i):
        wide_line = jnp.broadcast_to(line, (8, LANES))
        return jnp.concatenate(
            [
                jnp.sum(
                    jnp.where(lane_id == row_of + (i * rows + first), wide_line, 0.0),
                    axis=1,
                    keepdims=True,
                )
                for first in range(0, rows, 8)
            ],
            axis=0,
        )

    for name in ("tok", "len", "ld", "ag", "wq"):
        loads[name].start()
    pl.semaphore_wait(barrier, n_tp - 1 + me_kv)
    for k in range(n_kv - 1):

        @pl.when(me_kv > k)
        def _():
            pl.semaphore_signal(
                go_sem, inc=1, device_id={"kv": k}, device_id_type=pl.DeviceIdType.MESH
            )

    loads["tok"].wait()
    to_tp("tok", "tok", lambda target: tokens_ref, tok_buf.at[me_tp])
    for name in ("wk", "wv", "wg", "kc", "vc", "gg", "fg"):
        loads[name].start()
    tok_buf[me_tp] = tokens_ref[...]

    for name in ("len", "ld", "ag"):
        loads[name].wait()
    row_id = lax.broadcasted_iota(jnp.int32, (rows, LANES), 0)
    lens = jnp.zeros((rows, LANES), jnp.int32)
    for b in range(rows):
        lens = jnp.where(row_id == b, lengths_ref[b], lens)
    lane = lax.broadcasted_iota(jnp.int32, (rows, half), 1).astype(F32)
    inverse = jnp.exp(lane * (-math.log(ROPE_BASE) / half))
    angles = lens[:, :1].astype(F32) * inverse
    trig[0] = jnp.cos(angles)
    trig[1] = jnp.sin(angles)
    places = rows * span
    col = lax.broadcasted_iota(jnp.int32, (rows, places), 1)
    row = lax.broadcasted_iota(jnp.int32, (rows, places), 0)
    slot = col - row * span
    position = slot + me_kv * span
    gap = lens[:, :1] - position
    live = (slot >= 0) & (slot < span) & (gap > 0)
    gap_f = jnp.where(live, gap, 0).astype(F32)
    for h in range(heads):
        decay_buf[h] = jnp.where(live, jnp.exp(gap_f * log_decay_ref[h]), 0.0)

    def rotate_in(front, back):
        cosine, sine = trig[0], trig[1]
        return front * cosine - back * sine, front * sine + back * cosine

    wait_in("tok", tok_buf.at[pl.ds(0, n_tp - 1)])
    squares = jnp.zeros((rows, 1), F32)
    for c in range(n_tp):
        wide_tok = tok_buf[c].astype(F32)
        squares = squares + jnp.sum(wide_tok * wide_tok, axis=1, keepdims=True)
        cols = pl.ds(c * own_cols, own_cols)
        x_buf[:, cols] = (wide_tok * attn_gain_ref[:, cols]).astype(BF16)
    @pl.when(me_kv < n_kv - 1)
    def _():
        pl.semaphore_wait(go_sem, n_kv - 1 - me_kv)


    x = x_buf[...]
    loads["wq"].wait()
    for pair in range(heads // 2):
        q_own = jnp.dot(x, wq[:, pl.ds(pair * 2 * DK, 2 * DK)], preferred_element_type=F32)
        for i in range(2):
            h = pair * 2 + i
            piece = q_own[:, i * DK : (i + 1) * DK]
            q_send[h] = pack(piece)
            q_full[:, pl.ds(h * DK, DK)] = piece
            for j in kv_order:
                remote(
                    "q", f"q{h}", q_send.at[h], q_recv.at[h, j - 1], {"kv": kv_peer(j)}
                ).start()
    for name in ("wo", "wfg", "wfu", "wfd"):
        loads[name].start()

    for name in ("wk", "wv", "wg"):
        loads[name].wait()
    for i, weight in enumerate((wv, wg)):
        for pair in range(heads // 2):
            part = jnp.dot(x, weight[:, pl.ds(pair * 2 * DK, 2 * DK)], preferred_element_type=F32)
            for k in range(2):
                vg_send[pair * 2 + k, i] = pack(part[:, k * DK : (k + 1) * DK])
    key_own[...] = jnp.dot(x, wk[...], preferred_element_type=F32)

    loads["kc"].wait()
    loads["vc"].wait()

    def owner_slot(oi):
        apart = partner(me_kv, middle + oi, n_kv)
        return jnp.where(me_core == 0, me_kv, n_kv - 1 + apart)

    def to_owner(oi, copies):
        @pl.when(jnp.logical_not((me_core == 1) & (me_kv == middle + oi)))
        def _():
            for kind, src, dst in copies:
                where = {"kv": middle + oi, "tp": first_core + 1}
                remote(f"{kind}{oi}", kind, src, dst, where).start()

    own_scores = []
    for h in range(heads):
        cols = pl.ds(h * DK, DK)
        wait_in(f"q{h}", q_recv.at[h])
        query = q_full[:, cols]
        for j in kv_order:
            query = query + unpack(q_recv[h, j - 1])
        front, back = rotate_in(query[:, :half], query[:, half:])
        query = jnp.concatenate([front, back], axis=1) * DK ** (-0.5)
        scores = lax.dot_general(
            query.astype(BF16),
            kc[:, :, cols].reshape(places, DK),
            (((1,), (1,)), ((), ())),
            preferred_element_type=F32,
        )
        mixing = (scores * decay_buf[h]).astype(BF16)
        cached = jnp.dot(mixing, vc[:, :, cols].reshape(places, DK), preferred_element_type=F32)
        ca_send[h] = pack(cached)
        key = key_own[:, cols]
        front, back = rotate_in(key[:, :half], key[:, half:])
        own_scores.append(
            jnp.sum(query[:, :half] * front + query[:, half:] * back, axis=1, keepdims=True)
        )
        oi, hh = h // shared, h % shared
        copies = [("ca", ca_send.at[h], ca_in.at[owner_slot(oi), hh])]
        if hh == shared - 1:
            sc_send[oi] = lanes_of(own_scores[oi * shared :] + [squares])
            copies.append(("sc", sc_send.at[oi], sc_in.at[owner_slot(oi)]))
        to_owner(oi, copies)
        if h == VG_AFTER:
            for i in range(2):
                group = vg_send.at[pl.ds(i * shared, shared)]
                to_owner(i, [("vg", group, vg_in.at[owner_slot(i)])])

    @pl.when(is_owner)
    def _():
        oi = me_kv - middle
        base = oi * shared
        units = [(c, hh) for c in (1, 0) for hh in range(shared)]
        slots = {0: range(n_kv), 1: range(n_kv, 2 * n_kv - 1)}
        wait_in("sc", sc_in)
        lines = {}
        for c in (0, 1):
            parts = [sc_in[k] for k in slots[c]] + ([sc_send[oi]] if c else [])
            lines[c] = functools.reduce(lambda p, q: p + q, parts)
        factor = lax.rsqrt(column_of(lines[1], shared) / D + RMS_EPS)
        cubed = factor * factor * factor
        weights = {u: column_of(lines[u[0]], u[1]) * cubed for u in units}
        wait_in("vg", vg_in)
        gates, news = {}, {}
        for c, hh in units:
            parts = [[vg_in[k, hh, i] for k in slots[c]] for i in range(2)]
            if c:
                parts = [[vg_send[base + hh, i]] + parts[i] for i in range(2)]
            both = []
            for i in range(2):
                total = unpack(parts[i][0])
                for part in parts[i][1:]:
                    total = total + unpack(part)
                both.append(total)
            news[c, hh] = weights[c, hh] * both[0]
            both[1] = both[1] * factor
            gates[c, hh] = both[1] / (1.0 + jnp.exp(-both[1]))
        wait_in("ca", ca_in)
        totals = {}
        for c, hh in units:
            parts = [ca_in[k, hh] for k in slots[c]] + ([ca_send[base + hh]] if c else [])
            total = unpack(parts[0])
            for part in parts[1:]:
                total = total + unpack(part)
            totals[c, hh] = total * factor + news[c, hh]
        sums = {u: jnp.sum(totals[u], axis=1, keepdims=True) for u in units}
        squared = {u: jnp.sum(totals[u] * totals[u], axis=1, keepdims=True) for u in units}
        for c, hh in units:
            center = sums[c, hh] / DK
            spread = squared[c, hh] / DK - center * center
            normed = (totals[c, hh] - center) * lax.rsqrt(spread + GN_EPS)
            result = pack(gates[c, hh] * normed)
            gt_send[c, hh] = result
            if c:
                gt_buf[oi, hh] = result
        for c in (0, 1):
            for j in kv_order + ((0,) if c == 0 else ()):
                where = {"kv": kv_peer(j) if j else me_kv, "tp": first_core + c}
                for i in range(2):

                    @pl.when(oi == i)
                    def _():
                        remote("gt", f"gt{i}", gt_send.at[c], gt_buf.at[i], where).start()

    loads["wo"].wait()
    loads["gg"].wait()
    for i in range(2):

        @pl.when(jnp.logical_not((me_core == 1) & (me_kv == middle + i)))
        def _():
            wait_in(f"gt{i}", gt_buf.at[i])

    for h in range(heads):
        cols = pl.ds(h * DK, DK)
        x_buf[:, cols] = (
            unpack(gt_buf[h // shared, h % shared]) * gn_gain_ref[:, cols]
        ).astype(BF16)
    gated = x_buf[...]
    for part in range(2):
        width = depth // 2
        piece = jnp.dot(gated, wo[:, pl.ds(part * width, width)], preferred_element_type=F32)
        o_buf[part, me_tp] = pack(piece)
        to_tp("o", f"o{part}", lambda target: o_buf.at[part, me_tp], o_buf.at[part, me_tp])
    loads["fg"].wait()
    for part in range(2):
        wait_in(f"o{part}", o_buf.at[part, pl.ds(0, n_tp - 1)])
    squares = jnp.zeros((rows, 1), F32)
    halves = []
    for part in range(2):
        total = unpack(o_buf[part, 0])
        for t in range(1, n_tp):
            total = total + unpack(o_buf[part, t])
        halves.append(total)
    mixed = jnp.concatenate(halves, axis=1)
    for c in range(n_tp):
        cols = pl.ds(c * own_cols, own_cols)
        own_mixed = mixed[:, c * own_cols : (c + 1) * own_cols]
        resid = (tok_buf[c].astype(F32) + own_mixed).astype(BF16)
        resid_wide = resid.astype(F32)
        resid_buf[c] = resid_wide
        squares = squares + jnp.sum(resid_wide * resid_wide, axis=1, keepdims=True)
        x_buf[:, cols] = (resid_wide * ffn_gain_ref[:, cols]).astype(BF16)
    sqm_send[...] = lanes_of([squares])
    for j in kv_order:
        remote("sqm", "sqm", sqm_send, sqm_recv.at[j - 1], {"kv": kv_peer(j)}).start()

    x = x_buf[...]
    loads["wfg"].wait()
    loads["wfu"].wait()

    def stage_start(s, index):
        return pl.multiple_of((s * n_kv + index) * win, win)

    for s in range(n_full):
        for j in kv_order:
            cols = pl.ds(stage_start(s, kv_peer(j)), win)
            for i, weight in enumerate((wfg, wfu)):
                part = jnp.dot(x, weight[:, cols], preferred_element_type=F32)
                gu_send[s, j - 1, i] = pack(part)
            remote(
                "gu", f"gu{s}", gu_send.at[s, j - 1], gu_recv.at[s, j - 1], {"kv": kv_peer(j)}
            ).start()
    if rest:
        cols = pl.ds(rest_base, rest * LANES)
        both = [jnp.dot(x, w[:, cols], preferred_element_type=F32) for w in (wfg, wfu)]
        width = rest_tiles * LANES
        for o in range(2):
            mine = jnp.concatenate([b[:, o * width : (o + 1) * width] for b in both], axis=1)
            rest_send[o] = stack(mine, 2 * rest_tiles)
        for o in range(2):

            to_owner(o, [("rest", rest_send.at[o], rest_recv.at[owner_slot(o)])])

    for s in range(n_full):
        cols = pl.ds(stage_start(s, me_kv), win)
        for i, weight in enumerate((wfg, wfu)):
            gu_own[s, i] = jnp.dot(x, weight[:, cols], preferred_element_type=F32)

    wait_in("sqm", sqm_recv)
    total_sq = sqm_send[...]
    for j in range(1, n_kv):
        total_sq = total_sq + sqm_recv[j - 1]
    factor = lax.rsqrt(column_of(total_sq, 0) / D + RMS_EPS)

    def activate(gate, up):
        gate, up = gate * factor, up * factor
        return gate / (1.0 + jnp.exp(-gate)) * up

    for s in range(n_full):
        wait_in(f"gu{s}", gu_recv.at[s])
        both = []
        for i in range(2):
            total = gu_own[s, i]
            for j in kv_order:
                total = total + unpack(gu_recv[s, j - 1, i])
            both.append(total)
        hid_send[s] = pack(activate(*both))
        for j in kv_order:
            remote(
                "hid", f"hid{s}", hid_send.at[s], hid_recv.at[s, j - 1], {"kv": kv_peer(j)}
            ).start()

    if rest:

        @pl.when(is_owner)
        def _():
            o = me_kv - middle
            wait_in("rest", rest_recv)
            width = rest_tiles * LANES
            for c in (0, 1):
                slots = range(n_kv) if c == 0 else range(n_kv, 2 * n_kv - 1)
                parts = [rest_recv[k] for k in slots] + ([rest_send[o]] if c else [])
                total = unstack(parts[0], 2 * rest_tiles)
                for part in parts[1:]:
                    total = total + unstack(part, 2 * rest_tiles)
                result = stack(activate(total[:, :width], total[:, width:]), rest_tiles)
                rest_out[c] = result
                if c:
                    rest_hid[o] = result
                for j in kv_order + ((0,) if c == 0 else ()):
                    where = {"kv": kv_peer(j) if j else me_kv, "tp": first_core + c}
                    for i in range(2):

                        @pl.when(o == i)
                        def _():
                            remote(
                                "rhid", f"rhid{i}", rest_out.at[c], rest_hid.at[i], where
                            ).start()

    loads["wfd"].wait()

    def down_of(s, index, packed):
        weight = wfd[pl.ds(stage_start(s, index), win), :]
        return jnp.dot(unpack(packed).astype(BF16), weight, preferred_element_type=F32)

    down = None
    for s in range(n_full):
        part = down_of(s, me_kv, hid_send[s])
        down = part if down is None else down + part
    for s in range(n_full):
        wait_in(f"hid{s}", hid_recv.at[s])
        for j in range(1, n_kv):
            down = down + down_of(s, kv_peer(j), hid_recv[s, j - 1])
    if rest:
        near = jnp.where(me_kv > middle, 1, 0)
        width = rest_tiles * LANES
        for o in (near, 1 - near):

            @pl.when(jnp.logical_not((me_core == 1) & (me_kv == middle + o)))
            def _():
                for i in range(2):

                    @pl.when(o == i)
                    def _():
                        wait_in(f"rhid{i}", rest_hid.at[i])

            chunk = unstack(rest_hid[o], rest_tiles).astype(BF16)
            first = pl.multiple_of(rest_base + o * width, LANES)
            weight = wfd[pl.ds(first, width), :]
            down = down + jnp.dot(chunk, weight, preferred_element_type=F32)
    down_buf[...] = down
    for t in range(n_tp):
        d_send[t] = pack(down_buf[:, pl.ds(t * own_cols, own_cols)])
    to_tp("d", "d", lambda target: d_send.at[target], d_recv.at[me_tp])
    own = pl.ds(pl.multiple_of(me_tp * own_cols, own_cols), own_cols)
    result = down_buf[:, own] + resid_buf[me_tp]
    wait_in("d", d_recv.at[pl.ds(0, n_tp - 1)])
    for j in range(1, n_tp):
        result = result + unpack(d_recv[tp_peer(j)])
    out_ref[...] = result.astype(BF16)
    wait_out("tok", tok_buf.at[pl.ds(0, n_tp - 1)])
    wait_out("q", q_recv)
    wait_out("o", o_buf.at[:, pl.ds(0, n_tp - 1)])
    wait_out("sqm", sqm_recv)
    wait_out("gu", gu_recv)
    wait_out("hid", hid_recv)
    wait_out("d", d_recv.at[pl.ds(0, n_tp - 1)])
    for i in range(2):

        @pl.when(jnp.logical_not((me_core == 1) & (me_kv == middle + i)))
        def _():
            group = pl.ds(i * shared, shared)
            wait_out(f"vg{i}", vg_send.at[group])
            wait_out(f"ca{i}", ca_send.at[group])
            wait_out(f"sc{i}", sc_send.at[i])
            if rest:
                wait_out(f"rest{i}", rest_send.at[i])

    @pl.when(is_owner)
    def _():
        wait_out("gt", ca_in)
        if rest:
            wait_out("rhid", rest_hid)


def fused(
    n_kv,
    n_tp,
    tokens,
    lengths,
    attn_gain,
    w_query,
    w_key,
    w_value,
    w_gate,
    log_decay,
    key_cache,
    value_cache,
    gn_gain,
    w_out,
    ffn_gain,
    w_ffn_gate,
    w_ffn_up,
    w_ffn_down,
):
    rows, own_cols = tokens.shape
    depth, wide = w_query.shape
    span = key_cache.shape[1]
    heads = log_decay.shape[0]
    shared = heads // 2
    win = STAGE_TILES * LANES
    n_full, rest = plan(w_ffn_gate.shape[1] // LANES, n_kv)
    rest_rows = max(rest // 2, 1) * rows
    peers = n_kv - 1
    vmem = pl.BlockSpec(memory_space=pltpu.VMEM)
    hbm = pl.BlockSpec(memory_space=pl.ANY)
    small = (
        tokens,
        lengths,
        attn_gain[None, :],
        log_decay,
        gn_gain[None, :],
        ffn_gain[None, :],
    )
    streamed = (
        w_query,
        w_key,
        w_value,
        w_gate,
        key_cache,
        value_cache,
        w_out,
        w_ffn_gate,
        w_ffn_up,
        w_ffn_down,
    )
    scratch = [pltpu.VMEM(a.shape, a.dtype) for a in streamed] + [
        (pltpu.SMEM if a.ndim == 1 else pltpu.VMEM)(a.shape, a.dtype) for a in small
    ]
    piece = (2 * rows, DK // 2)
    scratch += [
        pltpu.VMEM((n_tp, rows, own_cols), BF16),
        pltpu.VMEM((rows, depth), BF16),
        pltpu.VMEM((heads, *piece), BF16),
        pltpu.VMEM((heads, peers, *piece), BF16),
        pltpu.VMEM((rows, wide), F32),
        pltpu.VMEM((2, rows, DK // 2), F32),
        pltpu.VMEM((heads, rows, rows * span), F32),
        pltpu.VMEM((rows, wide), F32),
        pltpu.VMEM((heads, 2, *piece), BF16),
        pltpu.VMEM((2 * n_kv - 1, shared, 2, *piece), BF16),
        pltpu.VMEM((heads, *piece), BF16),
        pltpu.VMEM((2 * n_kv - 1, shared, *piece), BF16),
        pltpu.VMEM((2, 1, LANES), F32),
        pltpu.VMEM((2 * n_kv - 1, 1, LANES), F32),
        pltpu.VMEM((2, shared, *piece), BF16),
        pltpu.VMEM((2, shared, *piece), BF16),
        pltpu.VMEM((2, n_tp, 2 * rows, depth // 4), BF16),
        pltpu.VMEM((n_tp, rows, own_cols), F32),
        pltpu.VMEM((1, LANES), F32),
        pltpu.VMEM((peers, 1, LANES), F32),
        pltpu.VMEM((n_full, 2, rows, win), F32),
        pltpu.VMEM((n_full, peers, 2, 2 * rows, win // 2), BF16),
        pltpu.VMEM((n_full, peers, 2, 2 * rows, win // 2), BF16),
        pltpu.VMEM((n_full, 2 * rows, win // 2), BF16),
        pltpu.VMEM((n_full, peers, 2 * rows, win // 2), BF16),
        pltpu.VMEM((2, 2 * rest_rows, LANES), BF16),
        pltpu.VMEM((2 * n_kv - 1, 2 * rest_rows, LANES), BF16),
        pltpu.VMEM((2, rest_rows, LANES), BF16),
        pltpu.VMEM((2 * n_kv - 1, rest_rows, LANES), BF16),
        pltpu.VMEM((rows, depth), F32),
        pltpu.VMEM((n_tp, 2 * rows, own_cols // 2), BF16),
        pltpu.VMEM((n_tp, 2 * rows, own_cols // 2), BF16),
        pltpu.SemaphoreType.DMA((len(small) + len(streamed),)),
        pltpu.SemaphoreType.DMA((17,)),
        pltpu.SemaphoreType.DMA((13 + heads + 2 * n_full,)),
        pltpu.SemaphoreType.REGULAR,
    ]
    return pl.pallas_call(
        functools.partial(layer_kernel, n_kv, n_tp),
        out_shape=pltpu.VMEM((rows, own_cols), BF16),
        in_specs=[hbm] * (len(small) + len(streamed)),
        out_specs=vmem,
        scratch_shapes=scratch,
        compiler_params=pltpu.CompilerParams(
            collective_id=0, has_side_effects=True, vmem_limit_bytes=60 * 1024 * 1024
        ),
    )(*small, *streamed)


def fits(mesh, tokens, log_decay, key_cache, w_query, w_ffn_gate):
    n_kv, n_tp, n_grp = mesh.shape["kv"], mesh.shape["tp"], mesh.shape["grp"]
    heads, span = log_decay.shape[0], key_cache.shape[1] // n_kv
    tiles = w_ffn_gate.shape[1] // n_tp // LANES
    rows = tokens.shape[0] // n_grp
    return (
        n_kv > 1
        and n_tp > 2
        and n_kv & (n_kv - 1) == 0
        and n_tp & (n_tp - 1) == 0
        and heads == n_kv * n_tp
        and (heads // n_tp // 2 + 1) * rows <= LANES
        and tokens.shape[1] // n_kv == heads * DK // n_tp
        and tokens.shape[1] % (n_kv * n_tp * 2 * LANES) == 0
        and heads * DK // n_tp % (4 * LANES) == 0
        and w_ffn_gate.shape[1] % (n_tp * LANES) == 0
        and plan(tiles, n_kv)[0] > 0
        and plan(tiles, n_kv)[1] % 2 == 0
        and n_kv > 2
        and tokens.shape[0] // n_grp % 8 == 0
        and span % 16 == 0
        and span <= 64
    )


def solution(mesh):
    specs = (
        P("grp", ("kv", "tp")),
        P("grp"),
        P("kv"),
        P("kv", "tp"),
        P("kv", "tp"),
        P("kv", "tp"),
        P("kv", "tp"),
        P("tp"),
        P("grp", "kv", "tp"),
        P("grp", "kv", "tp"),
        P("tp"),
        P("tp", "kv"),
        P("kv"),
        P("kv", "tp"),
        P("kv", "tp"),
        P("tp", "kv"),
    )

    def whole(*arrays):
        tokens, w_query, log_decay, key_cache = arrays[0], arrays[3], arrays[7], arrays[8]
        if fits(mesh, tokens, log_decay, key_cache, w_query, arrays[13]):
            body = functools.partial(fused, mesh.shape["kv"], mesh.shape["tp"])
        else:
            body = local
        return jax.shard_map(
            body,
            mesh=mesh,
            in_specs=specs,
            out_specs=P("grp", ("kv", "tp")),
            check_vma=False,
        )(*arrays)

    return whole
```

```python
import functools
import math

import jax
import jax.numpy as jnp
from jax import lax
from jax.experimental import pallas as pl
from jax.experimental.pallas import tpu as pltpu
from jax.sharding import PartitionSpec as P

DK = 256
D = 4096


RMS_EPS = 0.1
GN_EPS = 1.0
ROPE_BASE = 10000.0


def rotate(vectors, positions):
    half_dim = vectors.shape[-1] // 2
    inverse = ROPE_BASE ** (-jnp.arange(half_dim, dtype=jnp.float32) / half_dim)
    angles = positions[:, None, None] * inverse[None, None, :]
    cosine = jnp.cos(angles)
    sine_part = jnp.sin(angles)
    front_part = vectors[..., :half_dim]
    back_part = vectors[..., half_dim:]
    return jnp.concatenate(
        [front_part * cosine - back_part * sine_part, front_part * sine_part + back_part * cosine],
        axis=-1,
    )


def group_norm(totals, gn_gain):
    width = totals.shape[-1]
    center = jnp.sum(totals, axis=-1, keepdims=True) / width
    spread = jnp.sum(totals * totals, axis=-1, keepdims=True) / width - center * center
    normed = (totals - center) * lax.rsqrt(spread + GN_EPS)
    return normed.reshape(normed.shape[0], -1) * gn_gain


def channel_stat(own_squares):
    return lax.psum(own_squares, "kv")


def input_stat(own_squares):
    return lax.psum(own_squares, "kv")


def cache_partial(query_low, lengths, log_decay, key_cache, value_cache, heads_here):
    batch_rows = query_low.shape[0]
    span = key_cache.shape[1]
    slots = lax.axis_index("kv") * span + jnp.arange(span, dtype=jnp.int32)
    live = slots[None, :] < lengths[:, None]
    gaps = jnp.maximum((lengths[:, None] - slots[None, :]).astype(jnp.float32), 0.0)
    decays = jnp.exp(log_decay[None, None, :] * gaps[:, :, None])
    keys_here = key_cache.reshape(batch_rows, span, heads_here, DK)
    values_here = value_cache.reshape(batch_rows, span, heads_here, DK)
    scores = jnp.einsum("bphd,bhd->bph", keys_here, query_low, preferred_element_type=jnp.float32)
    mixing = jnp.where(live[:, :, None], scores * decays, 0.0).astype(jnp.bfloat16)
    return jnp.einsum("bph,bphd->bhd", mixing, values_here, preferred_element_type=jnp.float32)


def local(
    tokens,
    lengths,
    attn_gain,
    w_query,
    w_key,
    w_value,
    w_gate,
    log_decay,
    key_cache,
    value_cache,
    gn_gain,
    w_out,
    ffn_gain,
    w_ffn_gate,
    w_ffn_up,
    w_ffn_down,
):
    batch_rows = tokens.shape[0]
    heads_here = log_decay.shape[0]
    row_block = lax.all_gather(tokens, "tp", axis=1, tiled=True)
    widened = row_block.astype(jnp.float32)
    own_squares = jnp.sum(widened * widened, axis=1)
    scaled = (widened * attn_gain).astype(jnp.bfloat16)
    part_query = jnp.dot(scaled, w_query, preferred_element_type=jnp.float32)
    part_key = jnp.dot(scaled, w_key, preferred_element_type=jnp.float32)
    part_value = jnp.dot(scaled, w_value, preferred_element_type=jnp.float32)
    part_gate = jnp.dot(scaled, w_gate, preferred_element_type=jnp.float32)
    positions = lengths.astype(jnp.float32)
    total_squares = input_stat(own_squares)
    queries, new_keys, new_values, gates = lax.psum(
        (part_query, part_key, part_value, part_gate), "kv"
    )
    factor = lax.rsqrt(total_squares / D + RMS_EPS)[:, None]
    queries = rotate((queries * factor).reshape(batch_rows, heads_here, DK), positions) * DK ** (
        -0.5
    )
    new_keys = rotate((new_keys * factor).reshape(batch_rows, heads_here, DK), positions)
    new_values = (new_values * factor).reshape(batch_rows, heads_here, DK)
    gates = gates * factor
    query_low = queries.astype(jnp.bfloat16)
    partial_value = cache_partial(query_low, lengths, log_decay, key_cache, value_cache, heads_here)
    cached = lax.psum(partial_value.reshape(batch_rows, heads_here * DK), "kv")
    own_term = jnp.sum(queries * new_keys, axis=-1, keepdims=True) * new_values
    normed = group_norm(cached.reshape(batch_rows, heads_here, DK) + own_term, gn_gain)
    gated = (jax.nn.silu(gates) * normed).astype(jnp.bfloat16)
    out_partial = jnp.dot(gated, w_out, preferred_element_type=jnp.float32)
    mixed = lax.psum_scatter(out_partial, "tp", scatter_dimension=1, tiled=True)
    resid = (tokens.astype(jnp.float32) + mixed).astype(jnp.bfloat16)
    resid_block = lax.all_gather(resid, "tp", axis=1, tiled=True).astype(jnp.float32)
    mid_squares = jnp.sum(resid_block * resid_block, axis=1)
    scaled_mid = (resid_block * ffn_gain).astype(jnp.bfloat16)
    gate_part = jnp.dot(scaled_mid, w_ffn_gate, preferred_element_type=jnp.float32)
    up_part = jnp.dot(scaled_mid, w_ffn_up, preferred_element_type=jnp.float32)
    total_mid = channel_stat(mid_squares)
    gate_sum, up_sum = lax.psum((gate_part, up_part), "kv")
    factor_mid = lax.rsqrt(total_mid / D + RMS_EPS)[:, None]
    hidden = (jax.nn.silu(gate_sum * factor_mid) * (up_sum * factor_mid)).astype(jnp.bfloat16)
    down_partial = jnp.dot(hidden, w_ffn_down, preferred_element_type=jnp.float32)
    down = lax.psum_scatter(down_partial, "tp", scatter_dimension=1, tiled=True)
    return (resid.astype(jnp.float32) + down).astype(jnp.bfloat16)


LANES = 128
STAGE_TILES = 2
F32 = jnp.float32
BF16 = jnp.bfloat16


def partner(index, j, parts):
    found, bit = 0, 1
    while bit < parts:
        digit = (index // bit) % 2
        found = found + bit * ((1 - digit) if (j // bit) % 2 else digit)
        bit *= 2
    return found


def stack(value, pieces):
    width = value.shape[1] // pieces
    return jnp.concatenate(
        [value[:, i * width : (i + 1) * width] for i in range(pieces)], axis=0
    ).astype(BF16)


def unstack(packed, pieces):
    wide = packed.astype(F32)
    rows = wide.shape[0] // pieces
    return jnp.concatenate([wide[i * rows : (i + 1) * rows] for i in range(pieces)], axis=1)


def pack(value):
    return stack(value, 2)


def unpack(packed):
    return unstack(packed, 2)


def plan(tiles, n_kv):
    step = STAGE_TILES * n_kv
    return tiles // step, tiles % step


def layer_kernel(
    n_kv,
    n_tp,
    tokens_hbm,
    lengths_hbm,
    attn_gain_hbm,
    log_decay_hbm,
    gn_gain_hbm,
    ffn_gain_hbm,
    wq_hbm,
    wk_hbm,
    wv_hbm,
    wg_hbm,
    kc_hbm,
    vc_hbm,
    wo_hbm,
    wfg_hbm,
    wfu_hbm,
    wfd_hbm,
    out_ref,
    wq,
    wk,
    wv,
    wg,
    kc,
    vc,
    wo,
    wfg,
    wfu,
    wfd,
    tokens_ref,
    lengths_ref,
    attn_gain_ref,
    log_decay_ref,
    gn_gain_ref,
    ffn_gain_ref,
    tok_buf,
    x_buf,
    q_send,
    q_recv,
    q_full,
    trig,
    decay_buf,
    key_own,
    vg_send,
    vg_in,
    swap_send,
    swap_recv,
    ca_send,
    ca_in,
    sc_send,
    sc_in,
    gt_send,
    gt_buf,
    o_buf,
    resid_buf,
    sqm_send,
    sqm_recv,
    gu_own,
    gu_send,
    gu_recv,
    hid_send,
    hid_recv,
    rest_send,
    rest_recv,
    rest_out,
    rest_hid,
    down_buf,
    d_send,
    d_recv,
    load_sem,
    send_sem,
    recv_sem,
    go_sem,
):
    rows, own_cols = tokens_ref.shape
    depth, wide = wq.shape
    span = kc.shape[1]
    half = DK // 2
    tiles = wfg.shape[1] // LANES
    win = STAGE_TILES * LANES
    n_full, rest = plan(tiles, n_kv)
    rest_tiles = rest // 2
    rest_base = n_full * STAGE_TILES * n_kv * LANES
    heads = n_kv
    middle = n_kv // 2 - 1
    shared = heads // 2
    me_kv = lax.axis_index("kv")
    me_tp = lax.axis_index("tp")
    me_core = me_tp % 2
    first_core = me_tp - me_core
    is_middle = (me_kv >= middle) & (me_kv < middle + 2)
    is_owner = (me_core == 1) & is_middle

    def kv_peer(j):
        return partner(me_kv, j, n_kv)

    def tp_peer(j):
        return partner(me_tp, j, n_tp)

    kv_order = tuple(range(n_kv - 1, 0, -1))

    barrier = pltpu.get_barrier_semaphore()
    for j in range(1, n_tp):
        pl.semaphore_signal(
            barrier, inc=1, device_id={"tp": tp_peer(j)}, device_id_type=pl.DeviceIdType.MESH
        )
    for k in range(1, n_kv):

        @pl.when(me_kv < k)
        def _():
            pl.semaphore_signal(
                barrier, inc=1, device_id={"kv": k}, device_id_type=pl.DeviceIdType.MESH
            )

    loads = {}
    for slot, (name, src, dst) in enumerate(
        (
            ("tok", tokens_hbm, tokens_ref),
            ("len", lengths_hbm, lengths_ref),
            ("ag", attn_gain_hbm, attn_gain_ref),
            ("ld", log_decay_hbm, log_decay_ref),
            ("gg", gn_gain_hbm, gn_gain_ref),
            ("fg", ffn_gain_hbm, ffn_gain_ref),
            ("wq", wq_hbm, wq),
            ("kc", kc_hbm, kc),
            ("vc", vc_hbm, vc),
            ("wk", wk_hbm, wk),
            ("wv", wv_hbm, wv),
            ("wg", wg_hbm, wg),
            ("wo", wo_hbm, wo),
            ("wfg", wfg_hbm, wfg),
            ("wfu", wfu_hbm, wfu),
            ("wfd", wfd_hbm, wfd),
        )
    ):
        loads[name] = pltpu.make_async_copy(src, dst, load_sem.at[slot])

    names = ["tok", "q", "o", "sqm", "gu", "hid", "d", "gt", "rhid"]
    names += [f"{kind}{i}" for kind in ("ca", "sc", "rest") for i in range(2)]
    names += ["vg", "swap"]
    out_slot = {name: i for i, name in enumerate(names)}
    names = ["tok", "vg", "swap", "ca", "sc", "gt0", "gt1", "o0", "o1", "sqm", "d"]
    names += [f"q{h}" for h in range(heads)] + ["rest", "rhid0", "rhid1"]
    names += [f"{kind}{i}" for kind in ("gu", "hid") for i in range(n_full)]
    in_slot = {name: i for i, name in enumerate(names)}

    def remote(out, into, src, dst, where):
        return pltpu.make_async_remote_copy(
            src_ref=src,
            dst_ref=dst,
            send_sem=send_sem.at[out_slot[out]],
            recv_sem=recv_sem.at[in_slot[into]],
            device_id=where,
            device_id_type=pl.DeviceIdType.MESH,
        )

    def wait_in(into, ref):
        remote("tok", into, ref, ref, {"kv": kv_peer(1)}).wait_recv()

    def wait_out(out, ref):
        remote(out, "tok", ref, ref, {"kv": kv_peer(1)}).wait_send()

    def to_tp(out, into, src_of, dst):
        for chip in range(n_tp // 2 - 1, 0, -1):
            for core in (0, 1):
                target = partner(first_core, 2 * chip, n_tp) + core
                remote(out, into, src_of(target), dst, {"tp": target}).start()
        remote(out, into, src_of(tp_peer(1)), dst, {"tp": tp_peer(1)}).start()

    lane_id = lax.broadcasted_iota(jnp.int32, (8, LANES), 1)
    row_of = lax.broadcasted_iota(jnp.int32, (8, LANES), 0)

    def lanes_of(columns):
        spread = jnp.zeros((8, LANES), F32)
        for i, column in enumerate(columns):
            for first in range(0, rows, 8):
                part = jnp.broadcast_to(column[first : first + 8], (8, LANES))
                spread = jnp.where(lane_id == row_of + (i * rows + first), part, spread)
        return jnp.sum(spread, axis=0, keepdims=True)

    def column_of(line, i):
        wide_line = jnp.broadcast_to(line, (8, LANES))
        return jnp.concatenate(
            [
                jnp.sum(
                    jnp.where(lane_id == row_of + (i * rows + first), wide_line, 0.0),
                    axis=1,
                    keepdims=True,
                )
                for first in range(0, rows, 8)
            ],
            axis=0,
        )

    for name in ("tok", "len", "ld", "ag", "wq"):
        loads[name].start()
    pl.semaphore_wait(barrier, n_tp - 1 + me_kv)
    for k in range(n_kv - 1):

        @pl.when(me_kv > k)
        def _():
            pl.semaphore_signal(
                go_sem, inc=1, device_id={"kv": k}, device_id_type=pl.DeviceIdType.MESH
            )

    loads["tok"].wait()
    to_tp("tok", "tok", lambda target: tokens_ref, tok_buf.at[me_tp])
    for name in ("wk", "wv", "wg", "kc", "vc", "gg", "fg"):
        loads[name].start()
    tok_buf[me_tp] = tokens_ref[...]

    for name in ("len", "ld", "ag"):
        loads[name].wait()
    row_id = lax.broadcasted_iota(jnp.int32, (rows, LANES), 0)
    lens = jnp.zeros((rows, LANES), jnp.int32)
    for b in range(rows):
        lens = jnp.where(row_id == b, lengths_ref[b], lens)
    lane = lax.broadcasted_iota(jnp.int32, (rows, half), 1).astype(F32)
    inverse = jnp.exp(lane * (-math.log(ROPE_BASE) / half))
    angles = lens[:, :1].astype(F32) * inverse
    trig[0] = jnp.cos(angles)
    trig[1] = jnp.sin(angles)
    places = rows * span
    col = lax.broadcasted_iota(jnp.int32, (rows, places), 1)
    row = lax.broadcasted_iota(jnp.int32, (rows, places), 0)
    slot = col - row * span
    position = slot + me_kv * span
    gap = lens[:, :1] - position
    live = (slot >= 0) & (slot < span) & (gap > 0)
    gap_f = jnp.where(live, gap, 0).astype(F32)
    for h in range(heads):
        decay_buf[h] = jnp.where(live, jnp.exp(gap_f * log_decay_ref[h]), 0.0)

    def rotate_in(front, back):
        cosine, sine = trig[0], trig[1]
        return front * cosine - back * sine, front * sine + back * cosine

    wait_in("tok", tok_buf.at[pl.ds(0, n_tp - 1)])
    squares = jnp.zeros((rows, 1), F32)
    for c in range(n_tp):
        wide_tok = tok_buf[c].astype(F32)
        squares = squares + jnp.sum(wide_tok * wide_tok, axis=1, keepdims=True)
        cols = pl.ds(c * own_cols, own_cols)
        x_buf[:, cols] = (wide_tok * attn_gain_ref[:, cols]).astype(BF16)
    @pl.when(me_kv < n_kv - 1)
    def _():
        pl.semaphore_wait(go_sem, n_kv - 1 - me_kv)


    x = x_buf[...]
    loads["wq"].wait()
    for pair in range(heads // 2):
        q_own = jnp.dot(x, wq[:, pl.ds(pair * 2 * DK, 2 * DK)], preferred_element_type=F32)
        for i in range(2):
            h = pair * 2 + i
            piece = q_own[:, i * DK : (i + 1) * DK]
            q_send[h] = pack(piece)
            q_full[:, pl.ds(h * DK, DK)] = piece
            for j in kv_order:
                remote(
                    "q", f"q{h}", q_send.at[h], q_recv.at[h, j - 1], {"kv": kv_peer(j)}
                ).start()
    for name in ("wo", "wfg", "wfu", "wfd"):
        loads[name].start()

    for name in ("wk", "wv", "wg"):
        loads[name].wait()
    for i, weight in enumerate((wv, wg)):
        for pair in range(heads // 2):
            part = jnp.dot(x, weight[:, pl.ds(pair * 2 * DK, 2 * DK)], preferred_element_type=F32)
            for k in range(2):
                vg_send[pair * 2 + k, i] = pack(part[:, k * DK : (k + 1) * DK])
    side = jnp.where(me_kv > middle, 1, 0)
    away = jnp.where(me_kv > middle, me_kv - middle - 1, middle - me_kv)

    @pl.when(jnp.logical_not(is_owner))
    def _():
        slot = jnp.where(me_core == 0, away, n_kv // 2 - 1 + away)
        where = {"kv": middle + side, "tp": first_core + 1}
        remote("vg", "vg", vg_send, vg_in.at[slot], where).start()

    key_own[...] = jnp.dot(x, wk[...], preferred_element_type=F32)

    loads["kc"].wait()
    loads["vc"].wait()

    def owner_slot(oi):
        apart = partner(me_kv, middle + oi, n_kv)
        return jnp.where(me_core == 0, me_kv, n_kv - 1 + apart)

    def to_owner(oi, copies):
        @pl.when(jnp.logical_not((me_core == 1) & (me_kv == middle + oi)))
        def _():
            for kind, src, dst in copies:
                where = {"kv": middle + oi, "tp": first_core + 1}
                remote(f"{kind}{oi}", kind, src, dst, where).start()

    own_scores = []
    for h in range(heads):
        cols = pl.ds(h * DK, DK)
        wait_in(f"q{h}", q_recv.at[h])
        query = q_full[:, cols]
        for j in kv_order:
            query = query + unpack(q_recv[h, j - 1])
        front, back = rotate_in(query[:, :half], query[:, half:])
        query = jnp.concatenate([front, back], axis=1) * DK ** (-0.5)
        scores = lax.dot_general(
            query.astype(BF16),
            kc[:, :, cols].reshape(places, DK),
            (((1,), (1,)), ((), ())),
            preferred_element_type=F32,
        )
        mixing = (scores * decay_buf[h]).astype(BF16)
        cached = jnp.dot(mixing, vc[:, :, cols].reshape(places, DK), preferred_element_type=F32)
        ca_send[h] = pack(cached)
        key = key_own[:, cols]
        front, back = rotate_in(key[:, :half], key[:, half:])
        own_scores.append(
            jnp.sum(query[:, :half] * front + query[:, half:] * back, axis=1, keepdims=True)
        )
        oi, hh = h // shared, h % shared
        copies = [("ca", ca_send.at[h], ca_in.at[owner_slot(oi), hh])]
        if hh == shared - 1:
            sc_send[oi] = lanes_of(own_scores[oi * shared :] + [squares])
            copies.append(("sc", sc_send.at[oi], sc_in.at[owner_slot(oi)]))
        to_owner(oi, copies)

    @pl.when(is_owner)
    def _():
        oi = me_kv - middle
        base = oi * shared
        units = [(c, hh) for c in (1, 0) for hh in range(shared)]
        slots = {0: range(n_kv), 1: range(n_kv, 2 * n_kv - 1)}
        wait_in("vg", vg_in)
        near = {0: range(n_kv // 2), 1: range(n_kv // 2, n_kv - 1)}

        def half_sum(c, head, i):
            parts = [vg_in[k, head, i] for k in near[c]]
            if c:
                parts.append(vg_send[head, i])
            total = unpack(parts[0])
            for part in parts[1:]:
                total = total + unpack(part)
            return total

        for c, hh in units:
            for i in range(2):
                swap_send[c, hh, i] = pack(half_sum(c, shared - base + hh, i))
        for i in range(2):

            @pl.when(oi == i)
            def _():
                where = {"kv": middle + 1 - i}
                remote("swap", "swap", swap_send, swap_recv, where).start()

        sums_of = {(c, hh, i): half_sum(c, base + hh, i) for c, hh in units for i in range(2)}
        wait_in("sc", sc_in)
        lines = {}
        for c in (0, 1):
            parts = [sc_in[k] for k in slots[c]] + ([sc_send[oi]] if c else [])
            lines[c] = functools.reduce(lambda p, q: p + q, parts)
        factor = lax.rsqrt(column_of(lines[1], shared) / D + RMS_EPS)
        cubed = factor * factor * factor
        weights = {u: column_of(lines[u[0]], u[1]) * cubed for u in units}
        wait_in("swap", swap_recv)
        gates, news = {}, {}
        for c, hh in units:
            both = [sums_of[c, hh, i] + unpack(swap_recv[c, hh, i]) for i in range(2)]
            news[c, hh] = weights[c, hh] * both[0]
            gate = both[1] * factor
            gates[c, hh] = gate / (1.0 + jnp.exp(-gate))
        wait_in("ca", ca_in)
        totals = {}
        for c, hh in units:
            parts = [ca_in[k, hh] for k in slots[c]] + ([ca_send[base + hh]] if c else [])
            total = unpack(parts[0])
            for part in parts[1:]:
                total = total + unpack(part)
            totals[c, hh] = total * factor + news[c, hh]
        sums = {u: jnp.sum(totals[u], axis=1, keepdims=True) for u in units}
        squared = {u: jnp.sum(totals[u] * totals[u], axis=1, keepdims=True) for u in units}
        for c, hh in units:
            center = sums[c, hh] / DK
            spread = squared[c, hh] / DK - center * center
            normed = (totals[c, hh] - center) * lax.rsqrt(spread + GN_EPS)
            result = pack(gates[c, hh] * normed)
            gt_send[c, hh] = result
            if c:
                gt_buf[oi, hh] = result
        for c in (0, 1):
            for j in kv_order + ((0,) if c == 0 else ()):
                where = {"kv": kv_peer(j) if j else me_kv, "tp": first_core + c}
                for i in range(2):

                    @pl.when(oi == i)
                    def _():
                        remote("gt", f"gt{i}", gt_send.at[c], gt_buf.at[i], where).start()

    loads["wo"].wait()
    loads["gg"].wait()
    for i in range(2):

        @pl.when(jnp.logical_not((me_core == 1) & (me_kv == middle + i)))
        def _():
            wait_in(f"gt{i}", gt_buf.at[i])

    for h in range(heads):
        cols = pl.ds(h * DK, DK)
        x_buf[:, cols] = (
            unpack(gt_buf[h // shared, h % shared]) * gn_gain_ref[:, cols]
        ).astype(BF16)
    gated = x_buf[...]

    def o_send(part, core):
        mine = o_buf.at[part, me_tp]
        if core is None:
            remote("o", f"o{part}", mine, mine, {"tp": tp_peer(1)}).start()
        else:
            for chip in range(n_tp // 2 - 1, 0, -1):
                target = partner(first_core, 2 * chip, n_tp) + core
                remote("o", f"o{part}", mine, mine, {"tp": target}).start()

    for part in range(2):
        width = depth // 2
        piece = jnp.dot(gated, wo[:, pl.ds(part * width, width)], preferred_element_type=F32)
        o_buf[part, me_tp] = pack(piece)
        o_send(part, 0)
    for part in range(2):
        o_send(part, 1)
    for part in range(2):
        o_send(part, None)
    loads["fg"].wait()
    for part in range(2):
        wait_in(f"o{part}", o_buf.at[part, pl.ds(0, n_tp - 1)])
    squares = jnp.zeros((rows, 1), F32)
    halves = []
    for part in range(2):
        total = unpack(o_buf[part, 0])
        for t in range(1, n_tp):
            total = total + unpack(o_buf[part, t])
        halves.append(total)
    mixed = jnp.concatenate(halves, axis=1)
    for c in range(n_tp):
        cols = pl.ds(c * own_cols, own_cols)
        own_mixed = mixed[:, c * own_cols : (c + 1) * own_cols]
        resid = (tok_buf[c].astype(F32) + own_mixed).astype(BF16)
        resid_wide = resid.astype(F32)
        resid_buf[c] = resid_wide
        squares = squares + jnp.sum(resid_wide * resid_wide, axis=1, keepdims=True)
        x_buf[:, cols] = (resid_wide * ffn_gain_ref[:, cols]).astype(BF16)
    sqm_send[...] = lanes_of([squares])
    for j in kv_order:
        remote("sqm", "sqm", sqm_send, sqm_recv.at[j - 1], {"kv": kv_peer(j)}).start()

    x = x_buf[...]
    loads["wfg"].wait()
    loads["wfu"].wait()

    def stage_start(s, index):
        return pl.multiple_of((s * n_kv + index) * win, win)

    for s in range(n_full):
        for j in kv_order:
            cols = pl.ds(stage_start(s, kv_peer(j)), win)
            for i, weight in enumerate((wfg, wfu)):
                part = jnp.dot(x, weight[:, cols], preferred_element_type=F32)
                gu_send[s, j - 1, i] = pack(part)
            remote(
                "gu", f"gu{s}", gu_send.at[s, j - 1], gu_recv.at[s, j - 1], {"kv": kv_peer(j)}
            ).start()
    if rest:
        cols = pl.ds(rest_base, rest * LANES)
        both = [jnp.dot(x, w[:, cols], preferred_element_type=F32) for w in (wfg, wfu)]
        width = rest_tiles * LANES
        for o in range(2):
            mine = jnp.concatenate([b[:, o * width : (o + 1) * width] for b in both], axis=1)
            rest_send[o] = stack(mine, 2 * rest_tiles)
        for o in range(2):

            to_owner(o, [("rest", rest_send.at[o], rest_recv.at[owner_slot(o)])])

    for s in range(n_full):
        cols = pl.ds(stage_start(s, me_kv), win)
        for i, weight in enumerate((wfg, wfu)):
            gu_own[s, i] = jnp.dot(x, weight[:, cols], preferred_element_type=F32)

    wait_in("sqm", sqm_recv)
    total_sq = sqm_send[...]
    for j in range(1, n_kv):
        total_sq = total_sq + sqm_recv[j - 1]
    factor = lax.rsqrt(column_of(total_sq, 0) / D + RMS_EPS)

    def activate(gate, up):
        gate, up = gate * factor, up * factor
        return gate / (1.0 + jnp.exp(-gate)) * up

    for s in range(n_full):
        wait_in(f"gu{s}", gu_recv.at[s])
        both = []
        for i in range(2):
            total = gu_own[s, i]
            for j in kv_order:
                total = total + unpack(gu_recv[s, j - 1, i])
            both.append(total)
        hid_send[s] = pack(activate(*both))
        for j in kv_order:
            remote(
                "hid", f"hid{s}", hid_send.at[s], hid_recv.at[s, j - 1], {"kv": kv_peer(j)}
            ).start()

    if rest:

        @pl.when(is_owner)
        def _():
            o = me_kv - middle
            wait_in("rest", rest_recv)
            width = rest_tiles * LANES
            for c in (0, 1):
                slots = range(n_kv) if c == 0 else range(n_kv, 2 * n_kv - 1)
                parts = [rest_recv[k] for k in slots] + ([rest_send[o]] if c else [])
                total = unstack(parts[0], 2 * rest_tiles)
                for part in parts[1:]:
                    total = total + unstack(part, 2 * rest_tiles)
                result = stack(activate(total[:, :width], total[:, width:]), rest_tiles)
                rest_out[c] = result
                if c:
                    rest_hid[o] = result
                for j in kv_order + ((0,) if c == 0 else ()):
                    where = {"kv": kv_peer(j) if j else me_kv, "tp": first_core + c}
                    for i in range(2):

                        @pl.when(o == i)
                        def _():
                            remote(
                                "rhid", f"rhid{i}", rest_out.at[c], rest_hid.at[i], where
                            ).start()

    loads["wfd"].wait()

    def down_of(s, index, packed):
        weight = wfd[pl.ds(stage_start(s, index), win), :]
        return jnp.dot(unpack(packed).astype(BF16), weight, preferred_element_type=F32)

    down = None
    for s in range(n_full):
        part = down_of(s, me_kv, hid_send[s])
        down = part if down is None else down + part
    for s in range(n_full):
        wait_in(f"hid{s}", hid_recv.at[s])
        for j in range(1, n_kv):
            down = down + down_of(s, kv_peer(j), hid_recv[s, j - 1])
    if rest:
        near = jnp.where(me_kv > middle, 1, 0)
        width = rest_tiles * LANES
        for o in (near, 1 - near):

            @pl.when(jnp.logical_not((me_core == 1) & (me_kv == middle + o)))
            def _():
                for i in range(2):

                    @pl.when(o == i)
                    def _():
                        wait_in(f"rhid{i}", rest_hid.at[i])

            chunk = unstack(rest_hid[o], rest_tiles).astype(BF16)
            first = pl.multiple_of(rest_base + o * width, LANES)
            weight = wfd[pl.ds(first, width), :]
            down = down + jnp.dot(chunk, weight, preferred_element_type=F32)
    down_buf[...] = down
    for t in range(n_tp):
        d_send[t] = pack(down_buf[:, pl.ds(t * own_cols, own_cols)])
    to_tp("d", "d", lambda target: d_send.at[target], d_recv.at[me_tp])
    own = pl.ds(pl.multiple_of(me_tp * own_cols, own_cols), own_cols)
    result = down_buf[:, own] + resid_buf[me_tp]
    wait_in("d", d_recv.at[pl.ds(0, n_tp - 1)])
    for j in range(1, n_tp):
        result = result + unpack(d_recv[tp_peer(j)])
    out_ref[...] = result.astype(BF16)
    wait_out("tok", tok_buf.at[pl.ds(0, n_tp - 1)])
    wait_out("q", q_recv)
    wait_out("o", o_buf.at[:, pl.ds(0, n_tp - 1)])
    wait_out("sqm", sqm_recv)
    wait_out("gu", gu_recv)
    wait_out("hid", hid_recv)
    wait_out("d", d_recv.at[pl.ds(0, n_tp - 1)])
    for i in range(2):

        @pl.when(jnp.logical_not((me_core == 1) & (me_kv == middle + i)))
        def _():
            group = pl.ds(i * shared, shared)
            wait_out(f"ca{i}", ca_send.at[group])
            wait_out(f"sc{i}", sc_send.at[i])
            if rest:
                wait_out(f"rest{i}", rest_send.at[i])

    @pl.when(jnp.logical_not(is_owner))
    def _():
        wait_out("vg", vg_send)

    @pl.when(is_owner)
    def _():
        wait_out("gt", ca_in)
        wait_out("swap", swap_send)
        if rest:
            wait_out("rhid", rest_hid)


def fused(
    n_kv,
    n_tp,
    tokens,
    lengths,
    attn_gain,
    w_query,
    w_key,
    w_value,
    w_gate,
    log_decay,
    key_cache,
    value_cache,
    gn_gain,
    w_out,
    ffn_gain,
    w_ffn_gate,
    w_ffn_up,
    w_ffn_down,
):
    rows, own_cols = tokens.shape
    depth, wide = w_query.shape
    span = key_cache.shape[1]
    heads = log_decay.shape[0]
    shared = heads // 2
    win = STAGE_TILES * LANES
    n_full, rest = plan(w_ffn_gate.shape[1] // LANES, n_kv)
    rest_rows = max(rest // 2, 1) * rows
    peers = n_kv - 1
    vmem = pl.BlockSpec(memory_space=pltpu.VMEM)
    hbm = pl.BlockSpec(memory_space=pl.ANY)
    small = (
        tokens,
        lengths,
        attn_gain[None, :],
        log_decay,
        gn_gain[None, :],
        ffn_gain[None, :],
    )
    streamed = (
        w_query,
        w_key,
        w_value,
        w_gate,
        key_cache,
        value_cache,
        w_out,
        w_ffn_gate,
        w_ffn_up,
        w_ffn_down,
    )
    scratch = [pltpu.VMEM(a.shape, a.dtype) for a in streamed] + [
        (pltpu.SMEM if a.ndim == 1 else pltpu.VMEM)(a.shape, a.dtype) for a in small
    ]
    piece = (2 * rows, DK // 2)
    scratch += [
        pltpu.VMEM((n_tp, rows, own_cols), BF16),
        pltpu.VMEM((rows, depth), BF16),
        pltpu.VMEM((heads, *piece), BF16),
        pltpu.VMEM((heads, peers, *piece), BF16),
        pltpu.VMEM((rows, wide), F32),
        pltpu.VMEM((2, rows, DK // 2), F32),
        pltpu.VMEM((heads, rows, rows * span), F32),
        pltpu.VMEM((rows, wide), F32),
        pltpu.VMEM((heads, 2, *piece), BF16),
        pltpu.VMEM((peers, heads, 2, *piece), BF16),
        pltpu.VMEM((2, shared, 2, *piece), BF16),
        pltpu.VMEM((2, shared, 2, *piece), BF16),
        pltpu.VMEM((heads, *piece), BF16),
        pltpu.VMEM((2 * n_kv - 1, shared, *piece), BF16),
        pltpu.VMEM((2, 1, LANES), F32),
        pltpu.VMEM((2 * n_kv - 1, 1, LANES), F32),
        pltpu.VMEM((2, shared, *piece), BF16),
        pltpu.VMEM((2, shared, *piece), BF16),
        pltpu.VMEM((2, n_tp, 2 * rows, depth // 4), BF16),
        pltpu.VMEM((n_tp, rows, own_cols), F32),
        pltpu.VMEM((1, LANES), F32),
        pltpu.VMEM((peers, 1, LANES), F32),
        pltpu.VMEM((n_full, 2, rows, win), F32),
        pltpu.VMEM((n_full, peers, 2, 2 * rows, win // 2), BF16),
        pltpu.VMEM((n_full, peers, 2, 2 * rows, win // 2), BF16),
        pltpu.VMEM((n_full, 2 * rows, win // 2), BF16),
        pltpu.VMEM((n_full, peers, 2 * rows, win // 2), BF16),
        pltpu.VMEM((2, 2 * rest_rows, LANES), BF16),
        pltpu.VMEM((2 * n_kv - 1, 2 * rest_rows, LANES), BF16),
        pltpu.VMEM((2, rest_rows, LANES), BF16),
        pltpu.VMEM((2 * n_kv - 1, rest_rows, LANES), BF16),
        pltpu.VMEM((rows, depth), F32),
        pltpu.VMEM((n_tp, 2 * rows, own_cols // 2), BF16),
        pltpu.VMEM((n_tp, 2 * rows, own_cols // 2), BF16),
        pltpu.SemaphoreType.DMA((len(small) + len(streamed),)),
        pltpu.SemaphoreType.DMA((17,)),
        pltpu.SemaphoreType.DMA((14 + heads + 2 * n_full,)),
        pltpu.SemaphoreType.REGULAR,
    ]
    return pl.pallas_call(
        functools.partial(layer_kernel, n_kv, n_tp),
        out_shape=pltpu.VMEM((rows, own_cols), BF16),
        in_specs=[hbm] * (len(small) + len(streamed)),
        out_specs=vmem,
        scratch_shapes=scratch,
        compiler_params=pltpu.CompilerParams(
            collective_id=0, has_side_effects=True, vmem_limit_bytes=60 * 1024 * 1024
        ),
    )(*small, *streamed)


def fits(mesh, tokens, log_decay, key_cache, w_query, w_ffn_gate):
    n_kv, n_tp, n_grp = mesh.shape["kv"], mesh.shape["tp"], mesh.shape["grp"]
    heads, span = log_decay.shape[0], key_cache.shape[1] // n_kv
    tiles = w_ffn_gate.shape[1] // n_tp // LANES
    rows = tokens.shape[0] // n_grp
    return (
        n_kv > 1
        and n_tp > 2
        and n_kv & (n_kv - 1) == 0
        and n_tp & (n_tp - 1) == 0
        and heads == n_kv * n_tp
        and (heads // n_tp // 2 + 1) * rows <= LANES
        and tokens.shape[1] // n_kv == heads * DK // n_tp
        and tokens.shape[1] % (n_kv * n_tp * 2 * LANES) == 0
        and heads * DK // n_tp % (4 * LANES) == 0
        and w_ffn_gate.shape[1] % (n_tp * LANES) == 0
        and plan(tiles, n_kv)[0] > 0
        and plan(tiles, n_kv)[1] % 2 == 0
        and n_kv > 2
        and tokens.shape[0] // n_grp % 8 == 0
        and span % 16 == 0
        and span <= 64
    )


def solution(mesh):
    specs = (
        P("grp", ("kv", "tp")),
        P("grp"),
        P("kv"),
        P("kv", "tp"),
        P("kv", "tp"),
        P("kv", "tp"),
        P("kv", "tp"),
        P("tp"),
        P("grp", "kv", "tp"),
        P("grp", "kv", "tp"),
        P("tp"),
        P("tp", "kv"),
        P("kv"),
        P("kv", "tp"),
        P("kv", "tp"),
        P("tp", "kv"),
    )

    def whole(*arrays):
        tokens, w_query, log_decay, key_cache = arrays[0], arrays[3], arrays[7], arrays[8]
        if fits(mesh, tokens, log_decay, key_cache, w_query, arrays[13]):
            body = functools.partial(fused, mesh.shape["kv"], mesh.shape["tp"])
        else:
            body = local
        return jax.shard_map(
            body,
            mesh=mesh,
            in_specs=specs,
            out_specs=P("grp", ("kv", "tp")),
            check_vma=False,
        )(*arrays)

    return whole
```

```python
import functools
import math

import jax
import jax.numpy as jnp
from jax import lax
from jax.experimental import pallas as pl
from jax.experimental.pallas import tpu as pltpu
from jax.sharding import PartitionSpec as P

DK = 256
D = 4096


RMS_EPS = 0.1
GN_EPS = 1.0
ROPE_BASE = 10000.0


def rotate(vectors, positions):
    half_dim = vectors.shape[-1] // 2
    inverse = ROPE_BASE ** (-jnp.arange(half_dim, dtype=jnp.float32) / half_dim)
    angles = positions[:, None, None] * inverse[None, None, :]
    cosine = jnp.cos(angles)
    sine_part = jnp.sin(angles)
    front_part = vectors[..., :half_dim]
    back_part = vectors[..., half_dim:]
    return jnp.concatenate(
        [front_part * cosine - back_part * sine_part, front_part * sine_part + back_part * cosine],
        axis=-1,
    )


def group_norm(totals, gn_gain):
    width = totals.shape[-1]
    center = jnp.sum(totals, axis=-1, keepdims=True) / width
    spread = jnp.sum(totals * totals, axis=-1, keepdims=True) / width - center * center
    normed = (totals - center) * lax.rsqrt(spread + GN_EPS)
    return normed.reshape(normed.shape[0], -1) * gn_gain


def channel_stat(own_squares):
    return lax.psum(own_squares, "kv")


def input_stat(own_squares):
    return lax.psum(own_squares, "kv")


def cache_partial(query_low, lengths, log_decay, key_cache, value_cache, heads_here):
    batch_rows = query_low.shape[0]
    span = key_cache.shape[1]
    slots = lax.axis_index("kv") * span + jnp.arange(span, dtype=jnp.int32)
    live = slots[None, :] < lengths[:, None]
    gaps = jnp.maximum((lengths[:, None] - slots[None, :]).astype(jnp.float32), 0.0)
    decays = jnp.exp(log_decay[None, None, :] * gaps[:, :, None])
    keys_here = key_cache.reshape(batch_rows, span, heads_here, DK)
    values_here = value_cache.reshape(batch_rows, span, heads_here, DK)
    scores = jnp.einsum("bphd,bhd->bph", keys_here, query_low, preferred_element_type=jnp.float32)
    mixing = jnp.where(live[:, :, None], scores * decays, 0.0).astype(jnp.bfloat16)
    return jnp.einsum("bph,bphd->bhd", mixing, values_here, preferred_element_type=jnp.float32)


def local(
    tokens,
    lengths,
    attn_gain,
    w_query,
    w_key,
    w_value,
    w_gate,
    log_decay,
    key_cache,
    value_cache,
    gn_gain,
    w_out,
    ffn_gain,
    w_ffn_gate,
    w_ffn_up,
    w_ffn_down,
):
    batch_rows = tokens.shape[0]
    heads_here = log_decay.shape[0]
    row_block = lax.all_gather(tokens, "tp", axis=1, tiled=True)
    widened = row_block.astype(jnp.float32)
    own_squares = jnp.sum(widened * widened, axis=1)
    scaled = (widened * attn_gain).astype(jnp.bfloat16)
    part_query = jnp.dot(scaled, w_query, preferred_element_type=jnp.float32)
    part_key = jnp.dot(scaled, w_key, preferred_element_type=jnp.float32)
    part_value = jnp.dot(scaled, w_value, preferred_element_type=jnp.float32)
    part_gate = jnp.dot(scaled, w_gate, preferred_element_type=jnp.float32)
    positions = lengths.astype(jnp.float32)
    total_squares = input_stat(own_squares)
    queries, new_keys, new_values, gates = lax.psum(
        (part_query, part_key, part_value, part_gate), "kv"
    )
    factor = lax.rsqrt(total_squares / D + RMS_EPS)[:, None]
    queries = rotate((queries * factor).reshape(batch_rows, heads_here, DK), positions) * DK ** (
        -0.5
    )
    new_keys = rotate((new_keys * factor).reshape(batch_rows, heads_here, DK), positions)
    new_values = (new_values * factor).reshape(batch_rows, heads_here, DK)
    gates = gates * factor
    query_low = queries.astype(jnp.bfloat16)
    partial_value = cache_partial(query_low, lengths, log_decay, key_cache, value_cache, heads_here)
    cached = lax.psum(partial_value.reshape(batch_rows, heads_here * DK), "kv")
    own_term = jnp.sum(queries * new_keys, axis=-1, keepdims=True) * new_values
    normed = group_norm(cached.reshape(batch_rows, heads_here, DK) + own_term, gn_gain)
    gated = (jax.nn.silu(gates) * normed).astype(jnp.bfloat16)
    out_partial = jnp.dot(gated, w_out, preferred_element_type=jnp.float32)
    mixed = lax.psum_scatter(out_partial, "tp", scatter_dimension=1, tiled=True)
    resid = (tokens.astype(jnp.float32) + mixed).astype(jnp.bfloat16)
    resid_block = lax.all_gather(resid, "tp", axis=1, tiled=True).astype(jnp.float32)
    mid_squares = jnp.sum(resid_block * resid_block, axis=1)
    scaled_mid = (resid_block * ffn_gain).astype(jnp.bfloat16)
    gate_part = jnp.dot(scaled_mid, w_ffn_gate, preferred_element_type=jnp.float32)
    up_part = jnp.dot(scaled_mid, w_ffn_up, preferred_element_type=jnp.float32)
    total_mid = channel_stat(mid_squares)
    gate_sum, up_sum = lax.psum((gate_part, up_part), "kv")
    factor_mid = lax.rsqrt(total_mid / D + RMS_EPS)[:, None]
    hidden = (jax.nn.silu(gate_sum * factor_mid) * (up_sum * factor_mid)).astype(jnp.bfloat16)
    down_partial = jnp.dot(hidden, w_ffn_down, preferred_element_type=jnp.float32)
    down = lax.psum_scatter(down_partial, "tp", scatter_dimension=1, tiled=True)
    return (resid.astype(jnp.float32) + down).astype(jnp.bfloat16)


LANES = 128
STAGE_TILES = 2
F32 = jnp.float32
BF16 = jnp.bfloat16


def partner(index, j, parts):
    found, bit = 0, 1
    while bit < parts:
        digit = (index // bit) % 2
        found = found + bit * ((1 - digit) if (j // bit) % 2 else digit)
        bit *= 2
    return found


def stack(value, pieces):
    width = value.shape[1] // pieces
    return jnp.concatenate(
        [value[:, i * width : (i + 1) * width] for i in range(pieces)], axis=0
    ).astype(BF16)


def unstack(packed, pieces):
    wide = packed.astype(F32)
    rows = wide.shape[0] // pieces
    return jnp.concatenate([wide[i * rows : (i + 1) * rows] for i in range(pieces)], axis=1)


def pack(value):
    return stack(value, 2)


def unpack(packed):
    return unstack(packed, 2)


def plan(tiles, n_kv):
    step = STAGE_TILES * n_kv
    return tiles // step, tiles % step


def layer_kernel(
    n_kv,
    n_tp,
    tokens_hbm,
    lengths_hbm,
    attn_gain_hbm,
    log_decay_hbm,
    gn_gain_hbm,
    ffn_gain_hbm,
    wq_hbm,
    wk_hbm,
    wv_hbm,
    wg_hbm,
    kc_hbm,
    vc_hbm,
    wo_hbm,
    wfg_hbm,
    wfu_hbm,
    wfd_hbm,
    out_ref,
    wq,
    wk,
    wv,
    wg,
    kc,
    vc,
    wo,
    wfg,
    wfu,
    wfd,
    tokens_ref,
    lengths_ref,
    attn_gain_ref,
    log_decay_ref,
    gn_gain_ref,
    ffn_gain_ref,
    tok_buf,
    x_buf,
    q_send,
    q_recv,
    q_full,
    trig,
    decay_buf,
    key_own,
    vg_send,
    vg_in,
    swap_send,
    swap_recv,
    ca_send,
    ca_in,
    sc_send,
    sc_in,
    gt_send,
    gt_buf,
    o_buf,
    resid_buf,
    sqm_send,
    sqm_recv,
    gu_own,
    gu_send,
    gu_recv,
    hid_send,
    hid_recv,
    rest_send,
    rest_recv,
    rest_out,
    rest_hid,
    down_buf,
    d_send,
    d_recv,
    load_sem,
    send_sem,
    recv_sem,
    go_sem,
):
    rows, own_cols = tokens_ref.shape
    depth, wide = wq.shape
    span = kc.shape[1]
    half = DK // 2
    tiles = wfg.shape[1] // LANES
    win = STAGE_TILES * LANES
    n_full, rest = plan(tiles, n_kv)
    rest_tiles = rest // 2
    rest_base = n_full * STAGE_TILES * n_kv * LANES
    heads = n_kv
    middle = n_kv // 2 - 1
    shared = heads // 2
    me_kv = lax.axis_index("kv")
    me_tp = lax.axis_index("tp")
    me_core = me_tp % 2
    first_core = me_tp - me_core
    is_middle = (me_kv >= middle) & (me_kv < middle + 2)
    is_owner = (me_core == 1) & is_middle
    side = jnp.where(me_kv > middle, 1, 0)
    far_group = pl.ds((1 - side) * shared, shared)
    near_group = pl.ds(side * shared, shared)

    def kv_peer(j):
        return partner(me_kv, j, n_kv)

    def tp_peer(j):
        return partner(me_tp, j, n_tp)

    kv_order = tuple(range(n_kv - 1, 0, -1))

    barrier = pltpu.get_barrier_semaphore()
    for j in range(1, n_tp):
        pl.semaphore_signal(
            barrier, inc=1, device_id={"tp": tp_peer(j)}, device_id_type=pl.DeviceIdType.MESH
        )
    for k in range(1, n_kv):

        @pl.when(me_kv < k)
        def _():
            pl.semaphore_signal(
                barrier, inc=1, device_id={"kv": k}, device_id_type=pl.DeviceIdType.MESH
            )

    loads = {}
    for slot, (name, src, dst) in enumerate(
        (
            ("tok", tokens_hbm, tokens_ref),
            ("len", lengths_hbm, lengths_ref),
            ("ag", attn_gain_hbm, attn_gain_ref),
            ("ld", log_decay_hbm, log_decay_ref),
            ("gg", gn_gain_hbm, gn_gain_ref),
            ("fg", ffn_gain_hbm, ffn_gain_ref),
            ("wq", wq_hbm, wq),
            ("kc", kc_hbm, kc),
            ("vc", vc_hbm, vc),
            ("wk", wk_hbm, wk),
            ("wv", wv_hbm, wv),
            ("wg", wg_hbm, wg),
            ("wo", wo_hbm, wo),
            ("wfg", wfg_hbm, wfg),
            ("wfu", wfu_hbm, wfu),
            ("wfd", wfd_hbm, wfd),
        )
    ):
        loads[name] = pltpu.make_async_copy(src, dst, load_sem.at[slot])

    names = ["tok", "q", "o", "sqm", "gu", "hid", "d", "gt", "rhid"]
    names += [f"{kind}{i}" for kind in ("ca", "sc", "rest") for i in range(2)]
    names += ["vg", "swap"]
    out_slot = {name: i for i, name in enumerate(names)}
    names = ["tok", "vgf", "vgn", "swap", "ca", "sc", "gt0", "gt1", "o0", "o1", "sqm", "d"]
    names += [f"q{h}" for h in range(heads)] + ["rest", "rhid0", "rhid1"]
    names += [f"{kind}{i}" for kind in ("gu", "hid") for i in range(n_full)]
    in_slot = {name: i for i, name in enumerate(names)}

    def remote(out, into, src, dst, where):
        return pltpu.make_async_remote_copy(
            src_ref=src,
            dst_ref=dst,
            send_sem=send_sem.at[out_slot[out]],
            recv_sem=recv_sem.at[in_slot[into]],
            device_id=where,
            device_id_type=pl.DeviceIdType.MESH,
        )

    def wait_in(into, ref):
        remote("tok", into, ref, ref, {"kv": kv_peer(1)}).wait_recv()

    def wait_out(out, ref):
        remote(out, "tok", ref, ref, {"kv": kv_peer(1)}).wait_send()

    def to_tp(out, into, src_of, dst):
        for chip in range(n_tp // 2 - 1, 0, -1):
            for core in (0, 1):
                target = partner(first_core, 2 * chip, n_tp) + core
                remote(out, into, src_of(target), dst, {"tp": target}).start()
        remote(out, into, src_of(tp_peer(1)), dst, {"tp": tp_peer(1)}).start()

    lane_id = lax.broadcasted_iota(jnp.int32, (8, LANES), 1)
    row_of = lax.broadcasted_iota(jnp.int32, (8, LANES), 0)

    def lanes_of(columns):
        spread = jnp.zeros((8, LANES), F32)
        for i, column in enumerate(columns):
            for first in range(0, rows, 8):
                part = jnp.broadcast_to(column[first : first + 8], (8, LANES))
                spread = jnp.where(lane_id == row_of + (i * rows + first), part, spread)
        return jnp.sum(spread, axis=0, keepdims=True)

    def column_of(line, i):
        wide_line = jnp.broadcast_to(line, (8, LANES))
        return jnp.concatenate(
            [
                jnp.sum(
                    jnp.where(lane_id == row_of + (i * rows + first), wide_line, 0.0),
                    axis=1,
                    keepdims=True,
                )
                for first in range(0, rows, 8)
            ],
            axis=0,
        )

    for name in ("tok", "len", "ld", "ag", "wq"):
        loads[name].start()
    pl.semaphore_wait(barrier, n_tp - 1 + me_kv)
    for k in range(n_kv - 1):

        @pl.when(me_kv > k)
        def _():
            pl.semaphore_signal(
                go_sem, inc=1, device_id={"kv": k}, device_id_type=pl.DeviceIdType.MESH
            )

    loads["tok"].wait()
    to_tp("tok", "tok", lambda target: tokens_ref, tok_buf.at[me_tp])
    for name in ("wk", "wv", "wg", "kc", "vc", "gg", "fg"):
        loads[name].start()
    tok_buf[me_tp] = tokens_ref[...]

    for name in ("len", "ld", "ag"):
        loads[name].wait()
    row_id = lax.broadcasted_iota(jnp.int32, (rows, LANES), 0)
    lens = jnp.zeros((rows, LANES), jnp.int32)
    for b in range(rows):
        lens = jnp.where(row_id == b, lengths_ref[b], lens)
    lane = lax.broadcasted_iota(jnp.int32, (rows, half), 1).astype(F32)
    inverse = jnp.exp(lane * (-math.log(ROPE_BASE) / half))
    angles = lens[:, :1].astype(F32) * inverse
    trig[0] = jnp.cos(angles)
    trig[1] = jnp.sin(angles)
    places = rows * span
    col = lax.broadcasted_iota(jnp.int32, (rows, places), 1)
    row = lax.broadcasted_iota(jnp.int32, (rows, places), 0)
    slot = col - row * span
    position = slot + me_kv * span
    gap = lens[:, :1] - position
    live = (slot >= 0) & (slot < span) & (gap > 0)
    gap_f = jnp.where(live, gap, 0).astype(F32)
    for h in range(heads):
        decay_buf[h] = jnp.where(live, jnp.exp(gap_f * log_decay_ref[h]), 0.0)

    def rotate_in(front, back):
        cosine, sine = trig[0], trig[1]
        return front * cosine - back * sine, front * sine + back * cosine

    wait_in("tok", tok_buf.at[pl.ds(0, n_tp - 1)])
    squares = jnp.zeros((rows, 1), F32)
    for c in range(n_tp):
        wide_tok = tok_buf[c].astype(F32)
        squares = squares + jnp.sum(wide_tok * wide_tok, axis=1, keepdims=True)
        cols = pl.ds(c * own_cols, own_cols)
        x_buf[:, cols] = (wide_tok * attn_gain_ref[:, cols]).astype(BF16)
    @pl.when(me_kv < n_kv - 1)
    def _():
        pl.semaphore_wait(go_sem, n_kv - 1 - me_kv)


    x = x_buf[...]
    loads["wq"].wait()

    def head_at(place):
        return ((1 - side) if place < shared else side) * shared + place % shared

    def head_cols(h):
        return pl.ds(pl.multiple_of(h * DK, DK), DK)

    def q_slot(h):
        return recv_sem.at[in_slot["q0"] + h]

    def send_q(group, peers):
        for i in range(shared):
            h = group * shared + i
            for j in peers:
                pltpu.make_async_remote_copy(
                    src_ref=q_send.at[h],
                    dst_ref=q_recv.at[h, j - 1],
                    send_sem=send_sem.at[out_slot["q"]],
                    recv_sem=q_slot(h),
                    device_id={"kv": kv_peer(j)},
                    device_id_type=pl.DeviceIdType.MESH,
                ).start()

    across = [j for j in kv_order if j >= n_kv // 2]
    beside = [j for j in kv_order if j < n_kv // 2]
    for group in (side, 1 - side):
        cols = pl.ds(pl.multiple_of(group * shared * DK, DK), shared * DK)
        q_own = jnp.dot(x, wq[:, cols], preferred_element_type=F32)
        q_full[:, cols] = q_own
        for i in range(shared):
            q_send[group * shared + i] = pack(q_own[:, i * DK : (i + 1) * DK])
        if group is side:
            send_q(side, across)
    send_q(1 - side, beside)
    send_q(1 - side, across)
    send_q(side, beside)
    for name in ("wo", "wfg", "wfu", "wfd"):
        loads[name].start()

    for name in ("wk", "wv", "wg"):
        loads[name].wait()
    for i, weight in enumerate((wv, wg)):
        for pair in range(heads // 2):
            part = jnp.dot(x, weight[:, pl.ds(pair * 2 * DK, 2 * DK)], preferred_element_type=F32)
            for k in range(2):
                vg_send[pair * 2 + k, i] = pack(part[:, k * DK : (k + 1) * DK])
    away = jnp.where(me_kv > middle, me_kv - middle - 1, middle - me_kv)

    @pl.when(jnp.logical_not(is_owner))
    def _():
        slot = jnp.where(me_core == 0, away, n_kv // 2 - 1 + away)
        where = {"kv": middle + side, "tp": first_core + 1}
        for into, group in (("vgf", far_group), ("vgn", near_group)):
            remote("vg", into, vg_send.at[group], vg_in.at[slot, group], where).start()

    key_own[...] = jnp.dot(x, wk[...], preferred_element_type=F32)

    loads["kc"].wait()
    loads["vc"].wait()

    def apart_from(oi):
        both = [partner(me_kv, middle + i, n_kv) for i in range(2)]
        return jnp.where(oi == 1, both[1], both[0])

    def owner_slot(oi):
        apart = apart_from(oi)
        return jnp.where(me_core == 0, me_kv, n_kv - 1 + apart)

    def to_owner(oi, copies):
        @pl.when(jnp.logical_not((me_core == 1) & (me_kv == middle + oi)))
        def _():
            for kind, src, dst in copies:
                where = {"kv": middle + oi, "tp": first_core + 1}
                remote(f"{kind}{oi}", kind, src, dst, where).start()

    own_scores = []
    for place in range(heads):
        h = head_at(place)
        cols = head_cols(h)
        pltpu.make_async_remote_copy(
            src_ref=q_recv.at[h],
            dst_ref=q_recv.at[h],
            send_sem=send_sem.at[out_slot["q"]],
            recv_sem=q_slot(h),
            device_id={"kv": kv_peer(1)},
            device_id_type=pl.DeviceIdType.MESH,
        ).wait_recv()
        query = q_full[:, cols]
        for j in kv_order:
            query = query + unpack(q_recv[h, j - 1])
        front, back = rotate_in(query[:, :half], query[:, half:])
        query = jnp.concatenate([front, back], axis=1) * DK ** (-0.5)
        scores = lax.dot_general(
            query.astype(BF16),
            kc[:, :, cols].reshape(places, DK),
            (((1,), (1,)), ((), ())),
            preferred_element_type=F32,
        )
        mixing = (scores * decay_buf[h]).astype(BF16)
        cached = jnp.dot(mixing, vc[:, :, cols].reshape(places, DK), preferred_element_type=F32)
        ca_send[h] = pack(cached)
        key = key_own[:, cols]
        front, back = rotate_in(key[:, :half], key[:, half:])
        own_scores.append(
            jnp.sum(query[:, :half] * front + query[:, half:] * back, axis=1, keepdims=True)
        )
        near, hh = place // shared, place % shared
        oi = side if near else 1 - side
        copies = [(f"ca{near}", "ca", ca_send.at[h], ca_in.at[owner_slot(oi), hh])]
        if hh == shared - 1:
            sc_send[oi] = lanes_of(own_scores[near * shared :] + [squares])
            copies.append((f"sc{near}", "sc", sc_send.at[oi], sc_in.at[owner_slot(oi)]))

        def send_all():
            for out, into, src, dst in copies:
                where = {"kv": middle + oi, "tp": first_core + 1}
                remote(out, into, src, dst, where).start()

        if near:
            pl.when(jnp.logical_not(is_owner))(send_all)
        else:
            send_all()

    @pl.when(is_owner)
    def _():
        oi = me_kv - middle
        base = oi * shared
        units = [(c, hh) for c in (1, 0) for hh in range(shared)]
        slots = {0: range(n_kv), 1: range(n_kv, 2 * n_kv - 1)}
        wait_in("vgf", vg_in.at[:, pl.ds(0, shared)])
        near = {0: range(n_kv // 2), 1: range(n_kv // 2, n_kv - 1)}

        def half_sum(c, head, i):
            parts = [vg_in[k, head, i] for k in near[c]]
            if c:
                parts.append(vg_send[head, i])
            total = unpack(parts[0])
            for part in parts[1:]:
                total = total + unpack(part)
            return total

        for c, hh in units:
            for i in range(2):
                swap_send[c, hh, i] = pack(half_sum(c, shared - base + hh, i))
        for i in range(2):

            @pl.when(oi == i)
            def _():
                where = {"kv": middle + 1 - i}
                remote("swap", "swap", swap_send, swap_recv, where).start()

        wait_in("vgn", vg_in.at[:, pl.ds(0, shared)])
        sums_of = {(c, hh, i): half_sum(c, base + hh, i) for c, hh in units for i in range(2)}
        wait_in("sc", sc_in)
        lines = {}
        for c in (0, 1):
            parts = [sc_in[k] for k in slots[c]] + ([sc_send[oi]] if c else [])
            lines[c] = functools.reduce(lambda p, q: p + q, parts)
        factor = lax.rsqrt(column_of(lines[1], shared) / D + RMS_EPS)
        cubed = factor * factor * factor
        weights = {u: column_of(lines[u[0]], u[1]) * cubed for u in units}
        wait_in("swap", swap_recv)
        gates, news = {}, {}
        for c, hh in units:
            both = [sums_of[c, hh, i] + unpack(swap_recv[c, hh, i]) for i in range(2)]
            news[c, hh] = weights[c, hh] * both[0]
            gate = both[1] * factor
            gates[c, hh] = gate / (1.0 + jnp.exp(-gate))
        wait_in("ca", ca_in)
        totals = {}
        for c, hh in units:
            parts = [ca_in[k, hh] for k in slots[c]] + ([ca_send[base + hh]] if c else [])
            total = unpack(parts[0])
            for part in parts[1:]:
                total = total + unpack(part)
            totals[c, hh] = total * factor + news[c, hh]
        sums = {u: jnp.sum(totals[u], axis=1, keepdims=True) for u in units}
        squared = {u: jnp.sum(totals[u] * totals[u], axis=1, keepdims=True) for u in units}
        for c, hh in units:
            center = sums[c, hh] / DK
            spread = squared[c, hh] / DK - center * center
            normed = (totals[c, hh] - center) * lax.rsqrt(spread + GN_EPS)
            result = pack(gates[c, hh] * normed)
            gt_send[c, hh] = result
            if c:
                gt_buf[oi, hh] = result
        for c in (0, 1):
            for j in kv_order + ((0,) if c == 0 else ()):
                where = {"kv": kv_peer(j) if j else me_kv, "tp": first_core + c}
                for i in range(2):

                    @pl.when(oi == i)
                    def _():
                        remote("gt", f"gt{i}", gt_send.at[c], gt_buf.at[i], where).start()

    loads["wo"].wait()
    loads["gg"].wait()
    for i in range(2):

        @pl.when(jnp.logical_not((me_core == 1) & (me_kv == middle + i)))
        def _():
            wait_in(f"gt{i}", gt_buf.at[i])

    for h in range(heads):
        cols = pl.ds(h * DK, DK)
        x_buf[:, cols] = (
            unpack(gt_buf[h // shared, h % shared]) * gn_gain_ref[:, cols]
        ).astype(BF16)
    gated = x_buf[...]

    def o_send(part, core):
        mine = o_buf.at[part, me_tp]
        if core is None:
            remote("o", f"o{part}", mine, mine, {"tp": tp_peer(1)}).start()
        else:
            for chip in range(n_tp // 2 - 1, 0, -1):
                target = partner(first_core, 2 * chip, n_tp) + core
                remote("o", f"o{part}", mine, mine, {"tp": target}).start()

    for part in range(2):
        width = depth // 2
        piece = jnp.dot(gated, wo[:, pl.ds(part * width, width)], preferred_element_type=F32)
        o_buf[part, me_tp] = pack(piece)
        o_send(part, 0)
    for part in range(2):
        o_send(part, 1)
    for part in range(2):
        o_send(part, None)
    loads["fg"].wait()
    for part in range(2):
        wait_in(f"o{part}", o_buf.at[part, pl.ds(0, n_tp - 1)])
    squares = jnp.zeros((rows, 1), F32)
    halves = []
    for part in range(2):
        total = unpack(o_buf[part, 0])
        for t in range(1, n_tp):
            total = total + unpack(o_buf[part, t])
        halves.append(total)
    mixed = jnp.concatenate(halves, axis=1)
    for c in range(n_tp):
        cols = pl.ds(c * own_cols, own_cols)
        own_mixed = mixed[:, c * own_cols : (c + 1) * own_cols]
        resid = (tok_buf[c].astype(F32) + own_mixed).astype(BF16)
        resid_wide = resid.astype(F32)
        resid_buf[c] = resid_wide
        squares = squares + jnp.sum(resid_wide * resid_wide, axis=1, keepdims=True)
        x_buf[:, cols] = (resid_wide * ffn_gain_ref[:, cols]).astype(BF16)
    sqm_send[...] = lanes_of([squares])
    for j in kv_order:
        remote("sqm", "sqm", sqm_send, sqm_recv.at[j - 1], {"kv": kv_peer(j)}).start()

    x = x_buf[...]
    loads["wfg"].wait()
    loads["wfu"].wait()

    def stage_start(s, index):
        return pl.multiple_of((s * n_kv + index) * win, win)

    for s in range(n_full):
        for j in kv_order:
            cols = pl.ds(stage_start(s, kv_peer(j)), win)
            for i, weight in enumerate((wfg, wfu)):
                part = jnp.dot(x, weight[:, cols], preferred_element_type=F32)
                gu_send[s, j - 1, i] = pack(part)
            remote(
                "gu", f"gu{s}", gu_send.at[s, j - 1], gu_recv.at[s, j - 1], {"kv": kv_peer(j)}
            ).start()
    if rest:
        cols = pl.ds(rest_base, rest * LANES)
        both = [jnp.dot(x, w[:, cols], preferred_element_type=F32) for w in (wfg, wfu)]
        width = rest_tiles * LANES
        for o in range(2):
            mine = jnp.concatenate([b[:, o * width : (o + 1) * width] for b in both], axis=1)
            rest_send[o] = stack(mine, 2 * rest_tiles)
        for o in range(2):

            to_owner(o, [("rest", rest_send.at[o], rest_recv.at[owner_slot(o)])])

    for s in range(n_full):
        cols = pl.ds(stage_start(s, me_kv), win)
        for i, weight in enumerate((wfg, wfu)):
            gu_own[s, i] = jnp.dot(x, weight[:, cols], preferred_element_type=F32)

    wait_in("sqm", sqm_recv)
    total_sq = sqm_send[...]
    for j in range(1, n_kv):
        total_sq = total_sq + sqm_recv[j - 1]
    factor = lax.rsqrt(column_of(total_sq, 0) / D + RMS_EPS)

    def activate(gate, up):
        gate, up = gate * factor, up * factor
        return gate / (1.0 + jnp.exp(-gate)) * up

    for s in range(n_full):
        wait_in(f"gu{s}", gu_recv.at[s])
        both = []
        for i in range(2):
            total = gu_own[s, i]
            for j in kv_order:
                total = total + unpack(gu_recv[s, j - 1, i])
            both.append(total)
        hid_send[s] = pack(activate(*both))
        for j in kv_order:
            remote(
                "hid", f"hid{s}", hid_send.at[s], hid_recv.at[s, j - 1], {"kv": kv_peer(j)}
            ).start()

    if rest:

        @pl.when(is_owner)
        def _():
            o = me_kv - middle
            wait_in("rest", rest_recv)
            width = rest_tiles * LANES
            for c in (0, 1):
                slots = range(n_kv) if c == 0 else range(n_kv, 2 * n_kv - 1)
                parts = [rest_recv[k] for k in slots] + ([rest_send[o]] if c else [])
                total = unstack(parts[0], 2 * rest_tiles)
                for part in parts[1:]:
                    total = total + unstack(part, 2 * rest_tiles)
                result = stack(activate(total[:, :width], total[:, width:]), rest_tiles)
                rest_out[c] = result
                if c:
                    rest_hid[o] = result
                for j in kv_order + ((0,) if c == 0 else ()):
                    where = {"kv": kv_peer(j) if j else me_kv, "tp": first_core + c}
                    for i in range(2):

                        @pl.when(o == i)
                        def _():
                            remote(
                                "rhid", f"rhid{i}", rest_out.at[c], rest_hid.at[i], where
                            ).start()

    loads["wfd"].wait()

    def down_of(s, index, packed):
        weight = wfd[pl.ds(stage_start(s, index), win), :]
        return jnp.dot(unpack(packed).astype(BF16), weight, preferred_element_type=F32)

    down = None
    for s in range(n_full):
        part = down_of(s, me_kv, hid_send[s])
        down = part if down is None else down + part
    for s in range(n_full):
        wait_in(f"hid{s}", hid_recv.at[s])
        for j in range(1, n_kv):
            down = down + down_of(s, kv_peer(j), hid_recv[s, j - 1])
    if rest:
        near = jnp.where(me_kv > middle, 1, 0)
        width = rest_tiles * LANES
        for o in (near, 1 - near):

            @pl.when(jnp.logical_not((me_core == 1) & (me_kv == middle + o)))
            def _():
                for i in range(2):

                    @pl.when(o == i)
                    def _():
                        wait_in(f"rhid{i}", rest_hid.at[i])

            chunk = unstack(rest_hid[o], rest_tiles).astype(BF16)
            first = pl.multiple_of(rest_base + o * width, LANES)
            weight = wfd[pl.ds(first, width), :]
            down = down + jnp.dot(chunk, weight, preferred_element_type=F32)
    down_buf[...] = down
    for t in range(n_tp):
        d_send[t] = pack(down_buf[:, pl.ds(t * own_cols, own_cols)])
    to_tp("d", "d", lambda target: d_send.at[target], d_recv.at[me_tp])
    own = pl.ds(pl.multiple_of(me_tp * own_cols, own_cols), own_cols)
    result = down_buf[:, own] + resid_buf[me_tp]
    wait_in("d", d_recv.at[pl.ds(0, n_tp - 1)])
    for j in range(1, n_tp):
        result = result + unpack(d_recv[tp_peer(j)])
    out_ref[...] = result.astype(BF16)
    wait_out("tok", tok_buf.at[pl.ds(0, n_tp - 1)])
    wait_out("q", q_recv)
    wait_out("o", o_buf.at[:, pl.ds(0, n_tp - 1)])
    wait_out("sqm", sqm_recv)
    wait_out("gu", gu_recv)
    wait_out("hid", hid_recv)
    wait_out("d", d_recv.at[pl.ds(0, n_tp - 1)])
    for i in range(2):

        @pl.when(jnp.logical_not((me_core == 1) & (me_kv == middle + i)))
        def _():
            if rest:
                wait_out(f"rest{i}", rest_send.at[i])

    wait_out("ca0", ca_send.at[far_group])
    wait_out("sc0", sc_send.at[0])

    @pl.when(jnp.logical_not(is_owner))
    def _():
        wait_out("ca1", ca_send.at[near_group])
        wait_out("sc1", sc_send.at[0])

    @pl.when(jnp.logical_not(is_owner))
    def _():
        wait_out("vg", vg_send)

    @pl.when(is_owner)
    def _():
        wait_out("gt", ca_in)
        wait_out("swap", swap_send)
        if rest:
            wait_out("rhid", rest_hid)


def fused(
    n_kv,
    n_tp,
    tokens,
    lengths,
    attn_gain,
    w_query,
    w_key,
    w_value,
    w_gate,
    log_decay,
    key_cache,
    value_cache,
    gn_gain,
    w_out,
    ffn_gain,
    w_ffn_gate,
    w_ffn_up,
    w_ffn_down,
):
    rows, own_cols = tokens.shape
    depth, wide = w_query.shape
    span = key_cache.shape[1]
    heads = log_decay.shape[0]
    shared = heads // 2
    win = STAGE_TILES * LANES
    n_full, rest = plan(w_ffn_gate.shape[1] // LANES, n_kv)
    rest_rows = max(rest // 2, 1) * rows
    peers = n_kv - 1
    vmem = pl.BlockSpec(memory_space=pltpu.VMEM)
    hbm = pl.BlockSpec(memory_space=pl.ANY)
    small = (
        tokens,
        lengths,
        attn_gain[None, :],
        log_decay,
        gn_gain[None, :],
        ffn_gain[None, :],
    )
    streamed = (
        w_query,
        w_key,
        w_value,
        w_gate,
        key_cache,
        value_cache,
        w_out,
        w_ffn_gate,
        w_ffn_up,
        w_ffn_down,
    )
    scratch = [pltpu.VMEM(a.shape, a.dtype) for a in streamed] + [
        (pltpu.SMEM if a.ndim == 1 else pltpu.VMEM)(a.shape, a.dtype) for a in small
    ]
    piece = (2 * rows, DK // 2)
    scratch += [
        pltpu.VMEM((n_tp, rows, own_cols), BF16),
        pltpu.VMEM((rows, depth), BF16),
        pltpu.VMEM((heads, *piece), BF16),
        pltpu.VMEM((heads, peers, *piece), BF16),
        pltpu.VMEM((rows, wide), F32),
        pltpu.VMEM((2, rows, DK // 2), F32),
        pltpu.VMEM((heads, rows, rows * span), F32),
        pltpu.VMEM((rows, wide), F32),
        pltpu.VMEM((heads, 2, *piece), BF16),
        pltpu.VMEM((peers, heads, 2, *piece), BF16),
        pltpu.VMEM((2, shared, 2, *piece), BF16),
        pltpu.VMEM((2, shared, 2, *piece), BF16),
        pltpu.VMEM((heads, *piece), BF16),
        pltpu.VMEM((2 * n_kv - 1, shared, *piece), BF16),
        pltpu.VMEM((2, 1, LANES), F32),
        pltpu.VMEM((2 * n_kv - 1, 1, LANES), F32),
        pltpu.VMEM((2, shared, *piece), BF16),
        pltpu.VMEM((2, shared, *piece), BF16),
        pltpu.VMEM((2, n_tp, 2 * rows, depth // 4), BF16),
        pltpu.VMEM((n_tp, rows, own_cols), F32),
        pltpu.VMEM((1, LANES), F32),
        pltpu.VMEM((peers, 1, LANES), F32),
        pltpu.VMEM((n_full, 2, rows, win), F32),
        pltpu.VMEM((n_full, peers, 2, 2 * rows, win // 2), BF16),
        pltpu.VMEM((n_full, peers, 2, 2 * rows, win // 2), BF16),
        pltpu.VMEM((n_full, 2 * rows, win // 2), BF16),
        pltpu.VMEM((n_full, peers, 2 * rows, win // 2), BF16),
        pltpu.VMEM((2, 2 * rest_rows, LANES), BF16),
        pltpu.VMEM((2 * n_kv - 1, 2 * rest_rows, LANES), BF16),
        pltpu.VMEM((2, rest_rows, LANES), BF16),
        pltpu.VMEM((2 * n_kv - 1, rest_rows, LANES), BF16),
        pltpu.VMEM((rows, depth), F32),
        pltpu.VMEM((n_tp, 2 * rows, own_cols // 2), BF16),
        pltpu.VMEM((n_tp, 2 * rows, own_cols // 2), BF16),
        pltpu.SemaphoreType.DMA((len(small) + len(streamed),)),
        pltpu.SemaphoreType.DMA((17,)),
        pltpu.SemaphoreType.DMA((15 + heads + 2 * n_full,)),
        pltpu.SemaphoreType.REGULAR,
    ]
    return pl.pallas_call(
        functools.partial(layer_kernel, n_kv, n_tp),
        out_shape=pltpu.VMEM((rows, own_cols), BF16),
        in_specs=[hbm] * (len(small) + len(streamed)),
        out_specs=vmem,
        scratch_shapes=scratch,
        compiler_params=pltpu.CompilerParams(
            collective_id=0, has_side_effects=True, vmem_limit_bytes=60 * 1024 * 1024
        ),
    )(*small, *streamed)


def fits(mesh, tokens, log_decay, key_cache, w_query, w_ffn_gate):
    n_kv, n_tp, n_grp = mesh.shape["kv"], mesh.shape["tp"], mesh.shape["grp"]
    heads, span = log_decay.shape[0], key_cache.shape[1] // n_kv
    tiles = w_ffn_gate.shape[1] // n_tp // LANES
    rows = tokens.shape[0] // n_grp
    return (
        n_kv > 1
        and n_tp > 2
        and n_kv & (n_kv - 1) == 0
        and n_tp & (n_tp - 1) == 0
        and heads == n_kv * n_tp
        and (heads // n_tp // 2 + 1) * rows <= LANES
        and tokens.shape[1] // n_kv == heads * DK // n_tp
        and tokens.shape[1] % (n_kv * n_tp * 2 * LANES) == 0
        and heads * DK // n_tp % (4 * LANES) == 0
        and w_ffn_gate.shape[1] % (n_tp * LANES) == 0
        and plan(tiles, n_kv)[0] > 0
        and plan(tiles, n_kv)[1] % 2 == 0
        and n_kv > 2
        and tokens.shape[0] // n_grp % 8 == 0
        and span % 16 == 0
        and span <= 64
    )


def solution(mesh):
    specs = (
        P("grp", ("kv", "tp")),
        P("grp"),
        P("kv"),
        P("kv", "tp"),
        P("kv", "tp"),
        P("kv", "tp"),
        P("kv", "tp"),
        P("tp"),
        P("grp", "kv", "tp"),
        P("grp", "kv", "tp"),
        P("tp"),
        P("tp", "kv"),
        P("kv"),
        P("kv", "tp"),
        P("kv", "tp"),
        P("tp", "kv"),
    )

    def whole(*arrays):
        tokens, w_query, log_decay, key_cache = arrays[0], arrays[3], arrays[7], arrays[8]
        if fits(mesh, tokens, log_decay, key_cache, w_query, arrays[13]):
            body = functools.partial(fused, mesh.shape["kv"], mesh.shape["tp"])
        else:
            body = local
        return jax.shard_map(
            body,
            mesh=mesh,
            in_specs=specs,
            out_specs=P("grp", ("kv", "tp")),
            check_vma=False,
        )(*arrays)

    return whole
```

```python
import functools
import math

import jax
import jax.numpy as jnp
from jax import lax
from jax.experimental import pallas as pl
from jax.experimental.pallas import tpu as pltpu
from jax.sharding import PartitionSpec as P

DK = 256
D = 4096


RMS_EPS = 0.1
GN_EPS = 1.0
ROPE_BASE = 10000.0


def rotate(vectors, positions):
    half_dim = vectors.shape[-1] // 2
    inverse = ROPE_BASE ** (-jnp.arange(half_dim, dtype=jnp.float32) / half_dim)
    angles = positions[:, None, None] * inverse[None, None, :]
    cosine = jnp.cos(angles)
    sine_part = jnp.sin(angles)
    front_part = vectors[..., :half_dim]
    back_part = vectors[..., half_dim:]
    return jnp.concatenate(
        [front_part * cosine - back_part * sine_part, front_part * sine_part + back_part * cosine],
        axis=-1,
    )


def group_norm(totals, gn_gain):
    width = totals.shape[-1]
    center = jnp.sum(totals, axis=-1, keepdims=True) / width
    spread = jnp.sum(totals * totals, axis=-1, keepdims=True) / width - center * center
    normed = (totals - center) * lax.rsqrt(spread + GN_EPS)
    return normed.reshape(normed.shape[0], -1) * gn_gain


def channel_stat(own_squares):
    return lax.psum(own_squares, "kv")


def input_stat(own_squares):
    return lax.psum(own_squares, "kv")


def cache_partial(query_low, lengths, log_decay, key_cache, value_cache, heads_here):
    batch_rows = query_low.shape[0]
    span = key_cache.shape[1]
    slots = lax.axis_index("kv") * span + jnp.arange(span, dtype=jnp.int32)
    live = slots[None, :] < lengths[:, None]
    gaps = jnp.maximum((lengths[:, None] - slots[None, :]).astype(jnp.float32), 0.0)
    decays = jnp.exp(log_decay[None, None, :] * gaps[:, :, None])
    keys_here = key_cache.reshape(batch_rows, span, heads_here, DK)
    values_here = value_cache.reshape(batch_rows, span, heads_here, DK)
    scores = jnp.einsum("bphd,bhd->bph", keys_here, query_low, preferred_element_type=jnp.float32)
    mixing = jnp.where(live[:, :, None], scores * decays, 0.0).astype(jnp.bfloat16)
    return jnp.einsum("bph,bphd->bhd", mixing, values_here, preferred_element_type=jnp.float32)


def local(
    tokens,
    lengths,
    attn_gain,
    w_query,
    w_key,
    w_value,
    w_gate,
    log_decay,
    key_cache,
    value_cache,
    gn_gain,
    w_out,
    ffn_gain,
    w_ffn_gate,
    w_ffn_up,
    w_ffn_down,
):
    batch_rows = tokens.shape[0]
    heads_here = log_decay.shape[0]
    row_block = lax.all_gather(tokens, "tp", axis=1, tiled=True)
    widened = row_block.astype(jnp.float32)
    own_squares = jnp.sum(widened * widened, axis=1)
    scaled = (widened * attn_gain).astype(jnp.bfloat16)
    part_query = jnp.dot(scaled, w_query, preferred_element_type=jnp.float32)
    part_key = jnp.dot(scaled, w_key, preferred_element_type=jnp.float32)
    part_value = jnp.dot(scaled, w_value, preferred_element_type=jnp.float32)
    part_gate = jnp.dot(scaled, w_gate, preferred_element_type=jnp.float32)
    positions = lengths.astype(jnp.float32)
    total_squares = input_stat(own_squares)
    queries, new_keys, new_values, gates = lax.psum(
        (part_query, part_key, part_value, part_gate), "kv"
    )
    factor = lax.rsqrt(total_squares / D + RMS_EPS)[:, None]
    queries = rotate((queries * factor).reshape(batch_rows, heads_here, DK), positions) * DK ** (
        -0.5
    )
    new_keys = rotate((new_keys * factor).reshape(batch_rows, heads_here, DK), positions)
    new_values = (new_values * factor).reshape(batch_rows, heads_here, DK)
    gates = gates * factor
    query_low = queries.astype(jnp.bfloat16)
    partial_value = cache_partial(query_low, lengths, log_decay, key_cache, value_cache, heads_here)
    cached = lax.psum(partial_value.reshape(batch_rows, heads_here * DK), "kv")
    own_term = jnp.sum(queries * new_keys, axis=-1, keepdims=True) * new_values
    normed = group_norm(cached.reshape(batch_rows, heads_here, DK) + own_term, gn_gain)
    gated = (jax.nn.silu(gates) * normed).astype(jnp.bfloat16)
    out_partial = jnp.dot(gated, w_out, preferred_element_type=jnp.float32)
    mixed = lax.psum_scatter(out_partial, "tp", scatter_dimension=1, tiled=True)
    resid = (tokens.astype(jnp.float32) + mixed).astype(jnp.bfloat16)
    resid_block = lax.all_gather(resid, "tp", axis=1, tiled=True).astype(jnp.float32)
    mid_squares = jnp.sum(resid_block * resid_block, axis=1)
    scaled_mid = (resid_block * ffn_gain).astype(jnp.bfloat16)
    gate_part = jnp.dot(scaled_mid, w_ffn_gate, preferred_element_type=jnp.float32)
    up_part = jnp.dot(scaled_mid, w_ffn_up, preferred_element_type=jnp.float32)
    total_mid = channel_stat(mid_squares)
    gate_sum, up_sum = lax.psum((gate_part, up_part), "kv")
    factor_mid = lax.rsqrt(total_mid / D + RMS_EPS)[:, None]
    hidden = (jax.nn.silu(gate_sum * factor_mid) * (up_sum * factor_mid)).astype(jnp.bfloat16)
    down_partial = jnp.dot(hidden, w_ffn_down, preferred_element_type=jnp.float32)
    down = lax.psum_scatter(down_partial, "tp", scatter_dimension=1, tiled=True)
    return (resid.astype(jnp.float32) + down).astype(jnp.bfloat16)


LANES = 128
STAGE_TILES = 2
F32 = jnp.float32
BF16 = jnp.bfloat16


def partner(index, j, parts):
    found, bit = 0, 1
    while bit < parts:
        digit = (index // bit) % 2
        found = found + bit * ((1 - digit) if (j // bit) % 2 else digit)
        bit *= 2
    return found


def stack(value, pieces):
    width = value.shape[1] // pieces
    return jnp.concatenate(
        [value[:, i * width : (i + 1) * width] for i in range(pieces)], axis=0
    ).astype(BF16)


def unstack(packed, pieces):
    wide = packed.astype(F32)
    rows = wide.shape[0] // pieces
    return jnp.concatenate([wide[i * rows : (i + 1) * rows] for i in range(pieces)], axis=1)


def pack(value):
    return stack(value, 2)


def unpack(packed):
    return unstack(packed, 2)


def plan(tiles, n_kv):
    step = STAGE_TILES * n_kv
    return tiles // step, tiles % step


def layer_kernel(
    n_kv,
    n_tp,
    tokens_hbm,
    lengths_hbm,
    attn_gain_hbm,
    log_decay_hbm,
    gn_gain_hbm,
    ffn_gain_hbm,
    wq_hbm,
    wk_hbm,
    wv_hbm,
    wg_hbm,
    kc_hbm,
    vc_hbm,
    wo_hbm,
    wfg_hbm,
    wfu_hbm,
    wfd_hbm,
    out_ref,
    wq,
    wk,
    wv,
    wg,
    kc,
    vc,
    wo,
    wfg,
    wfu,
    wfd,
    tokens_ref,
    lengths_ref,
    attn_gain_ref,
    log_decay_ref,
    gn_gain_ref,
    ffn_gain_ref,
    tok_buf,
    x_buf,
    q_send,
    q_recv,
    q_full,
    trig,
    decay_buf,
    key_own,
    vg_send,
    vg_in,
    swap_send,
    swap_recv,
    ca_send,
    ca_in,
    sc_send,
    sc_in,
    gt_send,
    gt_buf,
    o_buf,
    resid_buf,
    sqm_send,
    sqm_recv,
    gu_own,
    gu_send,
    gu_recv,
    hid_send,
    hid_recv,
    rest_send,
    rest_recv,
    rest_out,
    rest_hid,
    down_buf,
    d_send,
    d_recv,
    load_sem,
    send_sem,
    recv_sem,
    go_sem,
):
    rows, own_cols = tokens_ref.shape
    depth, wide = wq.shape
    span = kc.shape[1]
    half = DK // 2
    tiles = wfg.shape[1] // LANES
    win = STAGE_TILES * LANES
    n_full, rest = plan(tiles, n_kv)
    rest_tiles = rest // 2
    rest_base = n_full * STAGE_TILES * n_kv * LANES
    heads = n_kv
    middle = n_kv // 2 - 1
    shared = heads // 2
    me_kv = lax.axis_index("kv")
    me_tp = lax.axis_index("tp")
    me_core = me_tp % 2
    first_core = me_tp - me_core
    is_middle = (me_kv >= middle) & (me_kv < middle + 2)
    is_owner = (me_core == 1) & is_middle
    side = jnp.where(me_kv > middle, 1, 0)
    far_group = pl.ds((1 - side) * shared, shared)
    near_group = pl.ds(side * shared, shared)

    def kv_peer(j):
        return partner(me_kv, j, n_kv)

    def tp_peer(j):
        return partner(me_tp, j, n_tp)

    kv_order = tuple(range(n_kv - 1, 0, -1))

    barrier = pltpu.get_barrier_semaphore()
    for j in range(1, n_tp):
        pl.semaphore_signal(
            barrier, inc=1, device_id={"tp": tp_peer(j)}, device_id_type=pl.DeviceIdType.MESH
        )
    for k in range(1, n_kv):

        @pl.when(me_kv < k)
        def _():
            pl.semaphore_signal(
                barrier, inc=1, device_id={"kv": k}, device_id_type=pl.DeviceIdType.MESH
            )

    loads = {}
    for slot, (name, src, dst) in enumerate(
        (
            ("tok", tokens_hbm, tokens_ref),
            ("len", lengths_hbm, lengths_ref),
            ("ag", attn_gain_hbm, attn_gain_ref),
            ("ld", log_decay_hbm, log_decay_ref),
            ("gg", gn_gain_hbm, gn_gain_ref),
            ("fg", ffn_gain_hbm, ffn_gain_ref),
            ("wq", wq_hbm, wq),
            ("kc", kc_hbm, kc),
            ("vc", vc_hbm, vc),
            ("wk", wk_hbm, wk),
            ("wv", wv_hbm, wv),
            ("wg", wg_hbm, wg),
            ("wo", wo_hbm, wo),
            ("wfg", wfg_hbm, wfg),
            ("wfu", wfu_hbm, wfu),
            ("wfd", wfd_hbm, wfd),
        )
    ):
        loads[name] = pltpu.make_async_copy(src, dst, load_sem.at[slot])

    names = ["tok", "q", "o", "sqm", "gu", "hid", "d", "gt", "rhid"]
    names += [f"{kind}{i}" for kind in ("ca", "sc", "rest") for i in range(2)]
    names += ["vg", "swap"]
    out_slot = {name: i for i, name in enumerate(names)}
    names = ["tok", "vgf", "vgn", "swap", "ca", "sc", "gt0", "gt1", "o0", "o1", "sqm", "d"]
    names += [f"q{h}" for h in range(heads)] + ["rest", "rhid0", "rhid1"]
    names += [f"{kind}{i}" for kind in ("gu", "hid") for i in range(n_full)]
    in_slot = {name: i for i, name in enumerate(names)}

    def remote(out, into, src, dst, where):
        return pltpu.make_async_remote_copy(
            src_ref=src,
            dst_ref=dst,
            send_sem=send_sem.at[out_slot[out]],
            recv_sem=recv_sem.at[in_slot[into]],
            device_id=where,
            device_id_type=pl.DeviceIdType.MESH,
        )

    def wait_in(into, ref):
        remote("tok", into, ref, ref, {"kv": kv_peer(1)}).wait_recv()

    def wait_out(out, ref):
        remote(out, "tok", ref, ref, {"kv": kv_peer(1)}).wait_send()

    def to_tp(out, into, src_of, dst):
        for chip in range(n_tp // 2 - 1, 0, -1):
            for core in (0, 1):
                target = partner(first_core, 2 * chip, n_tp) + core
                remote(out, into, src_of(target), dst, {"tp": target}).start()
        remote(out, into, src_of(tp_peer(1)), dst, {"tp": tp_peer(1)}).start()

    lane_id = lax.broadcasted_iota(jnp.int32, (8, LANES), 1)
    row_of = lax.broadcasted_iota(jnp.int32, (8, LANES), 0)

    def lanes_of(columns):
        spread = jnp.zeros((8, LANES), F32)
        for i, column in enumerate(columns):
            for first in range(0, rows, 8):
                part = jnp.broadcast_to(column[first : first + 8], (8, LANES))
                spread = jnp.where(lane_id == row_of + (i * rows + first), part, spread)
        return jnp.sum(spread, axis=0, keepdims=True)

    def column_of(line, i):
        wide_line = jnp.broadcast_to(line, (8, LANES))
        return jnp.concatenate(
            [
                jnp.sum(
                    jnp.where(lane_id == row_of + (i * rows + first), wide_line, 0.0),
                    axis=1,
                    keepdims=True,
                )
                for first in range(0, rows, 8)
            ],
            axis=0,
        )

    for name in ("tok", "len", "ld", "ag", "wq"):
        loads[name].start()
    pl.semaphore_wait(barrier, n_tp - 1 + me_kv)
    for k in range(n_kv - 1):

        @pl.when(me_kv > k)
        def _():
            pl.semaphore_signal(
                go_sem, inc=1, device_id={"kv": k}, device_id_type=pl.DeviceIdType.MESH
            )

    loads["tok"].wait()
    to_tp("tok", "tok", lambda target: tokens_ref, tok_buf.at[me_tp])
    for name in ("wk", "wv", "wg", "kc", "vc", "gg", "fg"):
        loads[name].start()
    tok_buf[me_tp] = tokens_ref[...]

    for name in ("len", "ld", "ag"):
        loads[name].wait()
    row_id = lax.broadcasted_iota(jnp.int32, (rows, LANES), 0)
    lens = jnp.zeros((rows, LANES), jnp.int32)
    for b in range(rows):
        lens = jnp.where(row_id == b, lengths_ref[b], lens)
    lane = lax.broadcasted_iota(jnp.int32, (rows, half), 1).astype(F32)
    inverse = jnp.exp(lane * (-math.log(ROPE_BASE) / half))
    angles = lens[:, :1].astype(F32) * inverse
    trig[0] = jnp.cos(angles)
    trig[1] = jnp.sin(angles)
    places = rows * span
    col = lax.broadcasted_iota(jnp.int32, (rows, places), 1)
    row = lax.broadcasted_iota(jnp.int32, (rows, places), 0)
    slot = col - row * span
    position = slot + me_kv * span
    gap = lens[:, :1] - position
    live = (slot >= 0) & (slot < span) & (gap > 0)
    gap_f = jnp.where(live, gap, 0).astype(F32)
    for h in range(heads):
        decay_buf[h] = jnp.where(live, jnp.exp(gap_f * log_decay_ref[h]), 0.0)

    def rotate_in(front, back):
        cosine, sine = trig[0], trig[1]
        return front * cosine - back * sine, front * sine + back * cosine

    wait_in("tok", tok_buf.at[pl.ds(0, n_tp - 1)])
    squares = jnp.zeros((rows, 1), F32)
    for c in range(n_tp):
        wide_tok = tok_buf[c].astype(F32)
        squares = squares + jnp.sum(wide_tok * wide_tok, axis=1, keepdims=True)
        cols = pl.ds(c * own_cols, own_cols)
        x_buf[:, cols] = (wide_tok * attn_gain_ref[:, cols]).astype(BF16)
    @pl.when(me_kv < n_kv - 1)
    def _():
        pl.semaphore_wait(go_sem, n_kv - 1 - me_kv)


    x = x_buf[...]
    loads["wq"].wait()

    def head_at(place):
        return ((1 - side) if place < shared else side) * shared + place % shared

    def head_cols(h):
        return pl.ds(pl.multiple_of(h * DK, DK), DK)

    def q_slot(h):
        return recv_sem.at[in_slot["q0"] + h]

    def send_q(group, peers):
        for i in range(shared):
            h = group * shared + i
            for j in peers:
                pltpu.make_async_remote_copy(
                    src_ref=q_send.at[h],
                    dst_ref=q_recv.at[h, j - 1],
                    send_sem=send_sem.at[out_slot["q"]],
                    recv_sem=q_slot(h),
                    device_id={"kv": kv_peer(j)},
                    device_id_type=pl.DeviceIdType.MESH,
                ).start()

    across = [j for j in range(1, n_kv) if j >= n_kv // 2]
    beside = [j for j in kv_order if j < n_kv // 2]
    for group in (side, 1 - side):
        cols = pl.ds(pl.multiple_of(group * shared * DK, DK), shared * DK)
        q_own = jnp.dot(x, wq[:, cols], preferred_element_type=F32)
        q_full[:, cols] = q_own
        for i in range(shared):
            q_send[group * shared + i] = pack(q_own[:, i * DK : (i + 1) * DK])
        if group is side:
            send_q(side, across)
    send_q(1 - side, beside)
    send_q(1 - side, across)
    send_q(side, beside)
    for name in ("wo", "wfg", "wfu", "wfd"):
        loads[name].start()

    for name in ("wk", "wv", "wg"):
        loads[name].wait()
    for i, weight in enumerate((wv, wg)):
        for pair in range(heads // 2):
            part = jnp.dot(x, weight[:, pl.ds(pair * 2 * DK, 2 * DK)], preferred_element_type=F32)
            for k in range(2):
                vg_send[pair * 2 + k, i] = pack(part[:, k * DK : (k + 1) * DK])
    away = jnp.where(me_kv > middle, me_kv - middle - 1, middle - me_kv)

    @pl.when(jnp.logical_not(is_owner))
    def _():
        slot = jnp.where(me_core == 0, away, n_kv // 2 - 1 + away)
        where = {"kv": middle + side, "tp": first_core + 1}
        for into, group in (("vgf", far_group), ("vgn", near_group)):
            remote("vg", into, vg_send.at[group], vg_in.at[slot, group], where).start()

    key_own[...] = jnp.dot(x, wk[...], preferred_element_type=F32)

    loads["kc"].wait()
    loads["vc"].wait()

    def apart_from(oi):
        both = [partner(me_kv, middle + i, n_kv) for i in range(2)]
        return jnp.where(oi == 1, both[1], both[0])

    def owner_slot(oi):
        apart = apart_from(oi)
        return jnp.where(me_core == 0, me_kv, n_kv - 1 + apart)

    def to_owner(oi, copies):
        @pl.when(jnp.logical_not((me_core == 1) & (me_kv == middle + oi)))
        def _():
            for kind, src, dst in copies:
                where = {"kv": middle + oi, "tp": first_core + 1}
                remote(f"{kind}{oi}", kind, src, dst, where).start()

    own_scores = []
    for place in range(heads):
        h = head_at(place)
        cols = head_cols(h)
        pltpu.make_async_remote_copy(
            src_ref=q_recv.at[h],
            dst_ref=q_recv.at[h],
            send_sem=send_sem.at[out_slot["q"]],
            recv_sem=q_slot(h),
            device_id={"kv": kv_peer(1)},
            device_id_type=pl.DeviceIdType.MESH,
        ).wait_recv()
        query = q_full[:, cols]
        for j in kv_order:
            query = query + unpack(q_recv[h, j - 1])
        front, back = rotate_in(query[:, :half], query[:, half:])
        query = jnp.concatenate([front, back], axis=1) * DK ** (-0.5)
        scores = lax.dot_general(
            query.astype(BF16),
            kc[:, :, cols].reshape(places, DK),
            (((1,), (1,)), ((), ())),
            preferred_element_type=F32,
        )
        mixing = (scores * decay_buf[h]).astype(BF16)
        cached = jnp.dot(mixing, vc[:, :, cols].reshape(places, DK), preferred_element_type=F32)
        ca_send[h] = pack(cached)
        key = key_own[:, cols]
        front, back = rotate_in(key[:, :half], key[:, half:])
        own_scores.append(
            jnp.sum(query[:, :half] * front + query[:, half:] * back, axis=1, keepdims=True)
        )
        near, hh = place // shared, place % shared
        oi = side if near else 1 - side
        copies = [(f"ca{near}", "ca", ca_send.at[h], ca_in.at[owner_slot(oi), hh])]
        if hh == shared - 1:
            sc_send[oi] = lanes_of(own_scores[near * shared :] + [squares])
            copies.append((f"sc{near}", "sc", sc_send.at[oi], sc_in.at[owner_slot(oi)]))

        def send_all():
            for out, into, src, dst in copies:
                where = {"kv": middle + oi, "tp": first_core + 1}
                remote(out, into, src, dst, where).start()

        if near:
            pl.when(jnp.logical_not(is_owner))(send_all)
        else:
            send_all()

    @pl.when(is_owner)
    def _():
        oi = me_kv - middle
        base = oi * shared
        units = [(c, hh) for c in (1, 0) for hh in range(shared)]
        slots = {0: range(n_kv), 1: range(n_kv, 2 * n_kv - 1)}
        wait_in("vgf", vg_in.at[:, pl.ds(0, shared)])
        near = {0: range(n_kv // 2), 1: range(n_kv // 2, n_kv - 1)}

        def half_sum(c, head, i):
            parts = [vg_in[k, head, i] for k in near[c]]
            if c:
                parts.append(vg_send[head, i])
            total = unpack(parts[0])
            for part in parts[1:]:
                total = total + unpack(part)
            return total

        for c, hh in units:
            for i in range(2):
                swap_send[c, hh, i] = pack(half_sum(c, shared - base + hh, i))
        for i in range(2):

            @pl.when(oi == i)
            def _():
                where = {"kv": middle + 1 - i}
                remote("swap", "swap", swap_send, swap_recv, where).start()

        wait_in("vgn", vg_in.at[:, pl.ds(0, shared)])
        sums_of = {(c, hh, i): half_sum(c, base + hh, i) for c, hh in units for i in range(2)}
        wait_in("sc", sc_in)
        lines = {}
        for c in (0, 1):
            parts = [sc_in[k] for k in slots[c]] + ([sc_send[oi]] if c else [])
            lines[c] = functools.reduce(lambda p, q: p + q, parts)
        factor = lax.rsqrt(column_of(lines[1], shared) / D + RMS_EPS)
        cubed = factor * factor * factor
        weights = {u: column_of(lines[u[0]], u[1]) * cubed for u in units}
        wait_in("swap", swap_recv)
        gates, news = {}, {}
        for c, hh in units:
            both = [sums_of[c, hh, i] + unpack(swap_recv[c, hh, i]) for i in range(2)]
            news[c, hh] = weights[c, hh] * both[0]
            gate = both[1] * factor
            gates[c, hh] = gate / (1.0 + jnp.exp(-gate))
        wait_in("ca", ca_in)
        totals = {}
        for c, hh in units:
            parts = [ca_in[k, hh] for k in slots[c]] + ([ca_send[base + hh]] if c else [])
            total = unpack(parts[0])
            for part in parts[1:]:
                total = total + unpack(part)
            totals[c, hh] = total * factor + news[c, hh]
        sums = {u: jnp.sum(totals[u], axis=1, keepdims=True) for u in units}
        squared = {u: jnp.sum(totals[u] * totals[u], axis=1, keepdims=True) for u in units}
        for c, hh in units:
            center = sums[c, hh] / DK
            spread = squared[c, hh] / DK - center * center
            normed = (totals[c, hh] - center) * lax.rsqrt(spread + GN_EPS)
            result = pack(gates[c, hh] * normed)
            gt_send[c, hh] = result
            if c:
                gt_buf[oi, hh] = result
        for c in (0, 1):
            for j in (3, 1, 2) + ((0,) if c == 0 else ()):
                where = {"kv": kv_peer(j) if j else me_kv, "tp": first_core + c}
                for i in range(2):

                    @pl.when(oi == i)
                    def _():
                        remote("gt", f"gt{i}", gt_send.at[c], gt_buf.at[i], where).start()

    loads["wo"].wait()
    loads["gg"].wait()
    for i in range(2):

        @pl.when(jnp.logical_not((me_core == 1) & (me_kv == middle + i)))
        def _():
            wait_in(f"gt{i}", gt_buf.at[i])

    for h in range(heads):
        cols = pl.ds(h * DK, DK)
        x_buf[:, cols] = (
            unpack(gt_buf[h // shared, h % shared]) * gn_gain_ref[:, cols]
        ).astype(BF16)
    gated = x_buf[...]

    def o_send(part, core):
        mine = o_buf.at[part, me_tp]
        if core is None:
            remote("o", f"o{part}", mine, mine, {"tp": tp_peer(1)}).start()
        else:
            for chip in range(n_tp // 2 - 1, 0, -1):
                target = partner(first_core, 2 * chip, n_tp) + core
                remote("o", f"o{part}", mine, mine, {"tp": target}).start()

    for part in range(2):
        width = depth // 2
        piece = jnp.dot(gated, wo[:, pl.ds(part * width, width)], preferred_element_type=F32)
        o_buf[part, me_tp] = pack(piece)
        o_send(part, 0)
    for part in range(2):
        o_send(part, 1)
    for part in range(2):
        o_send(part, None)
    loads["fg"].wait()
    for part in range(2):
        wait_in(f"o{part}", o_buf.at[part, pl.ds(0, n_tp - 1)])
    squares = jnp.zeros((rows, 1), F32)
    halves = []
    for part in range(2):
        total = unpack(o_buf[part, 0])
        for t in range(1, n_tp):
            total = total + unpack(o_buf[part, t])
        halves.append(total)
    mixed = jnp.concatenate(halves, axis=1)
    for c in range(n_tp):
        cols = pl.ds(c * own_cols, own_cols)
        own_mixed = mixed[:, c * own_cols : (c + 1) * own_cols]
        resid = (tok_buf[c].astype(F32) + own_mixed).astype(BF16)
        resid_wide = resid.astype(F32)
        resid_buf[c] = resid_wide
        squares = squares + jnp.sum(resid_wide * resid_wide, axis=1, keepdims=True)
        x_buf[:, cols] = (resid_wide * ffn_gain_ref[:, cols]).astype(BF16)
    sqm_send[...] = lanes_of([squares])
    for j in kv_order:
        remote("sqm", "sqm", sqm_send, sqm_recv.at[j - 1], {"kv": kv_peer(j)}).start()

    x = x_buf[...]
    loads["wfg"].wait()
    loads["wfu"].wait()

    def stage_start(s, index):
        return pl.multiple_of((s * n_kv + index) * win, win)

    for s in range(n_full):
        for j in kv_order:
            cols = pl.ds(stage_start(s, kv_peer(j)), win)
            for i, weight in enumerate((wfg, wfu)):
                part = jnp.dot(x, weight[:, cols], preferred_element_type=F32)
                gu_send[s, j - 1, i] = pack(part)
            remote(
                "gu", f"gu{s}", gu_send.at[s, j - 1], gu_recv.at[s, j - 1], {"kv": kv_peer(j)}
            ).start()
    if rest:
        cols = pl.ds(rest_base, rest * LANES)
        both = [jnp.dot(x, w[:, cols], preferred_element_type=F32) for w in (wfg, wfu)]
        width = rest_tiles * LANES
        for o in range(2):
            mine = jnp.concatenate([b[:, o * width : (o + 1) * width] for b in both], axis=1)
            rest_send[o] = stack(mine, 2 * rest_tiles)
        for o in range(2):

            to_owner(o, [("rest", rest_send.at[o], rest_recv.at[owner_slot(o)])])

    for s in range(n_full):
        cols = pl.ds(stage_start(s, me_kv), win)
        for i, weight in enumerate((wfg, wfu)):
            gu_own[s, i] = jnp.dot(x, weight[:, cols], preferred_element_type=F32)

    wait_in("sqm", sqm_recv)
    total_sq = sqm_send[...]
    for j in range(1, n_kv):
        total_sq = total_sq + sqm_recv[j - 1]
    factor = lax.rsqrt(column_of(total_sq, 0) / D + RMS_EPS)

    def activate(gate, up):
        gate, up = gate * factor, up * factor
        return gate / (1.0 + jnp.exp(-gate)) * up

    for s in range(n_full):
        wait_in(f"gu{s}", gu_recv.at[s])
        both = []
        for i in range(2):
            total = gu_own[s, i]
            for j in kv_order:
                total = total + unpack(gu_recv[s, j - 1, i])
            both.append(total)
        hid_send[s] = pack(activate(*both))
        for j in (2, 3, 1):
            remote(
                "hid", f"hid{s}", hid_send.at[s], hid_recv.at[s, j - 1], {"kv": kv_peer(j)}
            ).start()

    if rest:

        @pl.when(is_owner)
        def _():
            o = me_kv - middle
            wait_in("rest", rest_recv)
            width = rest_tiles * LANES
            for c in (0, 1):
                slots = range(n_kv) if c == 0 else range(n_kv, 2 * n_kv - 1)
                parts = [rest_recv[k] for k in slots] + ([rest_send[o]] if c else [])
                total = unstack(parts[0], 2 * rest_tiles)
                for part in parts[1:]:
                    total = total + unstack(part, 2 * rest_tiles)
                result = stack(activate(total[:, :width], total[:, width:]), rest_tiles)
                rest_out[c] = result
                if c:
                    rest_hid[o] = result
                for j in kv_order + ((0,) if c == 0 else ()):
                    where = {"kv": kv_peer(j) if j else me_kv, "tp": first_core + c}
                    for i in range(2):

                        @pl.when(o == i)
                        def _():
                            remote(
                                "rhid", f"rhid{i}", rest_out.at[c], rest_hid.at[i], where
                            ).start()

    loads["wfd"].wait()

    def down_of(s, index, packed):
        weight = wfd[pl.ds(stage_start(s, index), win), :]
        return jnp.dot(unpack(packed).astype(BF16), weight, preferred_element_type=F32)

    down = None
    for s in range(n_full):
        part = down_of(s, me_kv, hid_send[s])
        down = part if down is None else down + part
    for s in range(n_full):
        wait_in(f"hid{s}", hid_recv.at[s])
        for j in range(1, n_kv):
            down = down + down_of(s, kv_peer(j), hid_recv[s, j - 1])
    if rest:
        near = jnp.where(me_kv > middle, 1, 0)
        width = rest_tiles * LANES
        for o in (near, 1 - near):

            @pl.when(jnp.logical_not((me_core == 1) & (me_kv == middle + o)))
            def _():
                for i in range(2):

                    @pl.when(o == i)
                    def _():
                        wait_in(f"rhid{i}", rest_hid.at[i])

            chunk = unstack(rest_hid[o], rest_tiles).astype(BF16)
            first = pl.multiple_of(rest_base + o * width, LANES)
            weight = wfd[pl.ds(first, width), :]
            down = down + jnp.dot(chunk, weight, preferred_element_type=F32)
    down_buf[...] = down
    for t in range(n_tp):
        d_send[t] = pack(down_buf[:, pl.ds(t * own_cols, own_cols)])
    to_tp("d", "d", lambda target: d_send.at[target], d_recv.at[me_tp])
    own = pl.ds(pl.multiple_of(me_tp * own_cols, own_cols), own_cols)
    result = down_buf[:, own] + resid_buf[me_tp]
    wait_in("d", d_recv.at[pl.ds(0, n_tp - 1)])
    for j in range(1, n_tp):
        result = result + unpack(d_recv[tp_peer(j)])
    out_ref[...] = result.astype(BF16)
    wait_out("tok", tok_buf.at[pl.ds(0, n_tp - 1)])
    wait_out("q", q_recv)
    wait_out("o", o_buf.at[:, pl.ds(0, n_tp - 1)])
    wait_out("sqm", sqm_recv)
    wait_out("gu", gu_recv)
    wait_out("hid", hid_recv)
    wait_out("d", d_recv.at[pl.ds(0, n_tp - 1)])
    for i in range(2):

        @pl.when(jnp.logical_not((me_core == 1) & (me_kv == middle + i)))
        def _():
            if rest:
                wait_out(f"rest{i}", rest_send.at[i])

    wait_out("ca0", ca_send.at[far_group])
    wait_out("sc0", sc_send.at[0])

    @pl.when(jnp.logical_not(is_owner))
    def _():
        wait_out("ca1", ca_send.at[near_group])
        wait_out("sc1", sc_send.at[0])

    @pl.when(jnp.logical_not(is_owner))
    def _():
        wait_out("vg", vg_send)

    @pl.when(is_owner)
    def _():
        wait_out("gt", ca_in)
        wait_out("swap", swap_send)
        if rest:
            wait_out("rhid", rest_hid)


def fused(
    n_kv,
    n_tp,
    tokens,
    lengths,
    attn_gain,
    w_query,
    w_key,
    w_value,
    w_gate,
    log_decay,
    key_cache,
    value_cache,
    gn_gain,
    w_out,
    ffn_gain,
    w_ffn_gate,
    w_ffn_up,
    w_ffn_down,
):
    rows, own_cols = tokens.shape
    depth, wide = w_query.shape
    span = key_cache.shape[1]
    heads = log_decay.shape[0]
    shared = heads // 2
    win = STAGE_TILES * LANES
    n_full, rest = plan(w_ffn_gate.shape[1] // LANES, n_kv)
    rest_rows = max(rest // 2, 1) * rows
    peers = n_kv - 1
    vmem = pl.BlockSpec(memory_space=pltpu.VMEM)
    hbm = pl.BlockSpec(memory_space=pl.ANY)
    small = (
        tokens,
        lengths,
        attn_gain[None, :],
        log_decay,
        gn_gain[None, :],
        ffn_gain[None, :],
    )
    streamed = (
        w_query,
        w_key,
        w_value,
        w_gate,
        key_cache,
        value_cache,
        w_out,
        w_ffn_gate,
        w_ffn_up,
        w_ffn_down,
    )
    scratch = [pltpu.VMEM(a.shape, a.dtype) for a in streamed] + [
        (pltpu.SMEM if a.ndim == 1 else pltpu.VMEM)(a.shape, a.dtype) for a in small
    ]
    piece = (2 * rows, DK // 2)
    scratch += [
        pltpu.VMEM((n_tp, rows, own_cols), BF16),
        pltpu.VMEM((rows, depth), BF16),
        pltpu.VMEM((heads, *piece), BF16),
        pltpu.VMEM((heads, peers, *piece), BF16),
        pltpu.VMEM((rows, wide), F32),
        pltpu.VMEM((2, rows, DK // 2), F32),
        pltpu.VMEM((heads, rows, rows * span), F32),
        pltpu.VMEM((rows, wide), F32),
        pltpu.VMEM((heads, 2, *piece), BF16),
        pltpu.VMEM((peers, heads, 2, *piece), BF16),
        pltpu.VMEM((2, shared, 2, *piece), BF16),
        pltpu.VMEM((2, shared, 2, *piece), BF16),
        pltpu.VMEM((heads, *piece), BF16),
        pltpu.VMEM((2 * n_kv - 1, shared, *piece), BF16),
        pltpu.VMEM((2, 1, LANES), F32),
        pltpu.VMEM((2 * n_kv - 1, 1, LANES), F32),
        pltpu.VMEM((2, shared, *piece), BF16),
        pltpu.VMEM((2, shared, *piece), BF16),
        pltpu.VMEM((2, n_tp, 2 * rows, depth // 4), BF16),
        pltpu.VMEM((n_tp, rows, own_cols), F32),
        pltpu.VMEM((1, LANES), F32),
        pltpu.VMEM((peers, 1, LANES), F32),
        pltpu.VMEM((n_full, 2, rows, win), F32),
        pltpu.VMEM((n_full, peers, 2, 2 * rows, win // 2), BF16),
        pltpu.VMEM((n_full, peers, 2, 2 * rows, win // 2), BF16),
        pltpu.VMEM((n_full, 2 * rows, win // 2), BF16),
        pltpu.VMEM((n_full, peers, 2 * rows, win // 2), BF16),
        pltpu.VMEM((2, 2 * rest_rows, LANES), BF16),
        pltpu.VMEM((2 * n_kv - 1, 2 * rest_rows, LANES), BF16),
        pltpu.VMEM((2, rest_rows, LANES), BF16),
        pltpu.VMEM((2 * n_kv - 1, rest_rows, LANES), BF16),
        pltpu.VMEM((rows, depth), F32),
        pltpu.VMEM((n_tp, 2 * rows, own_cols // 2), BF16),
        pltpu.VMEM((n_tp, 2 * rows, own_cols // 2), BF16),
        pltpu.SemaphoreType.DMA((len(small) + len(streamed),)),
        pltpu.SemaphoreType.DMA((17,)),
        pltpu.SemaphoreType.DMA((15 + heads + 2 * n_full,)),
        pltpu.SemaphoreType.REGULAR,
    ]
    return pl.pallas_call(
        functools.partial(layer_kernel, n_kv, n_tp),
        out_shape=pltpu.VMEM((rows, own_cols), BF16),
        in_specs=[hbm] * (len(small) + len(streamed)),
        out_specs=vmem,
        scratch_shapes=scratch,
        compiler_params=pltpu.CompilerParams(
            collective_id=0, has_side_effects=True, vmem_limit_bytes=60 * 1024 * 1024
        ),
    )(*small, *streamed)


def fits(mesh, tokens, log_decay, key_cache, w_query, w_ffn_gate):
    n_kv, n_tp, n_grp = mesh.shape["kv"], mesh.shape["tp"], mesh.shape["grp"]
    heads, span = log_decay.shape[0], key_cache.shape[1] // n_kv
    tiles = w_ffn_gate.shape[1] // n_tp // LANES
    rows = tokens.shape[0] // n_grp
    return (
        n_kv > 1
        and n_tp > 2
        and n_kv & (n_kv - 1) == 0
        and n_tp & (n_tp - 1) == 0
        and heads == n_kv * n_tp
        and (heads // n_tp // 2 + 1) * rows <= LANES
        and tokens.shape[1] // n_kv == heads * DK // n_tp
        and tokens.shape[1] % (n_kv * n_tp * 2 * LANES) == 0
        and heads * DK // n_tp % (4 * LANES) == 0
        and w_ffn_gate.shape[1] % (n_tp * LANES) == 0
        and plan(tiles, n_kv)[0] > 0
        and plan(tiles, n_kv)[1] % 2 == 0
        and n_kv > 2
        and tokens.shape[0] // n_grp % 8 == 0
        and span % 16 == 0
        and span <= 64
    )


def solution(mesh):
    specs = (
        P("grp", ("kv", "tp")),
        P("grp"),
        P("kv"),
        P("kv", "tp"),
        P("kv", "tp"),
        P("kv", "tp"),
        P("kv", "tp"),
        P("tp"),
        P("grp", "kv", "tp"),
        P("grp", "kv", "tp"),
        P("tp"),
        P("tp", "kv"),
        P("kv"),
        P("kv", "tp"),
        P("kv", "tp"),
        P("tp", "kv"),
    )

    def whole(*arrays):
        tokens, w_query, log_decay, key_cache = arrays[0], arrays[3], arrays[7], arrays[8]
        if fits(mesh, tokens, log_decay, key_cache, w_query, arrays[13]):
            body = functools.partial(fused, mesh.shape["kv"], mesh.shape["tp"])
        else:
            body = local
        return jax.shard_map(
            body,
            mesh=mesh,
            in_specs=specs,
            out_specs=P("grp", ("kv", "tp")),
            check_vma=False,
        )(*arrays)

    return whole
```

```python
import functools
import math

import jax
import jax.numpy as jnp
from jax import lax
from jax.experimental import pallas as pl
from jax.experimental.pallas import tpu as pltpu
from jax.sharding import PartitionSpec as P

DK = 256
D = 4096


RMS_EPS = 0.1
GN_EPS = 1.0
ROPE_BASE = 10000.0


def rotate(vectors, positions):
    half_dim = vectors.shape[-1] // 2
    inverse = ROPE_BASE ** (-jnp.arange(half_dim, dtype=jnp.float32) / half_dim)
    angles = positions[:, None, None] * inverse[None, None, :]
    cosine = jnp.cos(angles)
    sine_part = jnp.sin(angles)
    front_part = vectors[..., :half_dim]
    back_part = vectors[..., half_dim:]
    return jnp.concatenate(
        [front_part * cosine - back_part * sine_part, front_part * sine_part + back_part * cosine],
        axis=-1,
    )


def group_norm(totals, gn_gain):
    width = totals.shape[-1]
    center = jnp.sum(totals, axis=-1, keepdims=True) / width
    spread = jnp.sum(totals * totals, axis=-1, keepdims=True) / width - center * center
    normed = (totals - center) * lax.rsqrt(spread + GN_EPS)
    return normed.reshape(normed.shape[0], -1) * gn_gain


def channel_stat(own_squares):
    return lax.psum(own_squares, "kv")


def input_stat(own_squares):
    return lax.psum(own_squares, "kv")


def cache_partial(query_low, lengths, log_decay, key_cache, value_cache, heads_here):
    batch_rows = query_low.shape[0]
    span = key_cache.shape[1]
    slots = lax.axis_index("kv") * span + jnp.arange(span, dtype=jnp.int32)
    live = slots[None, :] < lengths[:, None]
    gaps = jnp.maximum((lengths[:, None] - slots[None, :]).astype(jnp.float32), 0.0)
    decays = jnp.exp(log_decay[None, None, :] * gaps[:, :, None])
    keys_here = key_cache.reshape(batch_rows, span, heads_here, DK)
    values_here = value_cache.reshape(batch_rows, span, heads_here, DK)
    scores = jnp.einsum("bphd,bhd->bph", keys_here, query_low, preferred_element_type=jnp.float32)
    mixing = jnp.where(live[:, :, None], scores * decays, 0.0).astype(jnp.bfloat16)
    return jnp.einsum("bph,bphd->bhd", mixing, values_here, preferred_element_type=jnp.float32)


def local(
    tokens,
    lengths,
    attn_gain,
    w_query,
    w_key,
    w_value,
    w_gate,
    log_decay,
    key_cache,
    value_cache,
    gn_gain,
    w_out,
    ffn_gain,
    w_ffn_gate,
    w_ffn_up,
    w_ffn_down,
):
    batch_rows = tokens.shape[0]
    heads_here = log_decay.shape[0]
    row_block = lax.all_gather(tokens, "tp", axis=1, tiled=True)
    widened = row_block.astype(jnp.float32)
    own_squares = jnp.sum(widened * widened, axis=1)
    scaled = (widened * attn_gain).astype(jnp.bfloat16)
    part_query = jnp.dot(scaled, w_query, preferred_element_type=jnp.float32)
    part_key = jnp.dot(scaled, w_key, preferred_element_type=jnp.float32)
    part_value = jnp.dot(scaled, w_value, preferred_element_type=jnp.float32)
    part_gate = jnp.dot(scaled, w_gate, preferred_element_type=jnp.float32)
    positions = lengths.astype(jnp.float32)
    total_squares = input_stat(own_squares)
    queries, new_keys, new_values, gates = lax.psum(
        (part_query, part_key, part_value, part_gate), "kv"
    )
    factor = lax.rsqrt(total_squares / D + RMS_EPS)[:, None]
    queries = rotate((queries * factor).reshape(batch_rows, heads_here, DK), positions) * DK ** (
        -0.5
    )
    new_keys = rotate((new_keys * factor).reshape(batch_rows, heads_here, DK), positions)
    new_values = (new_values * factor).reshape(batch_rows, heads_here, DK)
    gates = gates * factor
    query_low = queries.astype(jnp.bfloat16)
    partial_value = cache_partial(query_low, lengths, log_decay, key_cache, value_cache, heads_here)
    cached = lax.psum(partial_value.reshape(batch_rows, heads_here * DK), "kv")
    own_term = jnp.sum(queries * new_keys, axis=-1, keepdims=True) * new_values
    normed = group_norm(cached.reshape(batch_rows, heads_here, DK) + own_term, gn_gain)
    gated = (jax.nn.silu(gates) * normed).astype(jnp.bfloat16)
    out_partial = jnp.dot(gated, w_out, preferred_element_type=jnp.float32)
    mixed = lax.psum_scatter(out_partial, "tp", scatter_dimension=1, tiled=True)
    resid = (tokens.astype(jnp.float32) + mixed).astype(jnp.bfloat16)
    resid_block = lax.all_gather(resid, "tp", axis=1, tiled=True).astype(jnp.float32)
    mid_squares = jnp.sum(resid_block * resid_block, axis=1)
    scaled_mid = (resid_block * ffn_gain).astype(jnp.bfloat16)
    gate_part = jnp.dot(scaled_mid, w_ffn_gate, preferred_element_type=jnp.float32)
    up_part = jnp.dot(scaled_mid, w_ffn_up, preferred_element_type=jnp.float32)
    total_mid = channel_stat(mid_squares)
    gate_sum, up_sum = lax.psum((gate_part, up_part), "kv")
    factor_mid = lax.rsqrt(total_mid / D + RMS_EPS)[:, None]
    hidden = (jax.nn.silu(gate_sum * factor_mid) * (up_sum * factor_mid)).astype(jnp.bfloat16)
    down_partial = jnp.dot(hidden, w_ffn_down, preferred_element_type=jnp.float32)
    down = lax.psum_scatter(down_partial, "tp", scatter_dimension=1, tiled=True)
    return (resid.astype(jnp.float32) + down).astype(jnp.bfloat16)


LANES = 128
STAGE_TILES = 2
F32 = jnp.float32
BF16 = jnp.bfloat16


def partner(index, j, parts):
    found, bit = 0, 1
    while bit < parts:
        digit = (index // bit) % 2
        found = found + bit * ((1 - digit) if (j // bit) % 2 else digit)
        bit *= 2
    return found


def stack(value, pieces):
    width = value.shape[1] // pieces
    return jnp.concatenate(
        [value[:, i * width : (i + 1) * width] for i in range(pieces)], axis=0
    ).astype(BF16)


def unstack(packed, pieces):
    wide = packed.astype(F32)
    rows = wide.shape[0] // pieces
    return jnp.concatenate([wide[i * rows : (i + 1) * rows] for i in range(pieces)], axis=1)


def pack(value):
    return stack(value, 2)


def unpack(packed):
    return unstack(packed, 2)


def plan(tiles, n_kv):
    step = STAGE_TILES * n_kv
    return tiles // step, tiles % step


def layer_kernel(
    n_kv,
    n_tp,
    tokens_hbm,
    lengths_hbm,
    attn_gain_hbm,
    log_decay_hbm,
    gn_gain_hbm,
    ffn_gain_hbm,
    wq_hbm,
    wk_hbm,
    wv_hbm,
    wg_hbm,
    kc_hbm,
    vc_hbm,
    wo_hbm,
    wfg_hbm,
    wfu_hbm,
    wfd_hbm,
    out_ref,
    wq,
    wkvg,
    caches,
    wo,
    wgu,
    wfd,
    tokens_ref,
    lengths_ref,
    attn_gain_ref,
    log_decay_ref,
    gn_gain_ref,
    ffn_gain_ref,
    tok_buf,
    x_buf,
    q_send,
    q_recv,
    q_full,
    trig,
    decay_buf,
    key_own,
    vg_send,
    vg_in,
    swap_send,
    swap_recv,
    ca_send,
    ca_in,
    sc_send,
    sc_in,
    gt_send,
    gt_buf,
    o_buf,
    resid_buf,
    sqm_send,
    sqm_recv,
    gu_own,
    gu_send,
    gu_recv,
    hid_send,
    hid_recv,
    rest_send,
    rest_recv,
    rest_out,
    rest_hid,
    down_buf,
    d_send,
    d_recv,
    load_sem,
    send_sem,
    recv_sem,
    go_sem,
):
    wk, wv, wg = [wkvg.at[i] for i in range(3)]
    kc, vc = [caches.at[i] for i in range(2)]
    wfg, wfu = [wgu.at[i] for i in range(2)]
    rows, own_cols = tokens_ref.shape
    depth, wide = wq.shape
    span = kc.shape[1]
    half = DK // 2
    tiles = wfg.shape[1] // LANES
    win = STAGE_TILES * LANES
    n_full, rest = plan(tiles, n_kv)
    rest_tiles = rest // 2
    rest_base = n_full * STAGE_TILES * n_kv * LANES
    heads = n_kv
    middle = n_kv // 2 - 1
    shared = heads // 2
    me_kv = lax.axis_index("kv")
    me_tp = lax.axis_index("tp")
    me_core = me_tp % 2
    first_core = me_tp - me_core
    is_middle = (me_kv >= middle) & (me_kv < middle + 2)
    is_owner = (me_core == 1) & is_middle
    side = jnp.where(me_kv > middle, 1, 0)
    far_group = pl.ds((1 - side) * shared, shared)
    near_group = pl.ds(side * shared, shared)

    def kv_peer(j):
        return partner(me_kv, j, n_kv)

    def tp_peer(j):
        return partner(me_tp, j, n_tp)

    kv_order = tuple(range(n_kv - 1, 0, -1))

    barrier = pltpu.get_barrier_semaphore()
    for j in range(1, n_tp):
        pl.semaphore_signal(
            barrier, inc=1, device_id={"tp": tp_peer(j)}, device_id_type=pl.DeviceIdType.MESH
        )
    for k in range(1, n_kv):

        @pl.when(me_kv < k)
        def _():
            pl.semaphore_signal(
                barrier, inc=1, device_id={"kv": k}, device_id_type=pl.DeviceIdType.MESH
            )

    loads, load_slot = {}, {}

    def wait_group(name, ref):
        pltpu.make_async_copy(ref, ref, load_sem.at[load_slot[name]]).wait()

    for slot, (name, src, dst) in enumerate(
        (
            ("tok", tokens_hbm, tokens_ref),
            ("len", lengths_hbm, lengths_ref),
            ("ag", attn_gain_hbm, attn_gain_ref),
            ("ld", log_decay_hbm, log_decay_ref),
            ("gg", gn_gain_hbm, gn_gain_ref),
            ("fg", ffn_gain_hbm, ffn_gain_ref),
            ("wq", wq_hbm, wq),
            ("kc", kc_hbm, kc),
            ("vc", vc_hbm, vc),
            ("wk", wk_hbm, wk),
            ("wv", wv_hbm, wv),
            ("wg", wg_hbm, wg),
            ("wo", wo_hbm, wo),
            ("wfg", wfg_hbm, wfg),
            ("wfu", wfu_hbm, wfu),
            ("wfd", wfd_hbm, wfd),
        )
    ):
        shared_slot = {"vc": "kc", "wv": "wk", "wg": "wk", "wfu": "wfg"}.get(name, name)
        load_slot.setdefault(shared_slot, len(load_slot))
        loads[name] = pltpu.make_async_copy(src, dst, load_sem.at[load_slot[shared_slot]])

    names = ["tok", "q", "o", "sqm", "gu", "hid", "d", "gt", "rhid"]
    names += [f"{kind}{i}" for kind in ("ca", "sc", "rest") for i in range(2)]
    names += ["vg", "swap"]
    out_slot = {name: i for i, name in enumerate(names)}
    names = ["tok", "vgf", "vgn", "swap", "ca", "sc", "gt0", "gt1", "o0", "o1", "sqm", "d"]
    names += [f"q{h}" for h in range(heads)] + ["rest", "rhid0", "rhid1"]
    names += [f"{kind}{i}" for kind in ("gu", "hid") for i in range(n_full)]
    in_slot = {name: i for i, name in enumerate(names)}

    def remote(out, into, src, dst, where):
        return pltpu.make_async_remote_copy(
            src_ref=src,
            dst_ref=dst,
            send_sem=send_sem.at[out_slot[out]],
            recv_sem=recv_sem.at[in_slot[into]],
            device_id=where,
            device_id_type=pl.DeviceIdType.MESH,
        )

    def wait_in(into, ref):
        remote("tok", into, ref, ref, {"kv": kv_peer(1)}).wait_recv()

    def wait_out(out, ref):
        remote(out, "tok", ref, ref, {"kv": kv_peer(1)}).wait_send()

    def to_tp(out, into, src_of, dst):
        for chip in range(n_tp // 2 - 1, 0, -1):
            for core in (0, 1):
                target = partner(first_core, 2 * chip, n_tp) + core
                remote(out, into, src_of(target), dst, {"tp": target}).start()
        remote(out, into, src_of(tp_peer(1)), dst, {"tp": tp_peer(1)}).start()

    lane_id = lax.broadcasted_iota(jnp.int32, (8, LANES), 1)
    row_of = lax.broadcasted_iota(jnp.int32, (8, LANES), 0)

    def lanes_of(columns):
        spread = jnp.zeros((8, LANES), F32)
        for i, column in enumerate(columns):
            for first in range(0, rows, 8):
                part = jnp.broadcast_to(column[first : first + 8], (8, LANES))
                spread = jnp.where(lane_id == row_of + (i * rows + first), part, spread)
        return jnp.sum(spread, axis=0, keepdims=True)

    def column_of(line, i):
        wide_line = jnp.broadcast_to(line, (8, LANES))
        return jnp.concatenate(
            [
                jnp.sum(
                    jnp.where(lane_id == row_of + (i * rows + first), wide_line, 0.0),
                    axis=1,
                    keepdims=True,
                )
                for first in range(0, rows, 8)
            ],
            axis=0,
        )

    for name in ("tok", "len", "ld", "ag", "wq"):
        loads[name].start()
    pl.semaphore_wait(barrier, n_tp - 1 + me_kv)
    for k in range(n_kv - 1):

        @pl.when(me_kv > k)
        def _():
            pl.semaphore_signal(
                go_sem, inc=1, device_id={"kv": k}, device_id_type=pl.DeviceIdType.MESH
            )

    loads["tok"].wait()
    to_tp("tok", "tok", lambda target: tokens_ref, tok_buf.at[me_tp])
    for name in ("wk", "wv", "wg", "kc", "vc", "gg", "fg"):
        loads[name].start()
    tok_buf[me_tp] = tokens_ref[...]

    for name in ("len", "ld", "ag"):
        loads[name].wait()
    row_id = lax.broadcasted_iota(jnp.int32, (rows, LANES), 0)
    lens = jnp.zeros((rows, LANES), jnp.int32)
    for b in range(rows):
        lens = jnp.where(row_id == b, lengths_ref[b], lens)
    lane = lax.broadcasted_iota(jnp.int32, (rows, half), 1).astype(F32)
    inverse = jnp.exp(lane * (-math.log(ROPE_BASE) / half))
    angles = lens[:, :1].astype(F32) * inverse
    trig[0] = jnp.cos(angles)
    trig[1] = jnp.sin(angles)
    places = rows * span
    col = lax.broadcasted_iota(jnp.int32, (rows, places), 1)
    row = lax.broadcasted_iota(jnp.int32, (rows, places), 0)
    slot = col - row * span
    position = slot + me_kv * span
    gap = lens[:, :1] - position
    live = (slot >= 0) & (slot < span) & (gap > 0)
    gap_f = jnp.where(live, gap, 0).astype(F32)
    for h in range(heads):
        decay_buf[h] = jnp.where(live, jnp.exp(gap_f * log_decay_ref[h]), 0.0)

    def rotate_in(front, back):
        cosine, sine = trig[0], trig[1]
        return front * cosine - back * sine, front * sine + back * cosine

    wait_in("tok", tok_buf.at[pl.ds(0, n_tp - 1)])
    squares = jnp.zeros((rows, 1), F32)
    for c in range(n_tp):
        wide_tok = tok_buf[c].astype(F32)
        squares = squares + jnp.sum(wide_tok * wide_tok, axis=1, keepdims=True)
        cols = pl.ds(c * own_cols, own_cols)
        x_buf[:, cols] = (wide_tok * attn_gain_ref[:, cols]).astype(BF16)
    @pl.when(me_kv < n_kv - 1)
    def _():
        pl.semaphore_wait(go_sem, n_kv - 1 - me_kv)


    x = x_buf[...]
    loads["wq"].wait()

    def head_at(place):
        return ((1 - side) if place < shared else side) * shared + place % shared

    def head_cols(h):
        return pl.ds(pl.multiple_of(h * DK, DK), DK)

    def q_slot(h):
        return recv_sem.at[in_slot["q0"] + h]

    def send_q(group, peers):
        for i in range(shared):
            h = group * shared + i
            for j in peers:
                pltpu.make_async_remote_copy(
                    src_ref=q_send.at[h],
                    dst_ref=q_recv.at[h, j - 1],
                    send_sem=send_sem.at[out_slot["q"]],
                    recv_sem=q_slot(h),
                    device_id={"kv": kv_peer(j)},
                    device_id_type=pl.DeviceIdType.MESH,
                ).start()

    across = [j for j in range(1, n_kv) if j >= n_kv // 2]
    beside = [j for j in kv_order if j < n_kv // 2]
    for group in (side, 1 - side):
        cols = pl.ds(pl.multiple_of(group * shared * DK, DK), shared * DK)
        q_own = jnp.dot(x, wq[:, cols], preferred_element_type=F32)
        q_full[:, cols] = q_own
        for i in range(shared):
            q_send[group * shared + i] = pack(q_own[:, i * DK : (i + 1) * DK])
        if group is side:
            send_q(side, across)
    send_q(1 - side, beside)
    send_q(1 - side, across)
    send_q(side, beside)
    for name in ("wo", "wfg", "wfu", "wfd"):
        loads[name].start()

    wait_group("wk", wkvg)
    for i, weight in enumerate((wv, wg)):
        for pair in range(heads // 2):
            part = jnp.dot(x, weight[:, pl.ds(pair * 2 * DK, 2 * DK)], preferred_element_type=F32)
            for k in range(2):
                vg_send[pair * 2 + k, i] = pack(part[:, k * DK : (k + 1) * DK])
    away = jnp.where(me_kv > middle, me_kv - middle - 1, middle - me_kv)

    @pl.when(jnp.logical_not(is_owner))
    def _():
        slot = jnp.where(me_core == 0, away, n_kv // 2 - 1 + away)
        where = {"kv": middle + side, "tp": first_core + 1}
        for into, group in (("vgf", far_group), ("vgn", near_group)):
            remote("vg", into, vg_send.at[group], vg_in.at[slot, group], where).start()

    key_own[...] = jnp.dot(x, wk[...], preferred_element_type=F32)

    wait_group("kc", caches)

    def apart_from(oi):
        both = [partner(me_kv, middle + i, n_kv) for i in range(2)]
        return jnp.where(oi == 1, both[1], both[0])

    def owner_slot(oi):
        apart = apart_from(oi)
        return jnp.where(me_core == 0, me_kv, n_kv - 1 + apart)

    def to_owner(oi, copies):
        @pl.when(jnp.logical_not((me_core == 1) & (me_kv == middle + oi)))
        def _():
            for kind, src, dst in copies:
                where = {"kv": middle + oi, "tp": first_core + 1}
                remote(f"{kind}{oi}", kind, src, dst, where).start()

    own_scores = []
    for place in range(heads):
        h = head_at(place)
        cols = head_cols(h)
        pltpu.make_async_remote_copy(
            src_ref=q_recv.at[h],
            dst_ref=q_recv.at[h],
            send_sem=send_sem.at[out_slot["q"]],
            recv_sem=q_slot(h),
            device_id={"kv": kv_peer(1)},
            device_id_type=pl.DeviceIdType.MESH,
        ).wait_recv()
        query = q_full[:, cols]
        for j in kv_order:
            query = query + unpack(q_recv[h, j - 1])
        front, back = rotate_in(query[:, :half], query[:, half:])
        query = jnp.concatenate([front, back], axis=1) * DK ** (-0.5)
        scores = lax.dot_general(
            query.astype(BF16),
            kc[:, :, cols].reshape(places, DK),
            (((1,), (1,)), ((), ())),
            preferred_element_type=F32,
        )
        mixing = (scores * decay_buf[h]).astype(BF16)
        cached = jnp.dot(mixing, vc[:, :, cols].reshape(places, DK), preferred_element_type=F32)
        ca_send[h] = pack(cached)
        key = key_own[:, cols]
        front, back = rotate_in(key[:, :half], key[:, half:])
        own_scores.append(
            jnp.sum(query[:, :half] * front + query[:, half:] * back, axis=1, keepdims=True)
        )
        near, hh = place // shared, place % shared
        oi = side if near else 1 - side
        copies = [(f"ca{near}", "ca", ca_send.at[h], ca_in.at[owner_slot(oi), hh])]
        if hh == shared - 1:
            sc_send[oi] = lanes_of(own_scores[near * shared :] + [squares])
            copies.append((f"sc{near}", "sc", sc_send.at[oi], sc_in.at[owner_slot(oi)]))

        def send_all():
            for out, into, src, dst in copies:
                where = {"kv": middle + oi, "tp": first_core + 1}
                remote(out, into, src, dst, where).start()

        if near:
            pl.when(jnp.logical_not(is_owner))(send_all)
        else:
            send_all()

    @pl.when(is_owner)
    def _():
        oi = me_kv - middle
        base = oi * shared
        units = [(c, hh) for c in (1, 0) for hh in range(shared)]
        slots = {0: range(n_kv), 1: range(n_kv, 2 * n_kv - 1)}
        wait_in("vgf", vg_in.at[:, pl.ds(0, shared)])
        near = {0: range(n_kv // 2), 1: range(n_kv // 2, n_kv - 1)}

        def half_sum(c, head, i):
            parts = [vg_in[k, head, i] for k in near[c]]
            if c:
                parts.append(vg_send[head, i])
            total = unpack(parts[0])
            for part in parts[1:]:
                total = total + unpack(part)
            return total

        for c, hh in units:
            for i in range(2):
                swap_send[c, hh, i] = pack(half_sum(c, shared - base + hh, i))
        for i in range(2):

            @pl.when(oi == i)
            def _():
                where = {"kv": middle + 1 - i}
                remote("swap", "swap", swap_send, swap_recv, where).start()

        wait_in("vgn", vg_in.at[:, pl.ds(0, shared)])
        sums_of = {(c, hh, i): half_sum(c, base + hh, i) for c, hh in units for i in range(2)}
        wait_in("sc", sc_in)
        lines = {}
        for c in (0, 1):
            parts = [sc_in[k] for k in slots[c]] + ([sc_send[oi]] if c else [])
            lines[c] = functools.reduce(lambda p, q: p + q, parts)
        factor = lax.rsqrt(column_of(lines[1], shared) / D + RMS_EPS)
        cubed = factor * factor * factor
        weights = {u: column_of(lines[u[0]], u[1]) * cubed for u in units}
        wait_in("swap", swap_recv)
        gates, news = {}, {}
        for c, hh in units:
            both = [sums_of[c, hh, i] + unpack(swap_recv[c, hh, i]) for i in range(2)]
            news[c, hh] = weights[c, hh] * both[0]
            gate = both[1] * factor
            gates[c, hh] = gate / (1.0 + jnp.exp(-gate))
        wait_in("ca", ca_in)
        totals = {}
        for c, hh in units:
            parts = [ca_in[k, hh] for k in slots[c]] + ([ca_send[base + hh]] if c else [])
            total = unpack(parts[0])
            for part in parts[1:]:
                total = total + unpack(part)
            totals[c, hh] = total * factor + news[c, hh]
        sums = {u: jnp.sum(totals[u], axis=1, keepdims=True) for u in units}
        squared = {u: jnp.sum(totals[u] * totals[u], axis=1, keepdims=True) for u in units}
        for c, hh in units:
            center = sums[c, hh] / DK
            spread = squared[c, hh] / DK - center * center
            normed = (totals[c, hh] - center) * lax.rsqrt(spread + GN_EPS)
            result = pack(gates[c, hh] * normed)
            gt_send[c, hh] = result
            if c:
                gt_buf[oi, hh] = result
        for c in (0, 1):
            for j in (3, 1, 2) + ((0,) if c == 0 else ()):
                where = {"kv": kv_peer(j) if j else me_kv, "tp": first_core + c}
                for i in range(2):

                    @pl.when(oi == i)
                    def _():
                        remote("gt", f"gt{i}", gt_send.at[c], gt_buf.at[i], where).start()

    loads["wo"].wait()
    loads["gg"].wait()
    for i in range(2):

        @pl.when(jnp.logical_not((me_core == 1) & (me_kv == middle + i)))
        def _():
            wait_in(f"gt{i}", gt_buf.at[i])

    for h in range(heads):
        cols = pl.ds(h * DK, DK)
        x_buf[:, cols] = (
            unpack(gt_buf[h // shared, h % shared]) * gn_gain_ref[:, cols]
        ).astype(BF16)
    gated = x_buf[...]

    def o_send(part, core):
        mine = o_buf.at[part, me_tp]
        if core is None:
            remote("o", f"o{part}", mine, mine, {"tp": tp_peer(1)}).start()
        else:
            for chip in range(n_tp // 2 - 1, 0, -1):
                target = partner(first_core, 2 * chip, n_tp) + core
                remote("o", f"o{part}", mine, mine, {"tp": target}).start()

    for part in range(2):
        width = depth // 2
        piece = jnp.dot(gated, wo[:, pl.ds(part * width, width)], preferred_element_type=F32)
        o_buf[part, me_tp] = pack(piece)
        o_send(part, 0)
    for part in range(2):
        o_send(part, 1)
    for part in range(2):
        o_send(part, None)
    loads["fg"].wait()
    for part in range(2):
        wait_in(f"o{part}", o_buf.at[part, pl.ds(0, n_tp - 1)])
    squares = jnp.zeros((rows, 1), F32)
    halves = []
    for part in range(2):
        total = unpack(o_buf[part, 0])
        for t in range(1, n_tp):
            total = total + unpack(o_buf[part, t])
        halves.append(total)
    mixed = jnp.concatenate(halves, axis=1)
    for c in range(n_tp):
        cols = pl.ds(c * own_cols, own_cols)
        own_mixed = mixed[:, c * own_cols : (c + 1) * own_cols]
        resid = (tok_buf[c].astype(F32) + own_mixed).astype(BF16)
        resid_wide = resid.astype(F32)
        resid_buf[c] = resid_wide
        squares = squares + jnp.sum(resid_wide * resid_wide, axis=1, keepdims=True)
        x_buf[:, cols] = (resid_wide * ffn_gain_ref[:, cols]).astype(BF16)
    sqm_send[...] = lanes_of([squares])
    for j in kv_order:
        remote("sqm", "sqm", sqm_send, sqm_recv.at[j - 1], {"kv": kv_peer(j)}).start()

    x = x_buf[...]
    wait_group("wfg", wgu)

    def stage_start(s, index):
        return pl.multiple_of((s * n_kv + index) * win, win)

    for s in range(n_full):
        for j in kv_order:
            cols = pl.ds(stage_start(s, kv_peer(j)), win)
            for i, weight in enumerate((wfg, wfu)):
                part = jnp.dot(x, weight[:, cols], preferred_element_type=F32)
                gu_send[s, j - 1, i] = pack(part)
            remote(
                "gu", f"gu{s}", gu_send.at[s, j - 1], gu_recv.at[s, j - 1], {"kv": kv_peer(j)}
            ).start()
    if rest:
        cols = pl.ds(rest_base, rest * LANES)
        both = [jnp.dot(x, w[:, cols], preferred_element_type=F32) for w in (wfg, wfu)]
        width = rest_tiles * LANES
        for o in range(2):
            mine = jnp.concatenate([b[:, o * width : (o + 1) * width] for b in both], axis=1)
            rest_send[o] = stack(mine, 2 * rest_tiles)
        for o in range(2):

            to_owner(o, [("rest", rest_send.at[o], rest_recv.at[owner_slot(o)])])

    for s in range(n_full):
        cols = pl.ds(stage_start(s, me_kv), win)
        for i, weight in enumerate((wfg, wfu)):
            gu_own[s, i] = jnp.dot(x, weight[:, cols], preferred_element_type=F32)

    wait_in("sqm", sqm_recv)
    total_sq = sqm_send[...]
    for j in range(1, n_kv):
        total_sq = total_sq + sqm_recv[j - 1]
    factor = lax.rsqrt(column_of(total_sq, 0) / D + RMS_EPS)

    def activate(gate, up):
        gate, up = gate * factor, up * factor
        return gate / (1.0 + jnp.exp(-gate)) * up

    for s in range(n_full):
        wait_in(f"gu{s}", gu_recv.at[s])
        both = []
        for i in range(2):
            total = gu_own[s, i]
            for j in kv_order:
                total = total + unpack(gu_recv[s, j - 1, i])
            both.append(total)
        hid_send[s] = pack(activate(*both))
        for j in (2, 3, 1):
            remote(
                "hid", f"hid{s}", hid_send.at[s], hid_recv.at[s, j - 1], {"kv": kv_peer(j)}
            ).start()

    if rest:

        @pl.when(is_owner)
        def _():
            o = me_kv - middle
            wait_in("rest", rest_recv)
            width = rest_tiles * LANES
            for c in (0, 1):
                slots = range(n_kv) if c == 0 else range(n_kv, 2 * n_kv - 1)
                parts = [rest_recv[k] for k in slots] + ([rest_send[o]] if c else [])
                total = unstack(parts[0], 2 * rest_tiles)
                for part in parts[1:]:
                    total = total + unstack(part, 2 * rest_tiles)
                result = stack(activate(total[:, :width], total[:, width:]), rest_tiles)
                rest_out[c] = result
                if c:
                    rest_hid[o] = result
                for j in kv_order + ((0,) if c == 0 else ()):
                    where = {"kv": kv_peer(j) if j else me_kv, "tp": first_core + c}
                    for i in range(2):

                        @pl.when(o == i)
                        def _():
                            remote(
                                "rhid", f"rhid{i}", rest_out.at[c], rest_hid.at[i], where
                            ).start()

    loads["wfd"].wait()

    def down_of(s, index, packed):
        weight = wfd[pl.ds(stage_start(s, index), win), :]
        return jnp.dot(unpack(packed).astype(BF16), weight, preferred_element_type=F32)

    down = None
    for s in range(n_full):
        part = down_of(s, me_kv, hid_send[s])
        down = part if down is None else down + part
    for s in range(n_full):
        wait_in(f"hid{s}", hid_recv.at[s])
        for j in range(1, n_kv):
            down = down + down_of(s, kv_peer(j), hid_recv[s, j - 1])
    if rest:
        near = jnp.where(me_kv > middle, 1, 0)
        width = rest_tiles * LANES
        for o in (near, 1 - near):

            @pl.when(jnp.logical_not((me_core == 1) & (me_kv == middle + o)))
            def _():
                for i in range(2):

                    @pl.when(o == i)
                    def _():
                        wait_in(f"rhid{i}", rest_hid.at[i])

            chunk = unstack(rest_hid[o], rest_tiles).astype(BF16)
            first = pl.multiple_of(rest_base + o * width, LANES)
            weight = wfd[pl.ds(first, width), :]
            down = down + jnp.dot(chunk, weight, preferred_element_type=F32)
    down_buf[...] = down
    for t in range(n_tp):
        d_send[t] = pack(down_buf[:, pl.ds(t * own_cols, own_cols)])
    to_tp("d", "d", lambda target: d_send.at[target], d_recv.at[me_tp])
    own = pl.ds(pl.multiple_of(me_tp * own_cols, own_cols), own_cols)
    result = down_buf[:, own] + resid_buf[me_tp]
    wait_in("d", d_recv.at[pl.ds(0, n_tp - 1)])
    for j in range(1, n_tp):
        result = result + unpack(d_recv[tp_peer(j)])
    out_ref[...] = result.astype(BF16)
    wait_out("tok", tok_buf.at[pl.ds(0, n_tp - 1)])
    wait_out("q", q_recv)
    wait_out("o", o_buf.at[:, pl.ds(0, n_tp - 1)])
    wait_out("sqm", sqm_recv)
    wait_out("gu", gu_recv)
    wait_out("hid", hid_recv)
    wait_out("d", d_recv.at[pl.ds(0, n_tp - 1)])
    for i in range(2):

        @pl.when(jnp.logical_not((me_core == 1) & (me_kv == middle + i)))
        def _():
            if rest:
                wait_out(f"rest{i}", rest_send.at[i])

    wait_out("ca0", ca_send.at[far_group])
    wait_out("sc0", sc_send.at[0])

    @pl.when(jnp.logical_not(is_owner))
    def _():
        wait_out("ca1", ca_send.at[near_group])
        wait_out("sc1", sc_send.at[0])

    @pl.when(jnp.logical_not(is_owner))
    def _():
        wait_out("vg", vg_send)

    @pl.when(is_owner)
    def _():
        wait_out("gt", ca_in)
        wait_out("swap", swap_send)
        if rest:
            wait_out("rhid", rest_hid)


def fused(
    n_kv,
    n_tp,
    tokens,
    lengths,
    attn_gain,
    w_query,
    w_key,
    w_value,
    w_gate,
    log_decay,
    key_cache,
    value_cache,
    gn_gain,
    w_out,
    ffn_gain,
    w_ffn_gate,
    w_ffn_up,
    w_ffn_down,
):
    rows, own_cols = tokens.shape
    depth, wide = w_query.shape
    span = key_cache.shape[1]
    heads = log_decay.shape[0]
    shared = heads // 2
    win = STAGE_TILES * LANES
    n_full, rest = plan(w_ffn_gate.shape[1] // LANES, n_kv)
    rest_rows = max(rest // 2, 1) * rows
    peers = n_kv - 1
    vmem = pl.BlockSpec(memory_space=pltpu.VMEM)
    hbm = pl.BlockSpec(memory_space=pl.ANY)
    small = (
        tokens,
        lengths,
        attn_gain[None, :],
        log_decay,
        gn_gain[None, :],
        ffn_gain[None, :],
    )
    streamed = (
        w_query,
        w_key,
        w_value,
        w_gate,
        key_cache,
        value_cache,
        w_out,
        w_ffn_gate,
        w_ffn_up,
        w_ffn_down,
    )
    resident = [
        w_query.shape,
        (3, *w_key.shape),
        (2, *key_cache.shape),
        w_out.shape,
        (2, *w_ffn_gate.shape),
        w_ffn_down.shape,
    ]
    scratch = [pltpu.VMEM(shape, BF16) for shape in resident] + [
        (pltpu.SMEM if a.ndim == 1 else pltpu.VMEM)(a.shape, a.dtype) for a in small
    ]
    piece = (2 * rows, DK // 2)
    scratch += [
        pltpu.VMEM((n_tp, rows, own_cols), BF16),
        pltpu.VMEM((rows, depth), BF16),
        pltpu.VMEM((heads, *piece), BF16),
        pltpu.VMEM((heads, peers, *piece), BF16),
        pltpu.VMEM((rows, wide), F32),
        pltpu.VMEM((2, rows, DK // 2), F32),
        pltpu.VMEM((heads, rows, rows * span), F32),
        pltpu.VMEM((rows, wide), F32),
        pltpu.VMEM((heads, 2, *piece), BF16),
        pltpu.VMEM((peers, heads, 2, *piece), BF16),
        pltpu.VMEM((2, shared, 2, *piece), BF16),
        pltpu.VMEM((2, shared, 2, *piece), BF16),
        pltpu.VMEM((heads, *piece), BF16),
        pltpu.VMEM((2 * n_kv - 1, shared, *piece), BF16),
        pltpu.VMEM((2, 1, LANES), F32),
        pltpu.VMEM((2 * n_kv - 1, 1, LANES), F32),
        pltpu.VMEM((2, shared, *piece), BF16),
        pltpu.VMEM((2, shared, *piece), BF16),
        pltpu.VMEM((2, n_tp, 2 * rows, depth // 4), BF16),
        pltpu.VMEM((n_tp, rows, own_cols), F32),
        pltpu.VMEM((1, LANES), F32),
        pltpu.VMEM((peers, 1, LANES), F32),
        pltpu.VMEM((n_full, 2, rows, win), F32),
        pltpu.VMEM((n_full, peers, 2, 2 * rows, win // 2), BF16),
        pltpu.VMEM((n_full, peers, 2, 2 * rows, win // 2), BF16),
        pltpu.VMEM((n_full, 2 * rows, win // 2), BF16),
        pltpu.VMEM((n_full, peers, 2 * rows, win // 2), BF16),
        pltpu.VMEM((2, 2 * rest_rows, LANES), BF16),
        pltpu.VMEM((2 * n_kv - 1, 2 * rest_rows, LANES), BF16),
        pltpu.VMEM((2, rest_rows, LANES), BF16),
        pltpu.VMEM((2 * n_kv - 1, rest_rows, LANES), BF16),
        pltpu.VMEM((rows, depth), F32),
        pltpu.VMEM((n_tp, 2 * rows, own_cols // 2), BF16),
        pltpu.VMEM((n_tp, 2 * rows, own_cols // 2), BF16),
        pltpu.SemaphoreType.DMA((len(small) + len(resident),)),
        pltpu.SemaphoreType.DMA((17,)),
        pltpu.SemaphoreType.DMA((15 + heads + 2 * n_full,)),
        pltpu.SemaphoreType.REGULAR,
    ]
    return pl.pallas_call(
        functools.partial(layer_kernel, n_kv, n_tp),
        out_shape=pltpu.VMEM((rows, own_cols), BF16),
        in_specs=[hbm] * (len(small) + len(streamed)),
        out_specs=vmem,
        scratch_shapes=scratch,
        compiler_params=pltpu.CompilerParams(
            collective_id=0, has_side_effects=True, vmem_limit_bytes=60 * 1024 * 1024
        ),
    )(*small, *streamed)


def fits(mesh, tokens, log_decay, key_cache, w_query, w_ffn_gate):
    n_kv, n_tp, n_grp = mesh.shape["kv"], mesh.shape["tp"], mesh.shape["grp"]
    heads, span = log_decay.shape[0], key_cache.shape[1] // n_kv
    tiles = w_ffn_gate.shape[1] // n_tp // LANES
    rows = tokens.shape[0] // n_grp
    return (
        n_kv > 1
        and n_tp > 2
        and n_kv & (n_kv - 1) == 0
        and n_tp & (n_tp - 1) == 0
        and heads == n_kv * n_tp
        and (heads // n_tp // 2 + 1) * rows <= LANES
        and tokens.shape[1] // n_kv == heads * DK // n_tp
        and tokens.shape[1] % (n_kv * n_tp * 2 * LANES) == 0
        and heads * DK // n_tp % (4 * LANES) == 0
        and w_ffn_gate.shape[1] % (n_tp * LANES) == 0
        and plan(tiles, n_kv)[0] > 0
        and plan(tiles, n_kv)[1] % 2 == 0
        and n_kv > 2
        and tokens.shape[0] // n_grp % 8 == 0
        and span % 16 == 0
        and span <= 64
    )


def solution(mesh):
    specs = (
        P("grp", ("kv", "tp")),
        P("grp"),
        P("kv"),
        P("kv", "tp"),
        P("kv", "tp"),
        P("kv", "tp"),
        P("kv", "tp"),
        P("tp"),
        P("grp", "kv", "tp"),
        P("grp", "kv", "tp"),
        P("tp"),
        P("tp", "kv"),
        P("kv"),
        P("kv", "tp"),
        P("kv", "tp"),
        P("tp", "kv"),
    )

    def whole(*arrays):
        tokens, w_query, log_decay, key_cache = arrays[0], arrays[3], arrays[7], arrays[8]
        if fits(mesh, tokens, log_decay, key_cache, w_query, arrays[13]):
            body = functools.partial(fused, mesh.shape["kv"], mesh.shape["tp"])
        else:
            body = local
        return jax.shard_map(
            body,
            mesh=mesh,
            in_specs=specs,
            out_specs=P("grp", ("kv", "tp")),
            check_vma=False,
        )(*arrays)

    return whole
```
